512 devices in a mesh: sp: 64 (over z, y), tp: 4 (over x), dp: 2 (over core).
Axes of the slice: x: 4, y: 8, z: 8, core: 2. Of those that a mesh axis runs over, the one named last changes fastest.
Arguments:
- latent: bfloat16 [2, 8192, 2048], P('dp', ('sp', 'tp')), may hold values from -10 to 10
- condition: bfloat16 [2, 2048], P('dp'), may hold values from -6 to 6
- context: bfloat16 [2, 512, 2048], P('dp', 'sp'), may hold values from -6 to 6
- context_source: bfloat16 [2048], replicated, may hold values from -6 to 6
- mod_weight: bfloat16 [3, 2048, 2048], P(None, 'sp', 'tp'), may hold values from -0.125 to 0.125
- norm_gain: bfloat16 [2048], replicated, may hold values from 0.099609375 to 1.8984375
- w_x: bfloat16 [2048, 2048], P('dp', 'tp'), may hold values from -0.125 to 0.125
- w_b: bfloat16 [2048, 512], P('dp', 'tp'), may hold values from -0.125 to 0.125
- w_c: bfloat16 [2048, 512], P('dp', 'tp'), may hold values from -0.125 to 0.125
- w_z: bfloat16 [2048, 2048], P('dp', 'tp'), may hold values from -0.125 to 0.125
- w_dt: bfloat16 [2, 2048, 32], P(None, 'dp', 'tp'), may hold values from -0.125 to 0.125
- conv_x: bfloat16 [3, 2048], P(None, 'tp'), may hold values from -3.5 to 3.5
- conv_b: bfloat16 [3, 512], P(None, 'tp'), may hold values from -3.5 to 3.5
- conv_c: bfloat16 [3, 512], P(None, 'tp'), may hold values from -3.5 to 3.5
- decay_rate: float32 [2, 32], P(None, 'tp'), may hold values from 0 to 1, as said below
- out_gain: bfloat16 [2048], P('tp'), may hold values from 0.099609375 to 1.8984375
- w_out: bfloat16 [2048, 2048], P(('tp', 'dp')), may hold values from -0.125 to 0.125
Outputs:
- update: bfloat16 [2, 8192, 2048], P('dp', ('sp', 'tp'))
The draws below stay inside these ranges and needn't reach their ends.
Inputs may be any that keep to these rules, and one draw needn't show every extreme that they name: `decay_rate`: positive rates.
All inputs are finite; a program needn't handle non-finite values.
Results may differ from the reference program's by a relative error of at most 0.014.
Values may be sent and summed in bfloat16 or wider, within the bound.
No kernel may reach another device: no remote copies, remote signals or barrier semaphores. Data moves between devices by JAX's collectives and lax.ppermute only.
A program may use at most 128 MiB of HBM per device.

```python
import jax
import jax.numpy as jnp
from jax import lax

D = 2048
HEADS = 32
HEAD_DIM = 64
GROUPS = 4
STATE = 128
CONV = 3
BLOCK = 128
TOK_DEV = 128
CTX = 512
INNER = 2048
SEQ = 8192
BATCH = 2
N_TP = 4


def draw_latent(key, part):
    noise_key, dir_key, span_key, block_key = jax.random.split(key, 4)
    shape = (BATCH, SEQ, D)
    noise = jax.random.truncated_normal(noise_key, -4.0, 4.0, shape, jnp.float32)
    direction = jax.random.truncated_normal(dir_key, -3.0, 3.0, (D,), jnp.float32)
    coarse = jnp.repeat(jax.random.uniform(span_key, (BATCH, SEQ // TOK_DEV, 1), jnp.float32, -1.5, 1.5), TOK_DEV, axis=1)
    finer = jnp.repeat(jax.random.uniform(block_key, (BATCH, SEQ // BLOCK, 1), jnp.float32, -0.5, 0.5), BLOCK, axis=1)
    return (noise + (coarse + finer) * direction).astype(jnp.bfloat16)


def draw_decay_rate(key, part):
    slow_key, fast_key, pick_key = jax.random.split(key, 3)
    chain = SEQ + CTX
    slow_rate = jax.random.uniform(slow_key, (2, HEADS), jnp.float32, 0.6, 2.0) / chain
    fast_rate = jax.random.uniform(fast_key, (2, HEADS), jnp.float32, 0.015, 0.04)
    picked = jax.random.uniform(pick_key, (2, HEADS), jnp.float32) < 0.25
    return jnp.where(picked, fast_rate, slow_rate)


def levels(rng, shape, cuts, smallest, top_value):
    def one(axis_at, blocks):
        steps = jax.random.uniform(jax.random.fold_in(jax.random.fold_in(rng, 6), axis_at), (blocks,), jnp.float32, smallest / len(cuts), top_value / len(cuts))
        return jnp.repeat(jnp.exp(steps), shape[axis_at] // blocks).reshape((-1,) + (1,) * (len(shape) - axis_at - 1))

    loudness = one(*cuts[0])
    for cut in cuts[1:]:
        loudness = loudness * one(*cut)
    return loudness


def gaussian(rng, shape, scale, limit, cuts=(), held_as=jnp.bfloat16):
    values = jax.random.normal(rng, shape, jnp.float32) * scale
    if len(cuts) > 0:
        values = levels(rng, shape, cuts, -0.22, 0.18) * values
    return jnp.clip(values, min=-limit, max=limit).astype(held_as)


def setup_inputs(seed: int = 0) -> dict:
    key_of = jax.random.split(jax.random.key(seed), 18)
    latent = draw_latent(jax.random.fold_in(key_of[17], 71), 0)
    condition = gaussian(key_of[1], (BATCH, D), 1.0, 6.0, ((0, 2),))
    context = gaussian(key_of[2], (BATCH, CTX, D), 1.0, 6.0, ((0, 2), (1, 64)))
    context_source = gaussian(key_of[3], (D,), 1.0, 6.0)
    mod_weight = gaussian(key_of[4], (3, D, D), D ** -0.5, 0.125, ((1, 64), (2, 4)))
    norm_gain = jnp.clip(1.0 + 0.18 * jax.random.normal(key_of[5], (D,), jnp.float32), 0.099609375, 1.8984375).astype(jnp.bfloat16)
    w_x = gaussian(key_of[6], (D, INNER), D ** -0.5, 0.125, ((0, 2), (1, 4)))
    w_b = gaussian(key_of[7], (D, GROUPS * STATE), D ** -0.5, 0.125, ((0, 2), (1, 4)))
    w_c = gaussian(key_of[8], (D, GROUPS * STATE), D ** -0.5, 0.125, ((0, 2), (1, 4)))
    w_z = gaussian(key_of[9], (D, INNER), D ** -0.5, 0.125, ((0, 2), (1, 4)))
    w_dt = gaussian(key_of[10], (2, D, HEADS), D ** -0.5, 0.125, ((1, 2), (2, 4)))
    conv_x = gaussian(key_of[11], (CONV, INNER), CONV ** -0.5, 3.5, ((1, 4),))
    conv_b = gaussian(key_of[12], (CONV, GROUPS * STATE), CONV ** -0.5, 3.5, ((1, 4),))
    conv_c = gaussian(key_of[13], (CONV, GROUPS * STATE), CONV ** -0.5, 3.5, ((1, 4),))
    decay_rate = draw_decay_rate(jax.random.fold_in(key_of[17], 71), 0)
    out_gain = jnp.clip(1.0 + 0.18 * jax.random.normal(key_of[15], (INNER,), jnp.float32), 0.099609375, 1.8984375).astype(jnp.bfloat16)
    w_out = gaussian(key_of[16], (INNER, D), INNER ** -0.5, 0.125, ((0, 8),))
    return dict(latent=latent, condition=condition, context=context, context_source=context_source, mod_weight=mod_weight, norm_gain=norm_gain, w_x=w_x, w_b=w_b, w_c=w_c, w_z=w_z, w_dt=w_dt, conv_x=conv_x, conv_b=conv_b, conv_c=conv_c, decay_rate=decay_rate, out_gain=out_gain, w_out=w_out)


EPSILON = 1e-06

def rounded(values):
    return lax.optimization_barrier(values.astype(jnp.bfloat16)).astype(jnp.float32)

def modulated(source, gain_vec, shift_vec, scale_vec):
    values = source.astype(jnp.float32)
    normed = values * lax.rsqrt(lax.optimization_barrier(jnp.mean(values * values, axis=-1, keepdims=True)) + EPSILON)
    return (normed * gain_vec.astype(jnp.float32) * (1.0 + scale_vec) + shift_vec).astype(jnp.bfloat16)

def project(source, weight):
    return jnp.dot(source, weight, preferred_element_type=jnp.float32).astype(jnp.bfloat16)

def centred_conv(source, weight):
    total_rows = source.shape[0]
    reach_rows = weight.shape[0] // 2
    padded = jnp.pad(source.astype(jnp.float32), ((reach_rows, reach_rows), (0, 0)))
    tap_weights = weight.astype(jnp.float32)
    summed = jnp.zeros(source.shape, jnp.float32)
    for offset in range(weight.shape[0]):
        summed = summed + padded[offset:offset + total_rows] * tap_weights[offset]
    return jax.nn.silu(summed).astype(jnp.bfloat16)

def final_state(x_vals, b_vals, step_size, rate_head):
    total_rows, head_count = step_size.shape
    per_group = head_count // GROUPS
    moved_x = rounded(x_vals.reshape(total_rows, head_count, HEAD_DIM).astype(jnp.float32) * step_size[:, :, None])
    running = jnp.cumsum(-rate_head * step_size, axis=0)
    weight = jnp.exp(running[-1:] - running)
    scaled = (moved_x * weight[:, :, None]).reshape(total_rows, GROUPS, per_group, HEAD_DIM)
    b_wide = b_vals.reshape(total_rows, GROUPS, STATE).astype(jnp.float32)
    return jnp.einsum('sgn,sghp->ghpn', b_wide, scaled, precision=lax.Precision.HIGHEST)

def ssd_direction(x_vals, b_vals, c_vals, step_size, rate_head, start_state):
    total_rows, head_count = step_size.shape
    per_group = head_count // GROUPS
    blocks = total_rows // BLOCK
    moved_x = rounded(x_vals.reshape(total_rows, head_count, HEAD_DIM).astype(jnp.float32) * step_size[:, :, None])
    decay_log = -rate_head * step_size
    lower_part = jnp.arange(BLOCK)[:, None] >= jnp.arange(BLOCK)[None, :]

    def advance(carried_in, inputs):
        x_block, b_block, c_block, d_block = inputs
        running = jnp.cumsum(d_block, axis=0)
        across = running.T
        spread = across[:, :, None] - across[:, None, :]
        decay_mask = jnp.where(lower_part, jnp.exp(jnp.minimum(spread, 0.0)), 0.0).reshape(GROUPS, per_group, BLOCK, BLOCK)
        b_wide = b_block.astype(jnp.float32)
        c_wide = c_block.astype(jnp.float32)
        scores = jnp.einsum('lgn,sgn->gls', c_wide, b_wide)
        weights = rounded(scores[:, None] * decay_mask)
        x_group = x_block.reshape(BLOCK, GROUPS, per_group, HEAD_DIM)
        inside = jnp.einsum('ghls,sghp->lghp', weights, x_group)
        carried = jnp.einsum('lgn,ghpn->lghp', c_wide, rounded(carried_in))
        growth = jnp.exp(running).reshape(BLOCK, GROUPS, per_group, 1)
        to_end = jnp.exp(running[-1:] - running).reshape(BLOCK, GROUPS, per_group, 1)
        fresh_state = jnp.einsum('sgn,sghp->ghpn', b_wide, rounded(x_group * to_end))
        ending = carried_in * jnp.exp(running[-1]).reshape(GROUPS, per_group, 1, 1) + fresh_state
        return (ending, inside + growth * carried)
    _, outputs = lax.scan(advance, start_state, (moved_x.reshape(blocks, BLOCK, head_count, HEAD_DIM), b_vals.reshape(blocks, BLOCK, GROUPS, STATE), c_vals.reshape(blocks, BLOCK, GROUPS, STATE), decay_log.reshape(blocks, BLOCK, head_count)))
    return outputs.reshape(total_rows, head_count * HEAD_DIM)

def reference(latent, condition, context, context_source, mod_weight, norm_gain, w_x, w_b, w_c, w_z, w_dt, conv_x, conv_b, conv_c, decay_rate, out_gain, w_out):
    activation = rounded(jax.nn.silu(condition.astype(jnp.float32)))
    source_act = rounded(jax.nn.silu(context_source.astype(jnp.float32)))
    weight_wide = mod_weight.astype(jnp.float32)
    mod_latent = jnp.einsum('bd,kdc->kbc', activation, weight_wide)
    mod_context = jnp.einsum('d,kdc->kc', source_act, weight_wide)
    part_width = INNER // N_TP
    outputs = []
    for sample in range(latent.shape[0]):
        ctx_rows = modulated(context[sample], norm_gain, mod_context[0], mod_context[1])
        ctx_x = centred_conv(project(ctx_rows, w_x), conv_x)
        ctx_b = centred_conv(project(ctx_rows, w_b), conv_b)
        ctx_fwd = jax.nn.softplus(project(ctx_rows, w_dt[0]).astype(jnp.float32))
        ctx_bwd = jax.nn.softplus(project(ctx_rows, w_dt[1]).astype(jnp.float32))
        state_fwd = final_state(ctx_x, ctx_b, ctx_fwd, decay_rate[0])
        state_bwd = final_state(jnp.flip(ctx_x, 0), jnp.flip(ctx_b, 0), jnp.flip(ctx_bwd, 0), decay_rate[1])
        latent_rows = modulated(latent[sample], norm_gain, mod_latent[0, sample], mod_latent[1, sample])
        x_vals = centred_conv(project(latent_rows, w_x), conv_x)
        b_vals = centred_conv(project(latent_rows, w_b), conv_b)
        c_vals = centred_conv(project(latent_rows, w_c), conv_c)
        step_fwd = jax.nn.softplus(project(latent_rows, w_dt[0]).astype(jnp.float32))
        step_bwd = jax.nn.softplus(project(latent_rows, w_dt[1]).astype(jnp.float32))
        gate_in = project(latent_rows, w_z)
        total_rows = latent_rows.shape[0]
        out_fwd = ssd_direction(x_vals, b_vals, c_vals, step_fwd, decay_rate[0], state_fwd)
        out_bwd = jnp.flip(ssd_direction(jnp.flip(x_vals, 0), jnp.flip(b_vals, 0), jnp.flip(c_vals, 0), jnp.flip(step_bwd, 0), decay_rate[1], state_bwd), 0)
        gated = (out_fwd + out_bwd) * jax.nn.silu(gate_in.astype(jnp.float32))
        grouped = gated.reshape(total_rows, GROUPS, -1)
        normed = grouped * lax.rsqrt(lax.optimization_barrier(jnp.mean(grouped * grouped, axis=-1, keepdims=True)) + EPSILON) * out_gain.reshape(GROUPS, -1).astype(jnp.float32)
        normed_out = normed.reshape(total_rows, -1).astype(jnp.bfloat16)
        mixed = jnp.zeros((total_rows, w_out.shape[1]), jnp.float32)
        for part_idx in range(N_TP):
            lower_col = part_idx * part_width
            term = jnp.dot(normed_out[:, lower_col:lower_col + part_width], w_out[lower_col:lower_col + part_width], preferred_element_type=jnp.float32)
            mixed = mixed + rounded(term)
        outputs.append((mod_latent[2, sample] * mixed).astype(jnp.bfloat16))
    return jnp.stack(outputs)
```

```python
import functools

import jax
import jax.numpy as jnp
from jax import lax
from jax.experimental import pallas as pl
from jax.experimental.pallas import tpu as pltpu
from jax.sharding import Mesh
from jax.sharding import PartitionSpec as P

SP = ("sp_0", "sp_1")
ALL = ("sp_0", "sp_1", "tp")
EPSILON = 1e-06
INTERPRET = False

D = 2048
HALF = D // 2
TOK = 128
OWN = 32
INNER = 512
HEADS = 8
HD = 64
STATE = 128
NSP = 64
CTX_DEV = 8
CTX = NSP * CTX_DEV
XB = INNER + STATE
XBC = INNER + 2 * STATE
COLS = XBC + INNER + 128
ROWS = TOK + 16

f32 = jnp.float32
bf16 = jnp.bfloat16
HIGHEST = lax.Precision.HIGHEST


def silu(v):
    return v / (1.0 + jnp.exp(-v))


def softplus(v):
    return jnp.maximum(v, 0.0) + jnp.log1p(jnp.exp(-jnp.abs(v)))


def rounded(v):
    return v.astype(bf16).astype(f32)


def lanes(shape):
    return lax.broadcasted_iota(jnp.int32, shape, 1)


def rows_of(shape):
    return lax.broadcasted_iota(jnp.int32, shape, 0)


def per_channel(table, first, chunk):
    left = table[:, first + 2 * chunk : first + 2 * chunk + 1]
    right = table[:, first + 2 * chunk + 1 : first + 2 * chunk + 2]
    shape = (table.shape[0], 128)
    return jnp.where(lanes(shape) < HD, left, right)


def project_kernel(
    place_ref, lat_ref, gain_ref, mod_ref, own_ref, other_ref, tap_ref, rate_ref,
    send_ref, x_ref, b_ref, c_ref, z_ref, step_ref, run_ref, gate_ref,
    h_ref, conv_ref,
):
    core = place_ref[0]
    at = place_ref[1]
    mods = []
    for t in range(4):
        total = mod_ref[t]
        for y in range(1, 8):
            total = total + mod_ref[4 * y + t]
        mods.append(total)
    squares = jnp.zeros((ROWS, 128), f32)
    for c in range(16):
        v = lat_ref[:, c * 128 : (c + 1) * 128].astype(f32)
        squares = squares + v * v
    inv = lax.rsqrt(jnp.sum(squares, axis=1, keepdims=True) * (1.0 / D) + EPSILON)
    inv_main, inv_ctx = inv[: ROWS - 8], inv[ROWS - 8 :]
    for c in range(16):
        t, q = c // 4, c % 4
        cols = slice(c * 128, (c + 1) * 128)
        v = lat_ref[:, cols].astype(f32)
        gain = gain_ref[0:1, cols].astype(f32)
        shift, scale = mods[t][q : q + 1], mods[t][4 + q : 5 + q]
        cshift, cscale = mods[t][8 + q : 9 + q], mods[t][12 + q : 13 + q]
        gate_ref[0:1, cols] = mods[t][16 + q : 17 + q]
        main = v[: ROWS - 8] * inv_main * gain * (1.0 + scale) + shift
        ctx = v[ROWS - 8 :] * inv_ctx * gain * (1.0 + cscale) + cshift
        h_ref[0:TOK, cols] = main[:TOK].astype(bf16)
        h_ref[TOK:ROWS, cols] = jnp.concatenate([main[TOK:], ctx], axis=0).astype(bf16)
    mine = pl.multiple_of(core * HALF, HALF)
    theirs = pl.multiple_of((1 - core) * HALF, HALF)

    def project(first, width):
        cols = slice(first, first + width)
        out = jnp.dot(h_ref[:, pl.ds(mine, HALF)], own_ref[:, cols], preferred_element_type=f32)
        out = out + jnp.dot(
            h_ref[:, pl.ds(theirs, HALF)], other_ref[:, cols], preferred_element_type=f32
        )
        return rounded(out)

    dt = project(XBC + INNER, 128)
    step = softplus(dt[:TOK])
    step_ref[...] = step
    log_decay = -(rate_ref[0:1, :] * step)
    ri, ci = rows_of((TOK, TOK)), lanes((TOK, TOK))
    lower = jnp.where(ri >= ci, 1.0, 0.0).astype(f32)
    upper = jnp.where(ri <= ci, 1.0, 0.0).astype(f32)
    ahead = jnp.dot(lower, log_decay, preferred_element_type=f32, precision=HIGHEST)
    behind = jnp.dot(upper, log_decay, preferred_element_type=f32, precision=HIGHEST)
    run = jnp.where(ci < HEADS, ahead, behind)
    run_ref[...] = run
    total = jnp.where(lanes((1, 128)) < HEADS, run[TOK - 1 : TOK], run[0:1])
    to_end = jnp.exp(total - run)

    before_ok = jnp.where(at > 0, 1.0, 0.0)
    after_ok = jnp.where(at < NSP - 1, 1.0, 0.0)

    def convolved(first, width):
        cols = slice(first, first + width)
        p = project(first, width)
        conv_ref[8 : 8 + TOK, cols] = p[:TOK]
        conv_ref[0:8, cols] = jnp.broadcast_to(p[TOK : TOK + 1] * before_ok, (8, width))
        conv_ref[8 + TOK : 16 + TOK, cols] = jnp.broadcast_to(
            p[TOK + 1 : TOK + 2] * after_ok, (8, width)
        )
        summed = (
            conv_ref[7 : 7 + TOK, cols] * tap_ref[0:1, cols]
            + conv_ref[8 : 8 + TOK, cols] * tap_ref[1:2, cols]
            + conv_ref[9 : 9 + TOK, cols] * tap_ref[2:3, cols]
        )
        return silu(summed).astype(bf16), p[TOK + 8 :]

    b_in, ctx_b = convolved(INNER, STATE)
    b_ref[...] = b_in
    x_in, ctx_x = convolved(0, INNER)
    x_ref[...] = x_in

    states = []
    for first in (0, HEADS):
        parts = []
        for q in range(4):
            moved = rounded(x_in[:, q * 128 : (q + 1) * 128].astype(f32) * per_channel(step, first, q))
            parts.append((moved * per_channel(to_end, first, q)).astype(bf16))
        states.append(
            lax.dot_general(
                jnp.concatenate(parts, axis=1), b_in, (((0,), (0,)), ((), ())),
                preferred_element_type=f32,
            ).reshape(NSP, 8, STATE)
        )
    send_ref[:, 0:16, :] = jnp.concatenate(states, axis=1).astype(bf16)

    ctx_dt = dt[TOK + 8 :]
    high = rounded(total)
    low = rounded(total - high)
    lane = lanes((8, 128))
    blocks = []
    for head in range(HEADS):
        misc = jnp.zeros((8, 128), f32)
        for spot, table, col in (
            (8, ctx_dt, head), (9, ctx_dt, HEADS + head), (10, high, head), (11, low, head),
            (12, high, HEADS + head), (13, low, HEADS + head),
        ):
            misc = jnp.where(lane == spot, table[:, col : col + 1], misc)
        for k in range(8):
            j = head * 8 + k
            chunk = ctx_x[:, (j // 16) * 128 : (j // 16 + 1) * 128]
            shift = (128 - 8 * (j % 16)) % 128
            if shift:
                chunk = pltpu.roll(chunk, shift, 1)
            blocks.append(jnp.concatenate([ctx_b, jnp.where(lane < 8, chunk, misc)], axis=0))
    for j in range(NSP):
        send_ref[j, 16:32, :] = blocks[j].astype(bf16)

    c_in, _ = convolved(XB, STATE)
    c_ref[...] = c_in
    z_ref[...] = project(XBC, INNER)[:TOK].astype(bf16)


def inside_kernel(x_ref, b_ref, c_ref, step_ref, run_ref, y_ref):
    step, run = step_ref[...], run_ref[...]
    turned = run.T
    scores = lax.dot_general(
        c_ref[...], b_ref[...], (((1,), (1,)), ((), ())), preferred_element_type=f32
    )
    ri, ci = rows_of((TOK, TOK)), lanes((TOK, TOK))
    for q in range(4):
        cols = slice(q * 128, (q + 1) * 128)
        x = x_ref[:, cols].astype(f32)
        moved = jnp.concatenate(
            [(x * per_channel(step, first, q)).astype(bf16) for first in (0, HEADS)], axis=0
        )
        outs = []
        for head in (2 * q, 2 * q + 1):
            weights = []
            for first, kept in ((0, ri >= ci), (HEADS, ri <= ci)):
                k = first + head
                spread = run[:, k : k + 1] - turned[k : k + 1, :]
                decay = jnp.where(kept, jnp.exp(jnp.minimum(spread, 0.0)), 0.0)
                weights.append((scores * decay).astype(bf16))
            outs.append(
                jnp.dot(jnp.concatenate(weights, axis=1), moved, preferred_element_type=f32)
            )
        y_ref[:, cols] = jnp.where(ci < HD, outs[0], outs[1])


def owner_kernel(rate_ref, recv_ref, tap_b_ref, tap_x_ref, out_ref, pad_ref, held_ref):
    def conv(values, tap_ref):
        pad_ref[0:8, :] = jnp.zeros((8, 128), f32)
        pad_ref[8 + CTX : 16 + CTX, :] = jnp.zeros((8, 128), f32)
        pad_ref[8 : 8 + CTX, :] = values
        summed = (
            pad_ref[7 : 7 + CTX, :] * tap_ref[0:1, :]
            + values * tap_ref[1:2, :]
            + pad_ref[9 : 9 + CTX, :] * tap_ref[2:3, :]
        )
        return silu(summed)

    both = recv_ref[:, 16:32, :].astype(f32)
    raw_b = both[:, 0:8, :].reshape(CTX, 128)
    misc = both[:, 8:16, :].reshape(CTX, 128)
    ctx_b = conv(raw_b, tap_b_ref).astype(bf16)
    ctx_x = rounded(conv(misc, tap_x_ref))
    step = softplus(misc)
    lane = lanes((CTX, 128))
    decay = -jnp.where(lane == 8, rate_ref[0] * step, rate_ref[1] * step)
    wide = jnp.where(lane < HD, decay[:, 8:9], decay[:, 9:10])
    high = rounded(wide)
    mid = rounded(wide - high)
    low = rounded(wide - high - mid)
    spot = lane % 4
    parts = jnp.where(spot == 0, high, jnp.where(spot == 1, mid, jnp.where(spot == 2, low, 0.0)))
    parts = parts.astype(bf16)
    ri, ci = rows_of((CTX, CTX)), lanes((CTX, CTX))
    later = jnp.where(ci > ri, 1.0, 0.0).astype(bf16)
    earlier = jnp.where(ci < ri, 1.0, 0.0).astype(bf16)
    fsum = jnp.dot(later, parts, preferred_element_type=f32)
    bsum = jnp.dot(earlier, parts, preferred_element_type=f32)
    wf = jnp.exp(fsum[:, 0:1] + fsum[:, 1:2] + fsum[:, 2:3])
    wb = jnp.exp(bsum[:, 64:65] + bsum[:, 65:66] + bsum[:, 66:67])
    xf = rounded(ctx_x * step[:, 8:9]) * wf
    xb = rounded(ctx_x * step[:, 9:10]) * wb
    x16 = jnp.where(lane < 8, xf, pltpu.roll(xb, 8, 1))
    x_high = rounded(x16)
    x_low = x16 - x_high
    x32 = jnp.where(lane < 16, x_high, jnp.where(lane < 32, pltpu.roll(x_low, 16, 1), 0.0))
    start = lax.dot_general(
        x32.astype(bf16), ctx_b, (((0,), (0,)), ((), ())), preferred_element_type=f32
    )
    ahead = start[0:8] + start[16:24]
    behind = start[8:16] + start[24:32]
    grow_f = jnp.exp(jnp.broadcast_to(misc[:, 10:11] + misc[:, 11:12], (CTX, 128))).reshape(
        NSP, 8, 128
    )
    grow_b = jnp.exp(jnp.broadcast_to(misc[:, 12:13] + misc[:, 13:14], (CTX, 128))).reshape(
        NSP, 8, 128
    )
    fresh = recv_ref[:, 0:16, :].astype(f32)
    for k in range(NSP):
        m = NSP - 1 - k
        held_ref[k, 0:8, :] = ahead
        held_ref[m, 8:16, :] = behind
        ahead = ahead * grow_f[k] + fresh[k, 0:8]
        behind = behind * grow_b[m] + fresh[m, 8:16]
    out_ref[...] = held_ref[...].astype(bf16)


def output_kernel(
    place_ref, state_ref, c_ref, y_ref, run_ref, z_ref, gain_ref, own_ref, other_ref,
    out_ref, ny_ref,
):
    core = place_ref[0]
    states = state_ref[...].astype(f32)
    growth = jnp.exp(run_ref[...])
    c_in = c_ref[...]
    ahead = states[:, 0:8, :].reshape(INNER, STATE).astype(bf16)
    behind = states[:, 8:16, :].reshape(INNER, STATE).astype(bf16)
    dims = (((1,), (1,)), ((), ()))
    carried_f = lax.dot_general(c_in, ahead, dims, preferred_element_type=f32)
    carried_b = lax.dot_general(c_in, behind, dims, preferred_element_type=f32)
    squares = jnp.zeros((TOK, 128), f32)
    gated = []
    for q in range(4):
        cols = slice(q * 128, (q + 1) * 128)
        y = (
            y_ref[:, cols]
            + per_channel(growth, 0, q) * carried_f[:, cols]
            + per_channel(growth, HEADS, q) * carried_b[:, cols]
        )
        g = y * silu(z_ref[:, cols].astype(f32))
        squares = squares + g * g
        gated.append(g)
    inv = lax.rsqrt(jnp.sum(squares, axis=1, keepdims=True) * (1.0 / INNER) + EPSILON)
    for q in range(4):
        cols = slice(q * 128, (q + 1) * 128)
        ny_ref[:, cols] = (gated[q] * inv * gain_ref[0:1, cols].astype(f32)).astype(bf16)
    half = INNER // 2
    mine = ny_ref[:, pl.ds(pl.multiple_of(core * half, half), half)]
    theirs = ny_ref[:, pl.ds(pl.multiple_of((1 - core) * half, half), half)]
    for n in range(4):
        cols = slice(n * 512, (n + 1) * 512)
        out = jnp.dot(mine, own_ref[:, cols], preferred_element_type=f32)
        out = out + jnp.dot(theirs, other_ref[:, cols], preferred_element_type=f32)
        out_ref[:, cols] = out.astype(bf16)


def call(kernel, out_shape, n_args, smem, scratch=(), flops=10**8, name=None):
    vmem = pl.BlockSpec(memory_space=pltpu.VMEM)
    in_specs = [pl.BlockSpec(memory_space=pltpu.SMEM) if i in smem else vmem for i in range(n_args)]
    many = isinstance(out_shape, (list, tuple))
    return pl.pallas_call(
        kernel,
        out_shape=out_shape,
        in_specs=in_specs,
        out_specs=[vmem] * len(out_shape) if many else vmem,
        scratch_shapes=list(scratch),
        compiler_params=pltpu.CompilerParams(vmem_limit_bytes=30 * 2**20),
        cost_estimate=pl.CostEstimate(flops=flops, bytes_accessed=2**20, transcendentals=0),
        interpret=INTERPRET,
        name=name,
    )


def project_call(*args):
    shape = jax.ShapeDtypeStruct
    return call(
        project_kernel,
        [
            shape((NSP, 32, 128), bf16),
            shape((TOK, INNER), bf16),
            shape((TOK, STATE), bf16),
            shape((TOK, STATE), bf16),
            shape((TOK, INNER), bf16),
            shape((TOK, 128), f32),
            shape((TOK, 128), f32),
            shape((1, D), f32),
        ],
        8,
        (0,),
        [pltpu.VMEM((ROWS, D), bf16), pltpu.VMEM((TOK + 16, XBC), f32)],
        name="project",
    )(*args)


def inside_call(*args):
    return call(inside_kernel, jax.ShapeDtypeStruct((TOK, INNER), f32), 5, (), name="inside")(*args)


def owner_call(*args):
    return call(
        owner_kernel,
        jax.ShapeDtypeStruct((NSP, 16, 128), bf16),
        4,
        (0,),
        [pltpu.VMEM((CTX + 16, 128), f32), pltpu.VMEM((NSP, 16, 128), f32)],
        name="owner",
    )(*args)


def output_call(*args):
    return call(
        output_kernel,
        jax.ShapeDtypeStruct((TOK, D), bf16),
        9,
        (0,),
        [pltpu.VMEM((TOK, INNER), bf16)],
        name="output",
    )(*args)


def swapped(x):
    return lax.ppermute(x, "dp", [(0, 1), (1, 0)])


def exchanged(x, axes):
    return lax.all_to_all(x, axes, 0, 0, tiled=True)


def sent_to_all(x, peers, axes):
    return exchanged(jnp.broadcast_to(x[None], (peers, *x.shape)), axes)


def joined_weights(w_x, w_b, w_c, w_z, w_dt):
    steps = jnp.concatenate([w_dt[0], w_dt[1]], axis=1)
    steps = jnp.pad(steps, ((0, 0), (0, 128 - steps.shape[1])))
    return jnp.concatenate([w_x, w_b, w_c, w_z, steps], axis=1)


def owner_taps(conv_x, conv_b, at):
    own = lax.dynamic_slice_in_dim(conv_x, at * 8, 8, 1)
    tap_x = jnp.pad(own.astype(f32), ((0, 0), (0, 120)))
    return conv_b.astype(f32), tap_x


def shards(
    latent, condition, context, context_source, mod_weight, norm_gain,
    w_x, w_b, w_c, w_z, w_dt, conv_x, conv_b, conv_c, decay_rate, out_gain, w_out,
):
    at = lax.axis_index(SP)
    core = lax.axis_index("dp")
    place = jnp.stack([core, at]).astype(jnp.int32)
    row_count = mod_weight.shape[1]

    act = jnp.stack(
        [silu(condition[0].astype(f32)), silu(context_source.astype(f32))]
    ).astype(bf16)
    act = lax.dynamic_slice_in_dim(act, at * row_count, row_count, 1)
    part = jnp.einsum("ar,krc->akc", act, mod_weight, preferred_element_type=f32)
    part = jnp.stack([part[0, 0], part[0, 1], part[1, 0], part[1, 1], part[0, 2]])
    part = part.reshape(20, 128)
    part = jnp.sum(sent_to_all(part, 8, "sp_0"), axis=0)
    mods = sent_to_all(part, 32, ("sp_1", "tp"))

    rows = latent[0]
    tp = lax.axis_index("tp")
    edge = jnp.where(tp == 3, rows[OWN - 1 :], rows[:1])
    pairs = [(4 * i + 3, 4 * i + 4) for i in range(NSP - 1)]
    pairs += [(j, i) for i, j in pairs]
    halo = lax.ppermute(edge, ALL, pairs)
    packed = jnp.concatenate([rows, jnp.pad(halo, ((0, 7), (0, 0)))], axis=0)
    block = sent_to_all(packed, 4, "tp")
    all_rows = jnp.concatenate(
        [
            block[:, :OWN].reshape(TOK, D),
            block[0, OWN : OWN + 1],
            block[3, OWN : OWN + 1],
            jnp.zeros((6, D), bf16),
            context[0],
        ],
        axis=0,
    )

    weights = joined_weights(w_x, w_b, w_c, w_z, w_dt)
    other_weights = swapped(weights)
    other_out = swapped(w_out)

    taps = jnp.concatenate([conv_x, conv_b, conv_c], axis=1).astype(f32)
    rates = jnp.pad(decay_rate.reshape(1, 2 * HEADS), ((0, 0), (0, 128 - 2 * HEADS)))
    tap_b, tap_x = owner_taps(conv_x, conv_b, at)
    own_rates = lax.dynamic_slice_in_dim(decay_rate, at // 8, 1, 1)[:, 0]

    send, x_in, b_in, c_in, z_in, step, run, gate = project_call(
        place, all_rows, norm_gain[None], mods, weights, other_weights, taps, rates
    )
    received = exchanged(send, SP)
    y_in = inside_call(x_in, b_in, c_in, step, run)
    states = exchanged(owner_call(own_rates, received, tap_b, tap_x), SP)
    partial = output_call(
        place, states, c_in, y_in, run, z_in, out_gain[None], w_out, other_out
    )
    tiles = exchanged(partial.reshape(4, OWN, D), "tp")
    mixed = jnp.sum(tiles.astype(f32), axis=0)
    return (gate * mixed).astype(bf16)[None]


def solution(mesh):
    torus = Mesh(
        mesh.devices.reshape(8, 8, mesh.shape["tp"], mesh.shape["dp"]), ("sp_0", "sp_1", "tp", "dp")
    )
    sp_tp = ("sp_0", "sp_1", "tp")
    placed = (
        P("dp", sp_tp, None),
        P("dp", None),
        P("dp", SP, None),
        P(),
        P(None, SP, "tp"),
        P(),
        P("dp", "tp"),
        P("dp", "tp"),
        P("dp", "tp"),
        P("dp", "tp"),
        P(None, "dp", "tp"),
        P(None, "tp"),
        P(None, "tp"),
        P(None, "tp"),
        P(None, "tp"),
        P("tp"),
        P(("tp", "dp"), None),
    )
    return jax.shard_map(
        shards, mesh=torus, in_specs=placed, out_specs=P("dp", sp_tp, None), check_vma=False
    )
```

```python
import jax
import jax.numpy as jnp
from jax import lax
from jax.experimental import pallas as pl
from jax.experimental.pallas import tpu as pltpu
from jax.sharding import Mesh
from jax.sharding import PartitionSpec as P


SP = ("sp_0", "sp_1")
ALL = ("sp_0", "sp_1", "tp")
EPSILON = 1e-06
INTERPRET = False

D = 2048
HALF = D // 2
TOK = 128
OWN = 32
INNER = 512
HEADS = 8
HD = 64
STATE = 128
NSP = 64
CTX_DEV = 8
CTX = NSP * CTX_DEV
XB = INNER + STATE
XBC = INNER + 2 * STATE
ROWS = TOK + 16

f32 = jnp.float32
bf16 = jnp.bfloat16
HIGHEST = lax.Precision.HIGHEST


def silu(v):
    return v / (1.0 + jnp.exp(-v))


def softplus(v):
    return jnp.maximum(v, 0.0) + jnp.log1p(jnp.exp(-jnp.abs(v)))


def rounded(v):
    return v.astype(bf16).astype(f32)


def lanes(shape):
    return lax.broadcasted_iota(jnp.int32, shape, 1)


def rows_of(shape):
    return lax.broadcasted_iota(jnp.int32, shape, 0)


def per_channel(table, first, chunk):
    left = table[:, first + 2 * chunk : first + 2 * chunk + 1]
    right = table[:, first + 2 * chunk + 1 : first + 2 * chunk + 2]
    shape = (table.shape[0], 128)
    return jnp.where(lanes(shape) < HD, left, right)


def softened(p, taps, first_col, conv_ref, before_ok, after_ok):
    width = p.shape[1]
    cols = slice(first_col, first_col + width)
    conv_ref[8 : 8 + TOK, :width] = p[:TOK]
    conv_ref[0:8, :width] = jnp.broadcast_to(p[TOK : TOK + 1] * before_ok, (8, width))
    conv_ref[8 + TOK : 16 + TOK, :width] = jnp.broadcast_to(
        p[TOK + 1 : TOK + 2] * after_ok, (8, width)
    )
    summed = (
        conv_ref[7 : 7 + TOK, :width] * taps[1:2, cols]
        + conv_ref[8 : 8 + TOK, :width] * taps[2:3, cols]
        + conv_ref[9 : 9 + TOK, :width] * taps[3:4, cols]
    )
    return silu(summed).astype(bf16)


def ends(at):
    return jnp.where(at > 0, 1.0, 0.0), jnp.where(at < NSP - 1, 1.0, 0.0)


def projected(h_ref, core, own_ref, other_ref, cols):
    mine = pl.multiple_of(core * HALF, HALF)
    theirs = pl.multiple_of((1 - core) * HALF, HALF)
    out = jnp.dot(h_ref[:, pl.ds(mine, HALF)], own_ref[:, cols], preferred_element_type=f32)
    return rounded(
        out
        + jnp.dot(h_ref[:, pl.ds(theirs, HALF)], other_ref[:, cols], preferred_element_type=f32)
    )


def project_kernel(
    place_ref, mod_ref, blk0_ref, blk1_ref, blk2_ref, blk3_ref, ctx_ref, misc_ref,
    own_x, other_x, own_s, other_s,
    send_hbm, h_hbm, xb_hbm, sr_hbm, gate_hbm,
    send_ref, h_ref, xb_ref, sr_ref, gate_ref, conv_ref, sems,
):
    def store(i, src, dst):
        copy = pltpu.make_async_copy(src, dst, sems.at[i])
        copy.start()
        return copy

    core, at, tp = place_ref[0], place_ref[1], place_ref[2]
    blocks = (blk0_ref, blk1_ref, blk2_ref, blk3_ref)
    origin = [lax.rem(tp + 4 - s, 4) for s in range(4)]
    is_first = [jnp.where(o == 0, 1.0, 0.0) for o in origin]
    is_last = [jnp.where(o == 3, 1.0, 0.0) for o in origin]
    mods = []
    for t in range(4):
        total = mod_ref[t]
        for y in range(1, 8):
            total = total + mod_ref[4 * y + t]
        mods.append(total)

    def inverse(ref):
        squares = jnp.zeros((ref.shape[0], 128), f32)
        for c in range(16):
            v = ref[:, c * 128 : (c + 1) * 128].astype(f32)
            squares = squares + v * v
        return lax.rsqrt(jnp.sum(squares, axis=1, keepdims=True) * (1.0 / D) + EPSILON)

    inv = [inverse(ref) for ref in blocks]
    inv_ctx = inverse(ctx_ref)
    row8 = rows_of((8, 128))
    for c in range(16):
        t, q = c // 4, c % 4
        cols = slice(c * 128, (c + 1) * 128)
        gain = misc_ref[0:1, cols]
        shift, scale = mods[t][q : q + 1], mods[t][4 + q : 5 + q]
        cshift, cscale = mods[t][8 + q : 9 + q], mods[t][12 + q : 13 + q]
        gate_ref[:, cols] = jnp.broadcast_to(mods[t][16 + q : 17 + q], (8, 128))
        before = jnp.zeros((8, 128), f32)
        after = jnp.zeros((8, 128), f32)
        for s in range(4):
            h = blocks[s][:, cols].astype(f32) * inv[s] * gain * (1.0 + scale) + shift
            h_ref[pl.ds(pl.multiple_of(origin[s] * OWN, OWN), OWN), cols] = h[:OWN].astype(bf16)
            before = before + h[OWN:] * is_first[s]
            after = after + h[OWN:] * is_last[s]
        halo = jnp.where(row8 == 0, before, pltpu.roll(after, 1, 0))
        ctx = ctx_ref[:, cols].astype(f32) * inv_ctx * gain * (1.0 + cscale) + cshift
        h_ref[TOK:ROWS, cols] = jnp.concatenate([halo, ctx], axis=0).astype(bf16)
    stores = [store(0, h_ref, h_hbm), store(1, gate_ref, gate_hbm)]

    p = projected(h_ref, core, own_s, other_s, slice(2 * STATE, 2 * STATE + 128))
    step = softplus(p[:TOK])
    ctx_dt = p[TOK + 8 :]
    log_decay = -(misc_ref[4:5, 0:128] * step)
    ri, ci = rows_of((TOK, TOK)), lanes((TOK, TOK))
    lower = jnp.where(ri >= ci, 1.0, 0.0).astype(f32)
    upper = jnp.where(ri <= ci, 1.0, 0.0).astype(f32)
    ahead = jnp.dot(lower, log_decay, preferred_element_type=f32, precision=HIGHEST)
    behind = jnp.dot(upper, log_decay, preferred_element_type=f32, precision=HIGHEST)
    run = jnp.where(ci < HEADS, ahead, behind)
    sr_ref[:, 0:128] = step
    sr_ref[:, 128:256] = run
    stores.append(store(2, sr_ref, sr_hbm))
    total = jnp.where(lanes((1, 128)) < HEADS, run[TOK - 1 : TOK], run[0:1])
    to_end = jnp.exp(total - run)

    before_ok, after_ok = ends(at)
    p = projected(h_ref, core, own_s, other_s, slice(0, STATE))
    ctx_b = p[TOK + 8 :]
    b_in = softened(p, misc_ref, INNER, conv_ref, before_ok, after_ok)
    xb_ref[:, INNER:] = b_in
    p = projected(h_ref, core, own_x, other_x, slice(0, INNER))
    ctx_x = p[TOK + 8 :]
    x_in = softened(p, misc_ref, 0, conv_ref, before_ok, after_ok)
    xb_ref[:, :INNER] = x_in
    stores.append(store(3, xb_ref, xb_hbm))

    states = []
    for first in (0, HEADS):
        parts = []
        for q in range(4):
            moved = rounded(x_in[:, q * 128 : (q + 1) * 128].astype(f32) * per_channel(step, first, q))
            parts.append((moved * per_channel(to_end, first, q)).astype(bf16))
        states.append(
            lax.dot_general(
                jnp.concatenate(parts, axis=1), b_in, (((0,), (0,)), ((), ())),
                preferred_element_type=f32,
            ).reshape(NSP, 8, STATE)
        )
    send_ref[:, 0:16, :] = jnp.concatenate(states, axis=1).astype(bf16)

    high = rounded(total)
    low = rounded(total - high)
    lane = lanes((8, 128))
    for head in range(HEADS):
        misc = jnp.zeros((8, 128), f32)
        for spot, table, col in (
            (8, ctx_dt, head), (9, ctx_dt, HEADS + head), (10, high, head), (11, low, head),
            (12, high, HEADS + head), (13, low, HEADS + head),
        ):
            misc = jnp.where(lane == spot, table[:, col : col + 1], misc)
        for k in range(8):
            j = head * 8 + k
            chunk = ctx_x[:, (j // 16) * 128 : (j // 16 + 1) * 128]
            shift = (128 - 8 * (j % 16)) % 128
            if shift:
                chunk = pltpu.roll(chunk, shift, 1)
            send_ref[j, 16:32, :] = jnp.concatenate(
                [ctx_b, jnp.where(lane < 8, chunk, misc)], axis=0
            ).astype(bf16)
    stores.append(store(4, send_ref, send_hbm))
    for copy in stores:
        copy.wait()


def inside_kernel(
    place_ref, h_ref, own_z, other_z, own_s, other_s, xb_ref, sr_ref, misc_ref,
    y_ref, c_out_ref, z_ref, conv_ref,
):
    core, at = place_ref[0], place_ref[1]
    before_ok, after_ok = ends(at)
    p = projected(h_ref, core, own_s, other_s, slice(STATE, 2 * STATE))
    c_in = softened(p, misc_ref, INNER + STATE, conv_ref, before_ok, after_ok)
    c_out_ref[...] = c_in
    z_ref[...] = projected(h_ref, core, own_z, other_z, slice(0, INNER))[:TOK].astype(bf16)
    step, run = sr_ref[:, 0:128], sr_ref[:, 128:256]
    turned = run.T
    scores = lax.dot_general(
        c_in, xb_ref[:, INNER:], (((1,), (1,)), ((), ())), preferred_element_type=f32
    )
    ri, ci = rows_of((TOK, TOK)), lanes((TOK, TOK))
    for q in range(4):
        cols = slice(q * 128, (q + 1) * 128)
        x = xb_ref[:, cols].astype(f32)
        moved = jnp.concatenate(
            [(x * per_channel(step, first, q)).astype(bf16) for first in (0, HEADS)], axis=0
        )
        outs = []
        for head in (2 * q, 2 * q + 1):
            weights = []
            for first, kept in ((0, ri >= ci), (HEADS, ri <= ci)):
                k = first + head
                spread = run[:, k : k + 1] - turned[k : k + 1, :]
                decay = jnp.where(kept, jnp.exp(jnp.minimum(spread, 0.0)), 0.0)
                weights.append((scores * decay).astype(bf16))
            outs.append(
                jnp.dot(jnp.concatenate(weights, axis=1), moved, preferred_element_type=f32)
            )
        y_ref[:, cols] = jnp.where(ci < HD, outs[0], outs[1])


def owner_kernel(rate_ref, recv_ref, tap_b_ref, tap_x_ref, out_ref, pad_ref, held_ref):
    def conv(values, tap_ref):
        pad_ref[0:8, :] = jnp.zeros((8, 128), f32)
        pad_ref[8 + CTX : 16 + CTX, :] = jnp.zeros((8, 128), f32)
        pad_ref[8 : 8 + CTX, :] = values
        summed = (
            pad_ref[7 : 7 + CTX, :] * tap_ref[0:1, :]
            + values * tap_ref[1:2, :]
            + pad_ref[9 : 9 + CTX, :] * tap_ref[2:3, :]
        )
        return silu(summed)

    both = recv_ref[:, 16:32, :].astype(f32)
    raw_b = both[:, 0:8, :].reshape(CTX, 128)
    misc = both[:, 8:16, :].reshape(CTX, 128)
    ctx_b = conv(raw_b, tap_b_ref).astype(bf16)
    ctx_x = rounded(conv(misc, tap_x_ref))
    step = softplus(misc)
    lane = lanes((CTX, 128))
    decay = -jnp.where(lane == 8, rate_ref[0] * step, rate_ref[1] * step)
    wide = jnp.where(lane < HD, decay[:, 8:9], decay[:, 9:10])
    high = rounded(wide)
    mid = rounded(wide - high)
    low = rounded(wide - high - mid)
    spot = lane % 4
    parts = jnp.where(spot == 0, high, jnp.where(spot == 1, mid, jnp.where(spot == 2, low, 0.0)))
    parts = parts.astype(bf16)
    ri, ci = rows_of((CTX, CTX)), lanes((CTX, CTX))
    later = jnp.where(ci > ri, 1.0, 0.0).astype(bf16)
    earlier = jnp.where(ci < ri, 1.0, 0.0).astype(bf16)
    fsum = jnp.dot(later, parts, preferred_element_type=f32)
    bsum = jnp.dot(earlier, parts, preferred_element_type=f32)
    wf = jnp.exp(fsum[:, 0:1] + fsum[:, 1:2] + fsum[:, 2:3])
    wb = jnp.exp(bsum[:, 64:65] + bsum[:, 65:66] + bsum[:, 66:67])
    xf = rounded(ctx_x * step[:, 8:9]) * wf
    xb = rounded(ctx_x * step[:, 9:10]) * wb
    x16 = jnp.where(lane < 8, xf, pltpu.roll(xb, 8, 1))
    x_high = rounded(x16)
    x_low = x16 - x_high
    x32 = jnp.where(lane < 16, x_high, jnp.where(lane < 32, pltpu.roll(x_low, 16, 1), 0.0))
    start = lax.dot_general(
        x32.astype(bf16), ctx_b, (((0,), (0,)), ((), ())), preferred_element_type=f32
    )
    ahead = start[0:8] + start[16:24]
    behind = start[8:16] + start[24:32]
    grow_f = jnp.exp(jnp.broadcast_to(misc[:, 10:11] + misc[:, 11:12], (CTX, 128))).reshape(
        NSP, 8, 128
    )
    grow_b = jnp.exp(jnp.broadcast_to(misc[:, 12:13] + misc[:, 13:14], (CTX, 128))).reshape(
        NSP, 8, 128
    )
    fresh = recv_ref[:, 0:16, :].astype(f32)
    for k in range(NSP):
        m = NSP - 1 - k
        held_ref[k, 0:8, :] = ahead
        held_ref[m, 8:16, :] = behind
        ahead = ahead * grow_f[k] + fresh[k, 0:8]
        behind = behind * grow_b[m] + fresh[m, 8:16]
    out_ref[...] = held_ref[...].astype(bf16)


def output_kernel(
    place_ref, state_ref, c_ref, y_ref, sr_ref, z_ref, gain_ref, own_ref, other_ref,
    out_ref, ny_ref,
):
    core = place_ref[0]
    states = state_ref[...].astype(f32)
    growth = jnp.exp(sr_ref[:, 128:256])
    c_in = c_ref[...]
    ahead = states[:, 0:8, :].reshape(INNER, STATE).astype(bf16)
    behind = states[:, 8:16, :].reshape(INNER, STATE).astype(bf16)
    dims = (((1,), (1,)), ((), ()))
    carried_f = lax.dot_general(c_in, ahead, dims, preferred_element_type=f32)
    carried_b = lax.dot_general(c_in, behind, dims, preferred_element_type=f32)
    squares = jnp.zeros((TOK, 128), f32)
    gated = []
    for q in range(4):
        cols = slice(q * 128, (q + 1) * 128)
        y = (
            y_ref[:, cols]
            + per_channel(growth, 0, q) * carried_f[:, cols]
            + per_channel(growth, HEADS, q) * carried_b[:, cols]
        )
        g = y * silu(z_ref[:, cols].astype(f32))
        squares = squares + g * g
        gated.append(g)
    inv = lax.rsqrt(jnp.sum(squares, axis=1, keepdims=True) * (1.0 / INNER) + EPSILON)
    for q in range(4):
        cols = slice(q * 128, (q + 1) * 128)
        ny_ref[:, cols] = (gated[q] * inv * gain_ref[0:1, cols].astype(f32)).astype(bf16)
    half = INNER // 2
    mine = ny_ref[:, pl.ds(pl.multiple_of(core * half, half), half)]
    theirs = ny_ref[:, pl.ds(pl.multiple_of((1 - core) * half, half), half)]
    for n in range(4):
        cols = slice(n * 512, (n + 1) * 512)
        out = jnp.dot(mine, own_ref[:, cols], preferred_element_type=f32)
        out = out + jnp.dot(theirs, other_ref[:, cols], preferred_element_type=f32)
        out_ref[:, cols] = out.astype(bf16)


def call(kernel, out_shape, n_args, smem, scratch=(), hbm=(), hbm_out=False, flops=10**8):
    space = {i: pltpu.SMEM for i in smem} | {i: pltpu.HBM for i in hbm}
    in_specs = [pl.BlockSpec(memory_space=space.get(i, pltpu.VMEM)) for i in range(n_args)]
    out = pl.BlockSpec(memory_space=pltpu.HBM if hbm_out else pltpu.VMEM)
    many = isinstance(out_shape, (list, tuple))
    return pl.pallas_call(
        kernel,
        out_shape=out_shape,
        in_specs=in_specs,
        out_specs=[out] * len(out_shape) if many else out,
        scratch_shapes=list(scratch),
        compiler_params=pltpu.CompilerParams(vmem_limit_bytes=30 * 2**20),
        cost_estimate=pl.CostEstimate(flops=flops, bytes_accessed=2**20, transcendentals=0),
        interpret=INTERPRET,
    )


def project_call(*args):
    outs = [
        ((NSP, 32, 128), bf16), ((ROWS, D), bf16), ((TOK, XB), bf16), ((TOK, 256), f32),
        ((8, D), f32),
    ]
    return call(
        project_kernel,
        [pltpu.HBM(*o) for o in outs],
        12,
        (0,),
        [
            *(pltpu.VMEM(*o) for o in outs),
            pltpu.VMEM((TOK + 16, INNER), f32),
            pltpu.SemaphoreType.DMA((5,)),
        ],
        hbm_out=True,
    )(*args)


def inside_call(*args):
    return call(
        inside_kernel,
        [
            jax.ShapeDtypeStruct((TOK, INNER), f32),
            jax.ShapeDtypeStruct((TOK, STATE), bf16),
            jax.ShapeDtypeStruct((TOK, INNER), bf16),
        ],
        9,
        (0,),
        [pltpu.VMEM((TOK + 16, STATE), f32)],
    )(*args)


def owner_call(*args):
    return call(
        owner_kernel,
        jax.ShapeDtypeStruct((NSP, 16, 128), bf16),
        4,
        (0,),
        [pltpu.VMEM((CTX + 16, 128), f32), pltpu.VMEM((NSP, 16, 128), f32)],
    )(*args)


def output_call(*args):
    return call(
        output_kernel,
        jax.ShapeDtypeStruct((TOK, D), bf16),
        9,
        (0,),
        [pltpu.VMEM((TOK, INNER), bf16)],
    )(*args)


def swapped(x):
    return lax.ppermute(x, "dp", [(0, 1), (1, 0)])


def exchanged(x, axes):
    return lax.all_to_all(x, axes, 0, 0, tiled=True)


def sent_to_all(x, peers, axes):
    return exchanged(jnp.broadcast_to(x[None], (peers, *x.shape)), axes)


def small_weights(w_b, w_c, w_dt):
    steps = jnp.concatenate([w_dt[0], w_dt[1]], axis=1)
    steps = jnp.pad(steps, ((0, 0), (0, 128 - steps.shape[1])))
    return jnp.concatenate([w_b, w_c, steps], axis=1)


def packed_vectors(norm_gain, conv_x, conv_b, conv_c, decay_rate):
    taps = jnp.concatenate([conv_x, conv_b, conv_c], axis=1).astype(f32)
    rates = decay_rate.reshape(1, 2 * HEADS)
    return jnp.concatenate(
        [
            norm_gain.astype(f32)[None],
            jnp.pad(taps, ((0, 0), (0, D - XBC))),
            jnp.pad(rates, ((0, 3), (0, D - 2 * HEADS))),
        ],
        axis=0,
    )


def owner_taps(conv_x, conv_b, at):
    own = lax.dynamic_slice_in_dim(conv_x, at * 8, 8, 1)
    tap_x = jnp.pad(own.astype(f32), ((0, 0), (0, 120)))
    return conv_b.astype(f32), tap_x


def shards(
    latent, condition, context, context_source, mod_weight, norm_gain,
    w_x, w_b, w_c, w_z, w_dt, conv_x, conv_b, conv_c, decay_rate, out_gain, w_out,
):
    at = lax.axis_index(SP)
    core = lax.axis_index("dp")
    tp = lax.axis_index("tp")
    place = jnp.stack([core, at, tp]).astype(jnp.int32)
    row_count = mod_weight.shape[1]

    rows = latent[0]
    edge = jnp.where(tp == 3, rows[OWN - 1 :], rows[:1])
    pairs = [(4 * i + 3, 4 * i + 4) for i in range(NSP - 1)]
    pairs += [(j, i) for i, j in pairs]
    halo = lax.ppermute(edge, ALL, pairs)

    act = jnp.stack(
        [silu(condition[0].astype(f32)), silu(context_source.astype(f32))]
    ).astype(bf16)
    act = lax.dynamic_slice_in_dim(act, at * row_count, row_count, 1)
    part = jnp.einsum("ar,krc->akc", act, mod_weight, preferred_element_type=f32)
    part = jnp.stack([part[0, 0], part[0, 1], part[1, 0], part[1, 1], part[0, 2]])
    part = part.reshape(20, 128)
    part = sent_to_all(part, 8, "sp_0")
    part = jnp.sum(part, axis=0)
    mods = sent_to_all(part, 32, ("sp_1", "tp"))

    packed = jnp.concatenate([rows, jnp.pad(halo, ((0, 7), (0, 0)))], axis=0)
    blocks = [packed]
    for s in (1, 2, 3):
        blocks.append(lax.ppermute(packed, "tp", [(i, (i + s) % 4) for i in range(4)]))

    small = small_weights(w_b, w_c, w_dt)
    other_x = swapped(w_x)
    other_small = swapped(small)
    other_z = swapped(w_z)
    other_out = swapped(w_out)

    misc = packed_vectors(norm_gain, conv_x, conv_b, conv_c, decay_rate)
    tap_b, tap_x = owner_taps(conv_x, conv_b, at)
    own_rates = lax.dynamic_slice_in_dim(decay_rate, at // 8, 1, 1)[:, 0]

    send, h, xb, sr, gate = project_call(
        place, mods, *blocks, context[0], misc, w_x, other_x, small, other_small
    )
    received = exchanged(send, SP)
    y_in, c_in, z_in = inside_call(
        place, h, w_z, other_z, small, other_small, xb, sr, misc
    )
    entering = owner_call(own_rates, received, tap_b, tap_x)
    states = exchanged(entering, SP)
    partial = output_call(
        place, states, c_in, y_in, sr, z_in, out_gain[None], w_out, other_out
    )
    tiles = exchanged(partial.reshape(4, OWN, D), "tp")
    mixed = jnp.sum(tiles.astype(f32), axis=0)
    return (gate[0:1] * mixed).astype(bf16)[None]


def solution(mesh):
    torus = Mesh(
        mesh.devices.reshape(8, 8, mesh.shape["tp"], mesh.shape["dp"]), ("sp_0", "sp_1", "tp", "dp")
    )
    sp_tp = ("sp_0", "sp_1", "tp")
    placed = (
        P("dp", sp_tp, None),
        P("dp", None),
        P("dp", SP, None),
        P(),
        P(None, SP, "tp"),
        P(),
        P("dp", "tp"),
        P("dp", "tp"),
        P("dp", "tp"),
        P("dp", "tp"),
        P(None, "dp", "tp"),
        P(None, "tp"),
        P(None, "tp"),
        P(None, "tp"),
        P(None, "tp"),
        P("tp"),
        P(("tp", "dp"), None),
    )

    return jax.shard_map(
        shards, mesh=torus, in_specs=placed, out_specs=P("dp", sp_tp, None), check_vma=False
    )
```

```python
import jax
import jax.numpy as jnp
from jax import lax
from jax.experimental import pallas as pl
from jax.experimental.pallas import tpu as pltpu
from jax.sharding import Mesh
from jax.sharding import PartitionSpec as P


SP = ("sp_0", "sp_1")
ALL = ("sp_0", "sp_1", "tp")
EPSILON = 1e-06
INTERPRET = False

D = 2048
HALF = D // 2
TOK = 128
OWN = 32
INNER = 512
HEADS = 8
HD = 64
STATE = 128
NSP = 64
CTX_DEV = 8
CTX = NSP * CTX_DEV
XB = INNER + STATE
XBC = INNER + 2 * STATE
ROWS = TOK + 16

f32 = jnp.float32
bf16 = jnp.bfloat16
HIGHEST = lax.Precision.HIGHEST


def silu(v):
    return v / (1.0 + jnp.exp(-v))


def softplus(v):
    return jnp.maximum(v, 0.0) + jnp.log1p(jnp.exp(-jnp.abs(v)))


def rounded(v):
    return v.astype(bf16).astype(f32)


def lanes(shape):
    return lax.broadcasted_iota(jnp.int32, shape, 1)


def rows_of(shape):
    return lax.broadcasted_iota(jnp.int32, shape, 0)


def per_channel(table, first, chunk):
    left = table[:, first + 2 * chunk : first + 2 * chunk + 1]
    right = table[:, first + 2 * chunk + 1 : first + 2 * chunk + 2]
    shape = (table.shape[0], 128)
    return jnp.where(lanes(shape) < HD, left, right)


def softened(p, taps, first_col, conv_ref, before_ok, after_ok):
    width = p.shape[1]
    cols = slice(first_col, first_col + width)
    conv_ref[8 : 8 + TOK, :width] = p[:TOK]
    conv_ref[0:8, :width] = jnp.broadcast_to(p[TOK : TOK + 1] * before_ok, (8, width))
    conv_ref[8 + TOK : 16 + TOK, :width] = jnp.broadcast_to(
        p[TOK + 1 : TOK + 2] * after_ok, (8, width)
    )
    summed = (
        conv_ref[7 : 7 + TOK, :width] * taps[1:2, cols]
        + conv_ref[8 : 8 + TOK, :width] * taps[2:3, cols]
        + conv_ref[9 : 9 + TOK, :width] * taps[3:4, cols]
    )
    return silu(summed).astype(bf16)


def ends(at):
    return jnp.where(at > 0, 1.0, 0.0), jnp.where(at < NSP - 1, 1.0, 0.0)


def projected(h_ref, core, own_ref, other_ref, cols):
    mine = pl.multiple_of(core * HALF, HALF)
    theirs = pl.multiple_of((1 - core) * HALF, HALF)
    out = jnp.dot(h_ref[:, pl.ds(mine, HALF)], own_ref[:, cols], preferred_element_type=f32)
    return rounded(
        out
        + jnp.dot(h_ref[:, pl.ds(theirs, HALF)], other_ref[:, cols], preferred_element_type=f32)
    )


def project_kernel(
    place_ref, mod_ref, blk0_ref, blk1_ref, blk2_ref, blk3_ref, ctx_ref, misc_ref,
    own_x, other_x, own_s, other_s,
    send_hbm, h_hbm, xb_hbm, sr_hbm, gate_hbm,
    send_ref, h_ref, xb_ref, sr_ref, gate_ref, conv_ref, sems,
):
    def store(i, src, dst):
        copy = pltpu.make_async_copy(src, dst, sems.at[i])
        copy.start()
        return copy

    core, at, tp = place_ref[0], place_ref[1], place_ref[2]
    blocks = (blk0_ref, blk1_ref, blk2_ref, blk3_ref)
    origin = [lax.rem(tp + 4 - s, 4) for s in range(4)]
    is_first = [jnp.where(o == 0, 1.0, 0.0) for o in origin]
    is_last = [jnp.where(o == 3, 1.0, 0.0) for o in origin]
    mods = []
    for t in range(4):
        total = mod_ref[t].astype(f32)
        for y in range(1, 8):
            total = total + mod_ref[4 * y + t].astype(f32)
        mods.append(total)

    def inverse(ref):
        squares = jnp.zeros((ref.shape[0], 128), f32)
        for c in range(16):
            v = ref[:, c * 128 : (c + 1) * 128].astype(f32)
            squares = squares + v * v
        return lax.rsqrt(jnp.sum(squares, axis=1, keepdims=True) * (1.0 / D) + EPSILON)

    inv = [inverse(ref) for ref in blocks]
    inv_ctx = inverse(ctx_ref)
    row8 = rows_of((8, 128))
    for c in range(16):
        t, q = c // 4, c % 4
        cols = slice(c * 128, (c + 1) * 128)
        gain = misc_ref[0:1, cols]
        shift, scale = mods[t][q : q + 1], mods[t][4 + q : 5 + q]
        cshift, cscale = mods[t][8 + q : 9 + q], mods[t][12 + q : 13 + q]
        gate_ref[:, cols] = jnp.broadcast_to(mods[t][16 + q : 17 + q], (8, 128))
        before = jnp.zeros((8, 128), f32)
        after = jnp.zeros((8, 128), f32)
        for s in range(4):
            h = blocks[s][:, cols].astype(f32) * inv[s] * gain * (1.0 + scale) + shift
            h_ref[pl.ds(pl.multiple_of(origin[s] * OWN, OWN), OWN), cols] = h[:OWN].astype(bf16)
            before = before + h[OWN:] * is_first[s]
            after = after + h[OWN:] * is_last[s]
        halo = jnp.where(row8 == 0, before, pltpu.roll(after, 1, 0))
        ctx = ctx_ref[:, cols].astype(f32) * inv_ctx * gain * (1.0 + cscale) + cshift
        h_ref[TOK:ROWS, cols] = jnp.concatenate([halo, ctx], axis=0).astype(bf16)
    stores = [store(0, h_ref, h_hbm), store(1, gate_ref, gate_hbm)]

    p = projected(h_ref, core, own_s, other_s, slice(2 * STATE, 2 * STATE + 128))
    step = softplus(p[:TOK])
    ctx_dt = p[TOK + 8 :]
    log_decay = -(misc_ref[4:5, 0:128] * step)
    ri, ci = rows_of((TOK, TOK)), lanes((TOK, TOK))
    lower = jnp.where(ri >= ci, 1.0, 0.0).astype(f32)
    upper = jnp.where(ri <= ci, 1.0, 0.0).astype(f32)
    ahead = jnp.dot(lower, log_decay, preferred_element_type=f32, precision=HIGHEST)
    behind = jnp.dot(upper, log_decay, preferred_element_type=f32, precision=HIGHEST)
    run = jnp.where(ci < HEADS, ahead, behind)
    sr_ref[:, 0:128] = step
    sr_ref[:, 128:256] = run
    stores.append(store(2, sr_ref, sr_hbm))
    total = jnp.where(lanes((1, 128)) < HEADS, run[TOK - 1 : TOK], run[0:1])
    to_end = jnp.exp(total - run)

    before_ok, after_ok = ends(at)
    p = projected(h_ref, core, own_s, other_s, slice(0, STATE))
    ctx_b = p[TOK + 8 :]
    b_in = softened(p, misc_ref, INNER, conv_ref, before_ok, after_ok)
    xb_ref[:, INNER:] = b_in
    p = projected(h_ref, core, own_x, other_x, slice(0, INNER))
    ctx_x = p[TOK + 8 :]
    x_in = softened(p, misc_ref, 0, conv_ref, before_ok, after_ok)
    xb_ref[:, :INNER] = x_in
    stores.append(store(3, xb_ref, xb_hbm))

    high = rounded(total)
    low = rounded(total - high)
    lane = lanes((8, 128))
    turned_b = [
        pltpu.roll(ctx_b, (64 - 16 * c) % 128, 1) if c != 4 else ctx_b for c in range(8)
    ]
    for head in range(HEADS):
        misc = jnp.zeros((8, 128), f32)
        for spot, table, col in (
            (80, ctx_dt, head), (81, ctx_dt, HEADS + head), (82, high, head), (83, low, head),
            (84, high, HEADS + head), (85, low, HEADS + head),
        ):
            misc = jnp.where(lane == spot, table[:, col : col + 1], misc)
        chunk = ctx_x[:, (head // 2) * 128 : (head // 2 + 1) * 128]
        if head % 2:
            chunk = pltpu.roll(chunk, HD, 1)
        misc = jnp.where(lane < HD, chunk, misc)
        for c in range(8):
            tile = jnp.where((lane >= 64) & (lane < 80), turned_b[c], misc)
            send_ref[head * 8 + c, 16:24, :] = tile.astype(bf16)

    left = ci < HD
    for q in range(4):
        sides = []
        for first in (0, HEADS):
            moved = rounded(x_in[:, q * 128 : (q + 1) * 128].astype(f32) * per_channel(step, first, q))
            ended = (moved * per_channel(to_end, first, q)).astype(bf16)
            sides.append(
                lax.dot_general(
                    b_in, ended, (((0,), (0,)), ((), ())), preferred_element_type=f32
                )
            )
        ahead, behind = sides
        for k, state in (
            (0, jnp.where(left, ahead, pltpu.roll(behind, HD, 1))),
            (1, jnp.where(left, pltpu.roll(ahead, HD, 1), behind)),
        ):
            head = 2 * q + k
            send_ref[head * 8 : head * 8 + 8, 0:16, :] = state.astype(bf16).reshape(8, 16, 128)
    stores.append(store(4, send_ref, send_hbm))
    for copy in stores:
        copy.wait()


def inside_kernel(
    place_ref, h_ref, own_z, other_z, own_s, other_s, xb_ref, sr_ref, misc_ref,
    y_ref, c_out_ref, z_ref, conv_ref,
):
    core, at = place_ref[0], place_ref[1]
    before_ok, after_ok = ends(at)
    p = projected(h_ref, core, own_s, other_s, slice(STATE, 2 * STATE))
    c_in = softened(p, misc_ref, INNER + STATE, conv_ref, before_ok, after_ok)
    c_out_ref[...] = c_in
    z_ref[...] = projected(h_ref, core, own_z, other_z, slice(0, INNER))[:TOK].astype(bf16)
    step, run = sr_ref[:, 0:128], sr_ref[:, 128:256]
    turned = run.T
    scores = lax.dot_general(
        c_in, xb_ref[:, INNER:], (((1,), (1,)), ((), ())), preferred_element_type=f32
    )
    ri, ci = rows_of((TOK, TOK)), lanes((TOK, TOK))
    for q in range(4):
        cols = slice(q * 128, (q + 1) * 128)
        x = xb_ref[:, cols].astype(f32)
        moved = jnp.concatenate(
            [(x * per_channel(step, first, q)).astype(bf16) for first in (0, HEADS)], axis=0
        )
        outs = []
        for head in (2 * q, 2 * q + 1):
            weights = []
            for first, kept in ((0, ri >= ci), (HEADS, ri <= ci)):
                k = first + head
                spread = run[:, k : k + 1] - turned[k : k + 1, :]
                decay = jnp.where(kept, jnp.exp(jnp.minimum(spread, 0.0)), 0.0)
                weights.append((scores * decay).astype(bf16))
            outs.append(
                jnp.dot(jnp.concatenate(weights, axis=1), moved, preferred_element_type=f32)
            )
        y_ref[:, cols] = jnp.where(ci < HD, outs[0], outs[1])


def owner_kernel(rate_ref, recv_ref, tap_ref, out_ref, pad_ref, held_ref):
    raw = recv_ref[:, 16:24, :].astype(f32).reshape(CTX, 128)
    pad_ref[0:8, :] = jnp.zeros((8, 128), f32)
    pad_ref[8 + CTX : 16 + CTX, :] = jnp.zeros((8, 128), f32)
    pad_ref[8 : 8 + CTX, :] = raw
    act = silu(
        pad_ref[7 : 7 + CTX, :] * tap_ref[0:1, :]
        + raw * tap_ref[1:2, :]
        + pad_ref[9 : 9 + CTX, :] * tap_ref[2:3, :]
    ).astype(bf16)
    lane = lanes((CTX, 128))
    left = lane < HD
    step = softplus(jnp.where(left, raw[:, 80:81], raw[:, 81:82]))
    rate = jnp.where(left, rate_ref[0], rate_ref[1])
    decay = -(rate * step)
    high = rounded(decay)
    mid = rounded(decay - high)
    spot = lane % 4
    parts = jnp.where(
        spot == 0, high, jnp.where(spot == 1, mid, jnp.where(spot == 2, decay - high - mid, 0.0))
    ).astype(bf16)
    earlier = jnp.where(lanes((CTX, CTX)) < rows_of((CTX, CTX)), 1.0, 0.0).astype(bf16)
    sums = jnp.dot(earlier, parts, preferred_element_type=f32)
    before_f = sums[:, 0:1] + sums[:, 1:2] + sums[:, 2:3]
    before_b = sums[:, 64:65] + sums[:, 65:66] + sums[:, 66:67]
    upto_f = before_f + decay[:, 0:1]
    later_f = jnp.minimum(upto_f[CTX - 1 :] - upto_f, 0.0)
    act_wide = act.astype(f32)
    moved = rounded(jnp.where(left, act_wide, pltpu.roll(act_wide, HD, 1)) * step)
    moved = moved * jnp.exp(jnp.where(left, later_f, before_b))
    top = rounded(moved)
    dims = (((0,), (0,)), ((), ()))
    start = lax.dot_general(act, top.astype(bf16), dims, preferred_element_type=f32)
    start = start + lax.dot_general(
        act, (moved - top).astype(bf16), dims, preferred_element_type=f32
    )
    state = start[64:80]
    grow = jnp.exp(
        jnp.where(left, raw[:, 82:83] + raw[:, 83:84], raw[:, 84:85] + raw[:, 85:86])
    ).reshape(NSP, 8, 128)
    left8, left16 = lanes((8, 128)) < HD, lanes((16, 128)) < HD
    for k in range(NSP):
        m = NSP - 1 - k
        held_ref[k, :, 0:HD] = state[:, 0:HD]
        held_ref[m, :, HD:128] = state[:, HD:128]
        fresh = jnp.where(left16, recv_ref[k, 0:16, :].astype(f32), recv_ref[m, 0:16, :].astype(f32))
        growth = jnp.where(left8, grow[k], grow[m])
        state = state * jnp.concatenate([growth, growth], axis=0) + fresh
    out_ref[...] = held_ref[...].astype(bf16)


def output_kernel(
    place_ref, state_ref, gain_ref, c_hbm, sr_hbm, y_hbm, z_hbm, own_hbm, other_hbm,
    out_ref, ny_ref, c_ref, sr_ref, y_ref, z_ref, own_ref, other_ref, sems,
):
    loads = [
        pltpu.make_async_copy(src, dst, sems.at[i])
        for i, (src, dst) in enumerate(
            (
                (c_hbm, c_ref), (sr_hbm, sr_ref), (y_hbm, y_ref), (z_hbm, z_ref),
                (own_hbm, own_ref), (other_hbm, other_ref),
            )
        )
    ]
    for copy in loads:
        copy.start()
    core = place_ref[0]
    for copy in loads[:4]:
        copy.wait()
    growth = jnp.exp(sr_ref[:, 128:256])
    c_in = c_ref[...]
    left = lanes((TOK, 128)) < HD
    squares = jnp.zeros((TOK, 128), f32)
    gated = []
    for q in range(4):
        cols = slice(q * 128, (q + 1) * 128)
        sums = []
        for head in (2 * q, 2 * q + 1):
            state = state_ref[head * 8 : head * 8 + 8].reshape(STATE, 128)
            both = jnp.dot(c_in, state, preferred_element_type=f32) * jnp.where(
                left, growth[:, head : head + 1], growth[:, HEADS + head : HEADS + head + 1]
            )
            sums.append(both + pltpu.roll(both, HD, 1))
        y = y_ref[:, cols] + jnp.where(left, sums[0], sums[1])
        g = y * silu(z_ref[:, cols].astype(f32))
        squares = squares + g * g
        gated.append(g)
    inv = lax.rsqrt(jnp.sum(squares, axis=1, keepdims=True) * (1.0 / INNER) + EPSILON)
    for q in range(4):
        cols = slice(q * 128, (q + 1) * 128)
        ny_ref[:, cols] = (gated[q] * inv * gain_ref[0:1, cols].astype(f32)).astype(bf16)
    half = INNER // 2
    mine = ny_ref[:, pl.ds(pl.multiple_of(core * half, half), half)]
    theirs = ny_ref[:, pl.ds(pl.multiple_of((1 - core) * half, half), half)]
    for copy in loads[4:]:
        copy.wait()
    for n in range(4):
        cols = slice(n * 512, (n + 1) * 512)
        out = jnp.dot(mine, own_ref[:, cols], preferred_element_type=f32)
        out = out + jnp.dot(theirs, other_ref[:, cols], preferred_element_type=f32)
        out_ref[:, cols] = out.astype(bf16)


def sum_kernel(tile_ref, gate_ref, out_hbm, out_ref, sem):
    total = tile_ref[0].astype(f32)
    for t in range(1, 4):
        total = total + tile_ref[t].astype(f32)
    out_ref[...] = (gate_ref[0:1, :] * total).astype(bf16)
    copy = pltpu.make_async_copy(out_ref, out_hbm, sem)
    copy.start()
    copy.wait()


def call(kernel, out_shape, n_args, smem, scratch=(), hbm=(), hbm_out=False, flops=10**8):
    space = {i: pltpu.SMEM for i in smem} | {i: pltpu.HBM for i in hbm}
    in_specs = [pl.BlockSpec(memory_space=space.get(i, pltpu.VMEM)) for i in range(n_args)]
    out = pl.BlockSpec(memory_space=pltpu.HBM if hbm_out else pltpu.VMEM)
    many = isinstance(out_shape, (list, tuple))
    return pl.pallas_call(
        kernel,
        out_shape=out_shape,
        in_specs=in_specs,
        out_specs=[out] * len(out_shape) if many else out,
        scratch_shapes=list(scratch),
        compiler_params=pltpu.CompilerParams(vmem_limit_bytes=30 * 2**20),
        cost_estimate=pl.CostEstimate(flops=flops, bytes_accessed=2**20, transcendentals=0),
        interpret=INTERPRET,
    )


def project_call(*args):
    outs = [
        ((NSP, 24, 128), bf16), ((ROWS, D), bf16), ((TOK, XB), bf16), ((TOK, 256), f32),
        ((8, D), f32),
    ]
    return call(
        project_kernel,
        [pltpu.HBM(*o) for o in outs],
        12,
        (0,),
        [
            *(pltpu.VMEM(*o) for o in outs),
            pltpu.VMEM((TOK + 16, INNER), f32),
            pltpu.SemaphoreType.DMA((5,)),
        ],
        hbm_out=True,
    )(*args)


def inside_call(*args):
    return call(
        inside_kernel,
        [
            jax.ShapeDtypeStruct((TOK, INNER), f32),
            jax.ShapeDtypeStruct((TOK, STATE), bf16),
            jax.ShapeDtypeStruct((TOK, INNER), bf16),
        ],
        9,
        (0,),
        [pltpu.VMEM((TOK + 16, STATE), f32)],
    )(*args)


def owner_call(*args):
    return call(
        owner_kernel,
        jax.ShapeDtypeStruct((NSP, 16, 128), bf16),
        3,
        (0,),
        [pltpu.VMEM((CTX + 16, 128), f32), pltpu.VMEM((NSP, 16, 128), f32)],
    )(*args)


def output_call(*args):
    return call(
        output_kernel,
        jax.ShapeDtypeStruct((TOK, D), bf16),
        9,
        (0,),
        [
            pltpu.VMEM((TOK, INNER), bf16),
            pltpu.VMEM((TOK, STATE), bf16),
            pltpu.VMEM((TOK, 256), f32),
            pltpu.VMEM((TOK, INNER), f32),
            pltpu.VMEM((TOK, INNER), bf16),
            pltpu.VMEM((INNER // 2, D), bf16),
            pltpu.VMEM((INNER // 2, D), bf16),
            pltpu.SemaphoreType.DMA((6,)),
        ],
        hbm=range(3, 9),
    )(*args[:3], *(pltpu.with_memory_space_constraint(a, pltpu.HBM) for a in args[3:]))


def sum_call(*args):
    return call(
        sum_kernel,
        pltpu.HBM((OWN, D), bf16),
        2,
        (),
        [pltpu.VMEM((OWN, D), bf16), pltpu.SemaphoreType.DMA(())],
        hbm_out=True,
    )(*args)


def swapped(x):
    return lax.ppermute(x, "dp", [(0, 1), (1, 0)])


def exchanged(x, axes):
    return lax.all_to_all(x, axes, 0, 0, tiled=True)


def sent_to_all(x, peers, axes):
    return exchanged(jnp.broadcast_to(x[None], (peers, *x.shape)), axes)


def small_weights(w_b, w_c, w_dt):
    steps = jnp.concatenate([w_dt[0], w_dt[1]], axis=1)
    steps = jnp.pad(steps, ((0, 0), (0, 128 - steps.shape[1])))
    return jnp.concatenate([w_b, w_c, steps], axis=1)


def packed_vectors(norm_gain, conv_x, conv_b, conv_c, decay_rate):
    taps = jnp.concatenate([conv_x, conv_b, conv_c], axis=1).astype(f32)
    rates = decay_rate.reshape(1, 2 * HEADS)
    return jnp.concatenate(
        [
            norm_gain.astype(f32)[None],
            jnp.pad(taps, ((0, 0), (0, D - XBC))),
            jnp.pad(rates, ((0, 3), (0, D - 2 * HEADS))),
        ],
        axis=0,
    )


def owner_taps(conv_x, conv_b, at):
    of_x = lax.dynamic_slice_in_dim(conv_x, at // 8 * HD, HD, 1)
    of_b = lax.dynamic_slice_in_dim(conv_b, at % 8 * 16, 16, 1)
    both = jnp.concatenate([of_x, of_b], axis=1).astype(f32)
    return jnp.pad(both, ((0, 0), (0, 128 - HD - 16)))


def shards(
    latent, condition, context, context_source, mod_weight, norm_gain,
    w_x, w_b, w_c, w_z, w_dt, conv_x, conv_b, conv_c, decay_rate, out_gain, w_out,
):
    at = lax.axis_index(SP)
    core = lax.axis_index("dp")
    tp = lax.axis_index("tp")
    place = jnp.stack([core, at, tp]).astype(jnp.int32)
    row_count = mod_weight.shape[1]

    rows = latent[0]
    edge = jnp.where(tp == 3, rows[OWN - 1 :], rows[:1])
    pairs = [(4 * i + 3, 4 * i + 4) for i in range(NSP - 1)]
    pairs += [(j, i) for i, j in pairs]
    halo = lax.ppermute(edge, ALL, pairs)

    act = jnp.stack(
        [silu(condition[0].astype(f32)), silu(context_source.astype(f32))]
    ).astype(bf16)
    act = lax.dynamic_slice_in_dim(act, at * row_count, row_count, 1)
    part = jnp.einsum("ar,krc->akc", act, mod_weight, preferred_element_type=f32)
    part = jnp.stack([part[0, 0], part[0, 1], part[1, 0], part[1, 1], part[0, 2]])
    part = part.reshape(20, 128)
    part = sent_to_all(part, 8, "sp_0")
    part = jnp.sum(part, axis=0)
    mods = sent_to_all(part.astype(bf16), 32, ("sp_1", "tp"))

    packed = jnp.concatenate([rows, jnp.pad(halo, ((0, 7), (0, 0)))], axis=0)
    blocks = [packed]
    for s in (1, 2, 3):
        blocks.append(lax.ppermute(packed, "tp", [(i, (i + s) % 4) for i in range(4)]))

    small = small_weights(w_b, w_c, w_dt)
    other_x = swapped(w_x)
    other_small = swapped(small)
    other_z = swapped(w_z)
    other_out = swapped(w_out)

    misc = packed_vectors(norm_gain, conv_x, conv_b, conv_c, decay_rate)
    own_taps = owner_taps(conv_x, conv_b, at)
    own_rates = lax.dynamic_slice_in_dim(decay_rate, at // 8, 1, 1)[:, 0]

    send, h, xb, sr, gate = project_call(
        place, mods, *blocks, context[0], misc, w_x, other_x, small, other_small
    )
    received = exchanged(send, SP)
    y_in, c_in, z_in = inside_call(
        place, h, w_z, other_z, small, other_small, xb, sr, misc
    )
    entering = owner_call(own_rates, received, own_taps)
    states = exchanged(entering, SP)
    partial = output_call(
        place, states, out_gain[None], c_in, sr, y_in, z_in, w_out, other_out
    )
    tiles = exchanged(partial.reshape(4, OWN, D), "tp")
    return sum_call(tiles, gate)[None]


def solution(mesh):
    torus = Mesh(
        mesh.devices.reshape(8, 8, mesh.shape["tp"], mesh.shape["dp"]), ("sp_0", "sp_1", "tp", "dp")
    )
    sp_tp = ("sp_0", "sp_1", "tp")
    placed = (
        P("dp", sp_tp, None),
        P("dp", None),
        P("dp", SP, None),
        P(),
        P(None, SP, "tp"),
        P(),
        P("dp", "tp"),
        P("dp", "tp"),
        P("dp", "tp"),
        P("dp", "tp"),
        P(None, "dp", "tp"),
        P(None, "tp"),
        P(None, "tp"),
        P(None, "tp"),
        P(None, "tp"),
        P("tp"),
        P(("tp", "dp"), None),
    )

    return jax.shard_map(
        shards, mesh=torus, in_specs=placed, out_specs=P("dp", sp_tp, None), check_vma=False
    )
```

```python
import jax
import jax.numpy as jnp
from jax import lax
from jax.experimental import pallas as pl
from jax.experimental.pallas import tpu as pltpu
from jax.sharding import Mesh
from jax.sharding import PartitionSpec as P


SP = ("sp_0", "sp_1")
ALL = ("sp_0", "sp_1", "tp")
EPSILON = 1e-06
INTERPRET = False

D = 2048
HALF = D // 2
TOK = 128
OWN = 32
INNER = 512
HEADS = 8
HD = 64
STATE = 128
NSP = 64
CTX_DEV = 8
CTX = NSP * CTX_DEV
XB = INNER + STATE
XBC = INNER + 2 * STATE
ROWS = TOK + 16

f32 = jnp.float32
bf16 = jnp.bfloat16
HIGHEST = lax.Precision.HIGHEST


def silu(v):
    return v / (1.0 + jnp.exp(-v))


def softplus(v):
    return jnp.maximum(v, 0.0) + jnp.log1p(jnp.exp(-jnp.abs(v)))


def rounded(v):
    return v.astype(bf16).astype(f32)


def lanes(shape):
    return lax.broadcasted_iota(jnp.int32, shape, 1)


def rows_of(shape):
    return lax.broadcasted_iota(jnp.int32, shape, 0)


def per_channel(table, first, chunk):
    left = table[:, first + 2 * chunk : first + 2 * chunk + 1]
    right = table[:, first + 2 * chunk + 1 : first + 2 * chunk + 2]
    shape = (table.shape[0], 128)
    return jnp.where(lanes(shape) < HD, left, right)


def softened(p, taps, first_col, conv_ref, before_ok, after_ok):
    width = p.shape[1]
    cols = slice(first_col, first_col + width)
    conv_ref[8 : 8 + TOK, :width] = p[:TOK]
    conv_ref[0:8, :width] = jnp.broadcast_to(p[TOK : TOK + 1] * before_ok, (8, width))
    conv_ref[8 + TOK : 16 + TOK, :width] = jnp.broadcast_to(
        p[TOK + 1 : TOK + 2] * after_ok, (8, width)
    )
    summed = (
        conv_ref[7 : 7 + TOK, :width] * taps[1:2, cols]
        + conv_ref[8 : 8 + TOK, :width] * taps[2:3, cols]
        + conv_ref[9 : 9 + TOK, :width] * taps[3:4, cols]
    )
    return silu(summed).astype(bf16)


def ends(at):
    return jnp.where(at > 0, 1.0, 0.0), jnp.where(at < NSP - 1, 1.0, 0.0)


def projected(h_ref, core, own_ref, other_ref, cols):
    mine = pl.multiple_of(core * HALF, HALF)
    theirs = pl.multiple_of((1 - core) * HALF, HALF)
    out = jnp.dot(h_ref[:, pl.ds(mine, HALF)], own_ref[:, cols], preferred_element_type=f32)
    return rounded(
        out
        + jnp.dot(h_ref[:, pl.ds(theirs, HALF)], other_ref[:, cols], preferred_element_type=f32)
    )


def pack_kernel(part_ref, rows_ref, halo_ref, out_hbm, tail_ref, sems):
    copies = [
        pltpu.make_async_copy(rows_ref, out_hbm.at[t, pl.ds(0, OWN)], sems.at[t]) for t in range(4)
    ]
    for copy in copies:
        copy.start()
    total = part_ref[0]
    for y in range(1, 8):
        total = total + part_ref[y]
    high = rounded(total)
    mid = rounded(total - high)
    parts = [high, mid, total - high - mid]
    zero = jnp.zeros((1, 128), f32)
    for m in range(16):
        cols = slice(m * 128, (m + 1) * 128)
        rows = [halo_ref[0:1, cols].astype(f32)]
        for r in range(7):
            k = r * 16 + m
            rows.append(parts[k // 20][k % 20 : k % 20 + 1] if k < 60 else zero)
        tail_ref[:, cols] = jnp.concatenate(rows, axis=0).astype(bf16)
    more = [
        pltpu.make_async_copy(tail_ref, out_hbm.at[t, pl.ds(OWN, 8)], sems.at[4 + t])
        for t in range(4)
    ]
    for copy in more:
        copy.start()
    for copy in copies + more:
        copy.wait()


def project_kernel(
    place_ref, blk_ref, ctx_ref, misc_ref, own_x, other_x, own_s, other_s,
    send_hbm, h_hbm, xb_hbm, sr_hbm, gate_hbm,
    send_ref, h_ref, xb_ref, sr_ref, gate_ref, conv_ref, sems,
):
    def store(i, src, dst):
        copy = pltpu.make_async_copy(src, dst, sems.at[i])
        copy.start()
        return copy

    core, at = place_ref[0], place_ref[1]
    mods, tails = [], []
    for t in range(4):
        tail = blk_ref[t, OWN:, :].astype(f32)
        tails.append(tail)

        def row(k, tail=tail):
            return tail[1 + k // 16 : 2 + k // 16, (k % 16) * 128 : (k % 16 + 1) * 128]

        mods.append([row(i) + row(20 + i) + row(40 + i) for i in range(20)])

    def inverse(rows, read):
        squares = jnp.zeros((rows, 128), f32)
        for c in range(16):
            v = read(slice(c * 128, (c + 1) * 128))
            squares = squares + v * v
        return lax.rsqrt(jnp.sum(squares, axis=1, keepdims=True) * (1.0 / D) + EPSILON)

    row8 = rows_of((8, 128))

    def neighbours(cols):
        last = pltpu.roll(tails[3][:, cols], 1, 0)
        return jnp.where(row8 == 0, tails[0][:, cols], jnp.where(row8 == 1, last, 0.0))

    inv = [inverse(OWN, lambda cols, t=t: blk_ref[t, :OWN, cols].astype(f32)) for t in range(4)]
    inv_halo = inverse(8, neighbours)
    inv_ctx = inverse(8, lambda cols: ctx_ref[:, cols].astype(f32))
    for c in range(16):
        t, q = c // 4, c % 4
        cols = slice(c * 128, (c + 1) * 128)
        gain = misc_ref[0:1, cols]
        shift, scale = mods[t][q], 1.0 + mods[t][4 + q]
        cshift, cscale = mods[t][8 + q], 1.0 + mods[t][12 + q]
        gate_ref[:, cols] = jnp.broadcast_to(mods[t][16 + q], (8, 128))
        for s in range(4):
            h = blk_ref[s, :OWN, cols].astype(f32) * inv[s] * gain * scale + shift
            h_ref[s * OWN : (s + 1) * OWN, cols] = h.astype(bf16)
        halo = neighbours(cols) * inv_halo * gain * scale + shift
        ctx = ctx_ref[:, cols].astype(f32) * inv_ctx * gain * cscale + cshift
        h_ref[TOK:ROWS, cols] = jnp.concatenate([halo, ctx], axis=0).astype(bf16)
    stores = [store(0, h_ref, h_hbm), store(1, gate_ref, gate_hbm)]

    p = projected(h_ref, core, own_s, other_s, slice(2 * STATE, 2 * STATE + 128))
    step = softplus(p[:TOK])
    ctx_dt = p[TOK + 8 :]
    log_decay = -(misc_ref[4:5, 0:128] * step)
    ri, ci = rows_of((TOK, TOK)), lanes((TOK, TOK))
    lower = jnp.where(ri >= ci, 1.0, 0.0).astype(f32)
    upper = jnp.where(ri <= ci, 1.0, 0.0).astype(f32)
    ahead = jnp.dot(lower, log_decay, preferred_element_type=f32, precision=HIGHEST)
    behind = jnp.dot(upper, log_decay, preferred_element_type=f32, precision=HIGHEST)
    run = jnp.where(ci < HEADS, ahead, behind)
    sr_ref[:, 0:128] = step
    sr_ref[:, 128:256] = run
    stores.append(store(2, sr_ref, sr_hbm))
    total = jnp.where(lanes((1, 128)) < HEADS, run[TOK - 1 : TOK], run[0:1])
    to_end = jnp.exp(total - run)

    before_ok, after_ok = ends(at)
    p = projected(h_ref, core, own_s, other_s, slice(0, STATE))
    ctx_b = p[TOK + 8 :]
    b_in = softened(p, misc_ref, INNER, conv_ref, before_ok, after_ok)
    xb_ref[:, INNER:] = b_in
    p = projected(h_ref, core, own_x, other_x, slice(0, INNER))
    ctx_x = p[TOK + 8 :]
    x_in = softened(p, misc_ref, 0, conv_ref, before_ok, after_ok)
    xb_ref[:, :INNER] = x_in
    stores.append(store(3, xb_ref, xb_hbm))

    high = rounded(total)
    low = rounded(total - high)
    lane = lanes((8, 128))
    turned_b = [
        pltpu.roll(ctx_b, (64 - 16 * c) % 128, 1) if c != 4 else ctx_b for c in range(8)
    ]
    for head in range(HEADS):
        misc = jnp.zeros((8, 128), f32)
        for spot, table, col in (
            (80, ctx_dt, head), (81, ctx_dt, HEADS + head), (82, high, head), (83, low, head),
            (84, high, HEADS + head), (85, low, HEADS + head),
        ):
            misc = jnp.where(lane == spot, table[:, col : col + 1], misc)
        chunk = ctx_x[:, (head // 2) * 128 : (head // 2 + 1) * 128]
        if head % 2:
            chunk = pltpu.roll(chunk, HD, 1)
        misc = jnp.where(lane < HD, chunk, misc)
        for c in range(8):
            tile = jnp.where((lane >= 64) & (lane < 80), turned_b[c], misc)
            send_ref[head * 8 + c, 16:24, :] = tile.astype(bf16)

    left = ci < HD
    for q in range(4):
        sides = []
        for first in (0, HEADS):
            moved = rounded(x_in[:, q * 128 : (q + 1) * 128].astype(f32) * per_channel(step, first, q))
            ended = (moved * per_channel(to_end, first, q)).astype(bf16)
            sides.append(
                lax.dot_general(
                    b_in, ended, (((0,), (0,)), ((), ())), preferred_element_type=f32
                )
            )
        ahead, behind = sides
        for k, state in (
            (0, jnp.where(left, ahead, pltpu.roll(behind, HD, 1))),
            (1, jnp.where(left, pltpu.roll(ahead, HD, 1), behind)),
        ):
            head = 2 * q + k
            send_ref[head * 8 : head * 8 + 8, 0:16, :] = state.astype(bf16).reshape(8, 16, 128)
    stores.append(store(4, send_ref, send_hbm))
    for copy in stores:
        copy.wait()


def inside_kernel(
    place_ref, h_ref, own_z, other_z, own_s, other_s, xb_ref, sr_ref, misc_ref,
    y_ref, c_out_ref, z_ref, conv_ref,
):
    core, at = place_ref[0], place_ref[1]
    before_ok, after_ok = ends(at)
    p = projected(h_ref, core, own_s, other_s, slice(STATE, 2 * STATE))
    c_in = softened(p, misc_ref, INNER + STATE, conv_ref, before_ok, after_ok)
    c_out_ref[...] = c_in
    z_ref[...] = projected(h_ref, core, own_z, other_z, slice(0, INNER))[:TOK].astype(bf16)
    step, run = sr_ref[:, 0:128], sr_ref[:, 128:256]
    turned = run.T
    scores = lax.dot_general(
        c_in, xb_ref[:, INNER:], (((1,), (1,)), ((), ())), preferred_element_type=f32
    )
    ri, ci = rows_of((TOK, TOK)), lanes((TOK, TOK))
    for q in range(4):
        cols = slice(q * 128, (q + 1) * 128)
        x = xb_ref[:, cols].astype(f32)
        moved = jnp.concatenate(
            [(x * per_channel(step, first, q)).astype(bf16) for first in (0, HEADS)], axis=0
        )
        outs = []
        for head in (2 * q, 2 * q + 1):
            weights = []
            for first, kept in ((0, ri >= ci), (HEADS, ri <= ci)):
                k = first + head
                spread = run[:, k : k + 1] - turned[k : k + 1, :]
                decay = jnp.where(kept, jnp.exp(jnp.minimum(spread, 0.0)), 0.0)
                weights.append((scores * decay).astype(bf16))
            outs.append(
                jnp.dot(jnp.concatenate(weights, axis=1), moved, preferred_element_type=f32)
            )
        y_ref[:, cols] = jnp.where(ci < HD, outs[0], outs[1])


def owner_kernel(rate_ref, recv_ref, tap_ref, out_ref, pad_ref, held_ref):
    raw = recv_ref[:, 16:24, :].astype(f32).reshape(CTX, 128)
    pad_ref[0:8, :] = jnp.zeros((8, 128), f32)
    pad_ref[8 + CTX : 16 + CTX, :] = jnp.zeros((8, 128), f32)
    pad_ref[8 : 8 + CTX, :] = raw
    act = silu(
        pad_ref[7 : 7 + CTX, :] * tap_ref[0:1, :]
        + raw * tap_ref[1:2, :]
        + pad_ref[9 : 9 + CTX, :] * tap_ref[2:3, :]
    ).astype(bf16)
    lane = lanes((CTX, 128))
    left = lane < HD
    step = softplus(jnp.where(left, raw[:, 80:81], raw[:, 81:82]))
    rate = jnp.where(left, rate_ref[0], rate_ref[1])
    decay = -(rate * step)
    high = rounded(decay)
    mid = rounded(decay - high)
    spot = lane % 4
    parts = jnp.where(
        spot == 0, high, jnp.where(spot == 1, mid, jnp.where(spot == 2, decay - high - mid, 0.0))
    ).astype(bf16)
    earlier = jnp.where(lanes((CTX, CTX)) < rows_of((CTX, CTX)), 1.0, 0.0).astype(bf16)
    sums = jnp.dot(earlier, parts, preferred_element_type=f32)
    before_f = sums[:, 0:1] + sums[:, 1:2] + sums[:, 2:3]
    before_b = sums[:, 64:65] + sums[:, 65:66] + sums[:, 66:67]
    upto_f = before_f + decay[:, 0:1]
    later_f = jnp.minimum(upto_f[CTX - 1 :] - upto_f, 0.0)
    act_wide = act.astype(f32)
    moved = rounded(jnp.where(left, act_wide, pltpu.roll(act_wide, HD, 1)) * step)
    moved = moved * jnp.exp(jnp.where(left, later_f, before_b))
    top = rounded(moved)
    dims = (((0,), (0,)), ((), ()))
    start = lax.dot_general(act, top.astype(bf16), dims, preferred_element_type=f32)
    start = start + lax.dot_general(
        act, (moved - top).astype(bf16), dims, preferred_element_type=f32
    )
    state = start[64:80]
    grow = jnp.exp(
        jnp.where(left, raw[:, 82:83] + raw[:, 83:84], raw[:, 84:85] + raw[:, 85:86])
    ).reshape(NSP, 8, 128)
    left8, left16 = lanes((8, 128)) < HD, lanes((16, 128)) < HD
    for k in range(NSP):
        m = NSP - 1 - k
        held_ref[k, :, 0:HD] = state[:, 0:HD]
        held_ref[m, :, HD:128] = state[:, HD:128]
        fresh = jnp.where(left16, recv_ref[k, 0:16, :].astype(f32), recv_ref[m, 0:16, :].astype(f32))
        growth = jnp.where(left8, grow[k], grow[m])
        state = state * jnp.concatenate([growth, growth], axis=0) + fresh
    out_ref[...] = held_ref[...].astype(bf16)


def output_kernel(
    place_ref, state_ref, gain_ref, c_ref, sr_ref, z_ref, y_hbm, own_hbm, other_hbm,
    out_ref, ny_ref, y_ref, own_ref, other_ref, sems,
):
    loads = [
        pltpu.make_async_copy(src, dst, sems.at[i])
        for i, (src, dst) in enumerate(
            ((y_hbm, y_ref), (own_hbm, own_ref), (other_hbm, other_ref))
        )
    ]
    for copy in loads:
        copy.start()
    core = place_ref[0]
    growth = jnp.exp(sr_ref[:, 128:256])
    c_in = c_ref[...]
    left = lanes((TOK, 128)) < HD
    squares = jnp.zeros((TOK, 128), f32)
    gated = []
    for q in range(4):
        cols = slice(q * 128, (q + 1) * 128)
        sums = []
        for head in (2 * q, 2 * q + 1):
            state = state_ref[head * 8 : head * 8 + 8].reshape(STATE, 128)
            both = jnp.dot(c_in, state, preferred_element_type=f32) * jnp.where(
                left, growth[:, head : head + 1], growth[:, HEADS + head : HEADS + head + 1]
            )
            sums.append(both + pltpu.roll(both, HD, 1))
        if q == 0:
            loads[0].wait()
        y = y_ref[:, cols] + jnp.where(left, sums[0], sums[1])
        g = y * silu(z_ref[:, cols].astype(f32))
        squares = squares + g * g
        gated.append(g)
    inv = lax.rsqrt(jnp.sum(squares, axis=1, keepdims=True) * (1.0 / INNER) + EPSILON)
    for q in range(4):
        cols = slice(q * 128, (q + 1) * 128)
        ny_ref[:, cols] = (gated[q] * inv * gain_ref[0:1, cols].astype(f32)).astype(bf16)
    half = INNER // 2
    mine = ny_ref[:, pl.ds(pl.multiple_of(core * half, half), half)]
    theirs = ny_ref[:, pl.ds(pl.multiple_of((1 - core) * half, half), half)]
    for copy in loads[1:]:
        copy.wait()
    for n in range(4):
        cols = slice(n * 512, (n + 1) * 512)
        out = jnp.dot(mine, own_ref[:, cols], preferred_element_type=f32)
        out = out + jnp.dot(theirs, other_ref[:, cols], preferred_element_type=f32)
        out_ref[:, cols] = out.astype(bf16)


def sum_kernel(tile_ref, gate_ref, out_hbm, out_ref, sem):
    total = tile_ref[0].astype(f32)
    for t in range(1, 4):
        total = total + tile_ref[t].astype(f32)
    out_ref[...] = (gate_ref[0:1, :] * total).astype(bf16)
    copy = pltpu.make_async_copy(out_ref, out_hbm, sem)
    copy.start()
    copy.wait()


def call(kernel, out_shape, n_args, smem, scratch=(), hbm=(), hbm_out=False, flops=10**8):
    space = {i: pltpu.SMEM for i in smem} | {i: pltpu.HBM for i in hbm}
    in_specs = [pl.BlockSpec(memory_space=space.get(i, pltpu.VMEM)) for i in range(n_args)]
    out = pl.BlockSpec(memory_space=pltpu.HBM if hbm_out else pltpu.VMEM)
    many = isinstance(out_shape, (list, tuple))
    return pl.pallas_call(
        kernel,
        out_shape=out_shape,
        in_specs=in_specs,
        out_specs=[out] * len(out_shape) if many else out,
        scratch_shapes=list(scratch),
        compiler_params=pltpu.CompilerParams(vmem_limit_bytes=30 * 2**20),
        cost_estimate=pl.CostEstimate(flops=flops, bytes_accessed=2**20, transcendentals=0),
        interpret=INTERPRET,
    )


def pack_call(*args):
    return call(
        pack_kernel,
        pltpu.HBM((4, OWN + 8, D), bf16),
        3,
        (),
        [pltpu.VMEM((8, D), bf16), pltpu.SemaphoreType.DMA((8,))],
        hbm_out=True,
    )(*args)


def project_call(*args):
    outs = [
        ((NSP, 24, 128), bf16), ((ROWS, D), bf16), ((TOK, XB), bf16), ((TOK, 256), f32),
        ((8, D), f32),
    ]
    return call(
        project_kernel,
        [pltpu.HBM(*o) for o in outs],
        8,
        (0,),
        [
            *(pltpu.VMEM(*o) for o in outs),
            pltpu.VMEM((TOK + 16, INNER), f32),
            pltpu.SemaphoreType.DMA((5,)),
        ],
        hbm_out=True,
    )(*args)


def inside_call(*args):
    return call(
        inside_kernel,
        [
            jax.ShapeDtypeStruct((TOK, INNER), f32),
            jax.ShapeDtypeStruct((TOK, STATE), bf16),
            jax.ShapeDtypeStruct((TOK, INNER), bf16),
        ],
        9,
        (0,),
        [pltpu.VMEM((TOK + 16, STATE), f32)],
    )(*args)


def owner_call(*args):
    return call(
        owner_kernel,
        jax.ShapeDtypeStruct((NSP, 16, 128), bf16),
        3,
        (0,),
        [pltpu.VMEM((CTX + 16, 128), f32), pltpu.VMEM((NSP, 16, 128), f32)],
    )(*args)


def output_call(*args):
    return call(
        output_kernel,
        jax.ShapeDtypeStruct((TOK, D), bf16),
        9,
        (0,),
        [
            pltpu.VMEM((TOK, INNER), bf16),
            pltpu.VMEM((TOK, INNER), f32),
            pltpu.VMEM((INNER // 2, D), bf16),
            pltpu.VMEM((INNER // 2, D), bf16),
            pltpu.SemaphoreType.DMA((3,)),
        ],
        hbm=(6, 7, 8),
    )(*args[:6], *(pltpu.with_memory_space_constraint(a, pltpu.HBM) for a in args[6:]))


def sum_call(*args):
    return call(
        sum_kernel,
        pltpu.HBM((OWN, D), bf16),
        2,
        (),
        [pltpu.VMEM((OWN, D), bf16), pltpu.SemaphoreType.DMA(())],
        hbm_out=True,
    )(*args)


def swapped(x):
    return lax.ppermute(x, "dp", [(0, 1), (1, 0)])


def exchanged(x, axes):
    return lax.all_to_all(x, axes, 0, 0, tiled=True)


def sent_to_all(x, peers, axes):
    return exchanged(jnp.broadcast_to(x[None], (peers, *x.shape)), axes)


def small_weights(w_b, w_c, w_dt):
    steps = jnp.concatenate([w_dt[0], w_dt[1]], axis=1)
    steps = jnp.pad(steps, ((0, 0), (0, 128 - steps.shape[1])))
    return jnp.concatenate([w_b, w_c, steps], axis=1)


def packed_vectors(norm_gain, conv_x, conv_b, conv_c, decay_rate):
    taps = jnp.concatenate([conv_x, conv_b, conv_c], axis=1).astype(f32)
    rates = decay_rate.reshape(1, 2 * HEADS)
    return jnp.concatenate(
        [
            norm_gain.astype(f32)[None],
            jnp.pad(taps, ((0, 0), (0, D - XBC))),
            jnp.pad(rates, ((0, 3), (0, D - 2 * HEADS))),
        ],
        axis=0,
    )


def owner_taps(conv_x, conv_b, at):
    of_x = lax.dynamic_slice_in_dim(conv_x, at // 8 * HD, HD, 1)
    of_b = lax.dynamic_slice_in_dim(conv_b, at % 8 * 16, 16, 1)
    both = jnp.concatenate([of_x, of_b], axis=1).astype(f32)
    return jnp.pad(both, ((0, 0), (0, 128 - HD - 16)))


def shards(
    latent, condition, context, context_source, mod_weight, norm_gain,
    w_x, w_b, w_c, w_z, w_dt, conv_x, conv_b, conv_c, decay_rate, out_gain, w_out,
):
    at = lax.axis_index(SP)
    core = lax.axis_index("dp")
    tp = lax.axis_index("tp")
    place = jnp.stack([core, at]).astype(jnp.int32)
    row_count = mod_weight.shape[1]

    rows = latent[0]
    edge = jnp.where(tp == 3, rows[OWN - 1 :], rows[:1])
    pairs = [(4 * i + 3, 4 * i + 4) for i in range(NSP - 1)]
    pairs += [(j, i) for i, j in pairs]
    halo = lax.ppermute(edge, ALL, pairs)

    act = jnp.stack(
        [silu(condition[0].astype(f32)), silu(context_source.astype(f32))]
    ).astype(bf16)
    act = lax.dynamic_slice_in_dim(act, at * row_count, row_count, 1)
    part = jnp.einsum("ar,krc->akc", act, mod_weight, preferred_element_type=f32)
    part = jnp.stack([part[0, 0], part[0, 1], part[1, 0], part[1, 1], part[0, 2]])
    part = part.reshape(20, 128)
    part = sent_to_all(part, 8, "sp_0")
    part = jnp.sum(part, axis=0)
    part = sent_to_all(part, 8, "sp_1")
    packed = pack_call(part, rows, halo)
    block = exchanged(packed, "tp")

    small = small_weights(w_b, w_c, w_dt)
    other_x = swapped(w_x)
    other_small = swapped(small)
    other_z = swapped(w_z)
    other_out = swapped(w_out)

    misc = packed_vectors(norm_gain, conv_x, conv_b, conv_c, decay_rate)
    own_taps = owner_taps(conv_x, conv_b, at)
    own_rates = lax.dynamic_slice_in_dim(decay_rate, at // 8, 1, 1)[:, 0]

    send, h, xb, sr, gate = project_call(
        place, block, context[0], misc, w_x, other_x, small, other_small
    )
    received = exchanged(send, SP)
    y_in, c_in, z_in = inside_call(
        place, h, w_z, other_z, small, other_small, xb, sr, misc
    )
    entering = owner_call(own_rates, received, own_taps)
    states = exchanged(entering, SP)
    partial = output_call(
        place, states, out_gain[None], c_in, sr, z_in, y_in, w_out, other_out
    )
    tiles = exchanged(partial.reshape(4, OWN, D), "tp")
    return sum_call(tiles, gate)[None]


def solution(mesh):
    torus = Mesh(
        mesh.devices.reshape(8, 8, mesh.shape["tp"], mesh.shape["dp"]), ("sp_0", "sp_1", "tp", "dp")
    )
    sp_tp = ("sp_0", "sp_1", "tp")
    placed = (
        P("dp", sp_tp, None),
        P("dp", None),
        P("dp", SP, None),
        P(),
        P(None, SP, "tp"),
        P(),
        P("dp", "tp"),
        P("dp", "tp"),
        P("dp", "tp"),
        P("dp", "tp"),
        P(None, "dp", "tp"),
        P(None, "tp"),
        P(None, "tp"),
        P(None, "tp"),
        P(None, "tp"),
        P("tp"),
        P(("tp", "dp"), None),
    )

    return jax.shard_map(
        shards, mesh=torus, in_specs=placed, out_specs=P("dp", sp_tp, None), check_vma=False
    )
```

```python
import jax
import jax.numpy as jnp
from jax import lax
from jax.experimental import pallas as pl
from jax.experimental.pallas import tpu as pltpu
from jax.sharding import Mesh
from jax.sharding import PartitionSpec as P


SP = ("sp_0", "sp_1")
EPSILON = 1e-06
INTERPRET = False

D = 2048
HALF = D // 2
TOK = 128
OWN = 32
INNER = 512
HEADS = 8
HD = 64
STATE = 128
NSP = 64
CTX_DEV = 8
CTX = NSP * CTX_DEV
XB = INNER + STATE
ROWS = TOK + 16

f32 = jnp.float32
bf16 = jnp.bfloat16
HIGHEST = lax.Precision.HIGHEST


def silu(v):
    return v / (1.0 + jnp.exp(-v))


def softplus(v):
    return jnp.maximum(v, 0.0) + jnp.log1p(jnp.exp(-jnp.abs(v)))


def rounded(v):
    return v.astype(bf16).astype(f32)


def lanes(shape):
    return lax.broadcasted_iota(jnp.int32, shape, 1)


def rows_of(shape):
    return lax.broadcasted_iota(jnp.int32, shape, 0)


def per_channel(table, first, chunk):
    left = table[:, first + 2 * chunk : first + 2 * chunk + 1]
    right = table[:, first + 2 * chunk + 1 : first + 2 * chunk + 2]
    shape = (table.shape[0], 128)
    return jnp.where(lanes(shape) < HD, left, right)


def softened(p, taps, first_col, conv_ref, before_ok, after_ok):
    width = p.shape[1]
    cols = slice(first_col, first_col + width)
    conv_ref[8 : 8 + TOK, :width] = p[:TOK]
    conv_ref[0:8, :width] = jnp.broadcast_to(p[TOK : TOK + 1] * before_ok, (8, width))
    conv_ref[8 + TOK : 16 + TOK, :width] = jnp.broadcast_to(
        p[TOK + 1 : TOK + 2] * after_ok, (8, width)
    )
    summed = (
        conv_ref[7 : 7 + TOK, :width] * taps[1:2, cols]
        + conv_ref[8 : 8 + TOK, :width] * taps[2:3, cols]
        + conv_ref[9 : 9 + TOK, :width] * taps[3:4, cols]
    )
    return silu(summed).astype(bf16)


def ends(at):
    return jnp.where(at > 0, 1.0, 0.0), jnp.where(at < NSP - 1, 1.0, 0.0)


def projected(h_ref, core, own_ref, other_ref, cols):
    mine = pl.multiple_of(core * HALF, HALF)
    theirs = pl.multiple_of((1 - core) * HALF, HALF)
    out = jnp.dot(h_ref[:, pl.ds(mine, HALF)], own_ref[:, cols], preferred_element_type=f32)
    return rounded(
        out
        + jnp.dot(h_ref[:, pl.ds(theirs, HALF)], other_ref[:, cols], preferred_element_type=f32)
    )


def start_kernel(place_ref, cond_ref, source_ref, weight_ref, out_hbm, out_ref, sem):
    at = place_ref[1]
    both = jnp.concatenate(
        [
            ref[0:1, pl.ds(pl.multiple_of(at // 4 * 128, 128), 128)].astype(f32)
            for ref in (cond_ref, source_ref)
        ]
        + [jnp.zeros((6, 128), f32)],
        axis=0,
    )
    both = pltpu.roll(both, (128 - at % 4 * 32) % 128, 1)
    act = silu(both)[:, 0:32].astype(bf16)
    rows = []
    sums = [jnp.dot(act, weight_ref[k], preferred_element_type=f32) for k in range(3)]
    for k, which in ((0, 0), (1, 0), (0, 1), (1, 1), (2, 0)):
        rows += [sums[k][which : which + 1, q * 128 : (q + 1) * 128] for q in range(4)]
    out = jnp.concatenate(rows, axis=0)
    for peer in range(8):
        out_ref[peer] = out
    copy = pltpu.make_async_copy(out_ref, out_hbm, sem)
    copy.start()
    copy.wait()


def project_kernel(
    place_ref, mod_ref, blk0_ref, blk1_ref, blk2_ref, blk3_ref, edge_ref, ctx_ref, misc_ref,
    own_x, own_s, other_s, other_x_hbm,
    send_hbm, h_hbm, xb_hbm, sr_hbm, gate_hbm,
    send_ref, h_ref, xb_ref, sr_ref, gate_ref, conv_ref, other_x, sems,
):
    load = pltpu.make_async_copy(other_x_hbm, other_x, sems.at[5])
    load.start()

    def store(i, src, dst):
        copy = pltpu.make_async_copy(src, dst, sems.at[i])
        copy.start()
        return copy

    core, at, tp = place_ref[0], place_ref[1], place_ref[2]
    blocks = (blk0_ref, blk1_ref, blk2_ref, blk3_ref)
    origin = [lax.rem(tp + 4 - s, 4) for s in range(4)]
    mods = []
    for t in range(4):
        total = mod_ref[t]
        for y in range(1, 8):
            total = total + mod_ref[4 * y + t]
        mods.append(total)

    def inverse(ref):
        squares = jnp.zeros((ref.shape[0], 128), f32)
        for c in range(16):
            v = ref[:, c * 128 : (c + 1) * 128].astype(f32)
            squares = squares + v * v
        return lax.rsqrt(jnp.sum(squares, axis=1, keepdims=True) * (1.0 / D) + EPSILON)

    inv = [inverse(ref) for ref in blocks]
    inv_edge = inverse(edge_ref)
    inv_ctx = inverse(ctx_ref)
    for c in range(16):
        t, q = c // 4, c % 4
        cols = slice(c * 128, (c + 1) * 128)
        gain = misc_ref[0:1, cols]
        shift, scale = mods[t][q : q + 1], 1.0 + mods[t][4 + q : 5 + q]
        cshift, cscale = mods[t][8 + q : 9 + q], 1.0 + mods[t][12 + q : 13 + q]
        gate_ref[:, cols] = jnp.broadcast_to(mods[t][16 + q : 17 + q], (8, 128))
        for s in range(4):
            h = blocks[s][:, cols].astype(f32) * inv[s] * gain * scale + shift
            h_ref[pl.ds(pl.multiple_of(origin[s] * OWN, OWN), OWN), cols] = h.astype(bf16)
        edge = edge_ref[:, cols].astype(f32) * inv_edge * gain * scale + shift
        ctx = ctx_ref[:, cols].astype(f32) * inv_ctx * gain * cscale + cshift
        h_ref[TOK:ROWS, cols] = jnp.concatenate([edge, ctx], axis=0).astype(bf16)
    stores = [store(0, h_ref, h_hbm), store(1, gate_ref, gate_hbm)]

    p = projected(h_ref, core, own_s, other_s, slice(2 * STATE, 2 * STATE + 128))
    step = softplus(p[:TOK])
    ctx_dt = p[TOK + 8 :]
    rate = misc_ref[4:5, 0:128] + pltpu.roll(misc_ref[4:8, 0:128], HEADS, 1)[1:2]
    log_decay = -(rate * step)
    ri, ci = rows_of((TOK, TOK)), lanes((TOK, TOK))
    lower = jnp.where(ri >= ci, 1.0, 0.0).astype(f32)
    upper = jnp.where(ri <= ci, 1.0, 0.0).astype(f32)
    ahead = jnp.dot(lower, log_decay, preferred_element_type=f32, precision=HIGHEST)
    behind = jnp.dot(upper, log_decay, preferred_element_type=f32, precision=HIGHEST)
    run = jnp.where(ci < HEADS, ahead, behind)
    sr_ref[:, 0:128] = step
    sr_ref[:, 128:256] = run
    stores.append(store(2, sr_ref, sr_hbm))
    total = jnp.where(lanes((1, 128)) < HEADS, run[TOK - 1 : TOK], run[0:1])
    to_end = jnp.exp(total - run)

    before_ok, after_ok = ends(at)
    p = projected(h_ref, core, own_s, other_s, slice(0, STATE))
    ctx_b = p[TOK + 8 :]
    b_in = softened(p, misc_ref, INNER, conv_ref, before_ok, after_ok)
    xb_ref[:, INNER:] = b_in
    load.wait()
    p = projected(h_ref, core, own_x, other_x, slice(0, INNER))
    ctx_x = p[TOK + 8 :]
    x_in = softened(p, misc_ref, 0, conv_ref, before_ok, after_ok)
    xb_ref[:, :INNER] = x_in
    stores.append(store(3, xb_ref, xb_hbm))

    high = rounded(total)
    low = rounded(total - high)
    lane = lanes((8, 128))
    turned_b = [
        pltpu.roll(ctx_b, (64 - 16 * c) % 128, 1) if c != 4 else ctx_b for c in range(8)
    ]
    for head in range(HEADS):
        misc = jnp.zeros((8, 128), f32)
        for spot, table, col in (
            (80, ctx_dt, head), (81, ctx_dt, HEADS + head), (82, high, head), (83, low, head),
            (84, high, HEADS + head), (85, low, HEADS + head),
        ):
            misc = jnp.where(lane == spot, table[:, col : col + 1], misc)
        chunk = ctx_x[:, (head // 2) * 128 : (head // 2 + 1) * 128]
        if head % 2:
            chunk = pltpu.roll(chunk, HD, 1)
        misc = jnp.where(lane < HD, chunk, misc)
        for c in range(8):
            tile = jnp.where((lane >= 64) & (lane < 80), turned_b[c], misc)
            send_ref[head * 8 + c, 16:24, :] = tile.astype(bf16)

    left = ci < HD
    for q in range(4):
        sides = []
        for first in (0, HEADS):
            moved = rounded(x_in[:, q * 128 : (q + 1) * 128].astype(f32) * per_channel(step, first, q))
            ended = (moved * per_channel(to_end, first, q)).astype(bf16)
            sides.append(
                lax.dot_general(
                    b_in, ended, (((0,), (0,)), ((), ())), preferred_element_type=f32
                )
            )
        ahead, behind = sides
        for k, state in (
            (0, jnp.where(left, ahead, pltpu.roll(behind, HD, 1))),
            (1, jnp.where(left, pltpu.roll(ahead, HD, 1), behind)),
        ):
            head = 2 * q + k
            send_ref[head * 8 : head * 8 + 8, 0:16, :] = state.astype(bf16).reshape(8, 16, 128)
    stores.append(store(4, send_ref, send_hbm))
    for copy in stores:
        copy.wait()


def inside_kernel(
    place_ref, h_ref, own_z, other_z, own_s, other_s, xb_ref, sr_ref, misc_ref,
    y_ref, c_out_ref, z_ref, conv_ref,
):
    core, at = place_ref[0], place_ref[1]
    before_ok, after_ok = ends(at)
    p = projected(h_ref, core, own_s, other_s, slice(STATE, 2 * STATE))
    c_in = softened(p, misc_ref, INNER + STATE, conv_ref, before_ok, after_ok)
    c_out_ref[...] = c_in
    z_ref[...] = projected(h_ref, core, own_z, other_z, slice(0, INNER))[:TOK].astype(bf16)
    step, run = sr_ref[:, 0:128], sr_ref[:, 128:256]
    turned = run.T
    scores = lax.dot_general(
        c_in, xb_ref[:, INNER:], (((1,), (1,)), ((), ())), preferred_element_type=f32
    )
    ri, ci = rows_of((TOK, TOK)), lanes((TOK, TOK))
    for q in range(4):
        cols = slice(q * 128, (q + 1) * 128)
        x = xb_ref[:, cols].astype(f32)
        moved = jnp.concatenate(
            [(x * per_channel(step, first, q)).astype(bf16) for first in (0, HEADS)], axis=0
        )
        outs = []
        for head in (2 * q, 2 * q + 1):
            weights = []
            for first, kept in ((0, ri >= ci), (HEADS, ri <= ci)):
                k = first + head
                spread = run[:, k : k + 1] - turned[k : k + 1, :]
                decay = jnp.where(kept, jnp.exp(jnp.minimum(spread, 0.0)), 0.0)
                weights.append((scores * decay).astype(bf16))
            outs.append(
                jnp.dot(jnp.concatenate(weights, axis=1), moved, preferred_element_type=f32)
            )
        y_ref[:, cols] = jnp.where(ci < HD, outs[0], outs[1])


def owner_kernel(rate_ref, recv_ref, tap_ref, out_ref, pad_ref, held_ref):
    raw = recv_ref[:, 16:24, :].astype(f32).reshape(CTX, 128)
    pad_ref[0:8, :] = jnp.zeros((8, 128), f32)
    pad_ref[8 + CTX : 16 + CTX, :] = jnp.zeros((8, 128), f32)
    pad_ref[8 : 8 + CTX, :] = raw
    act = silu(
        pad_ref[7 : 7 + CTX, :] * tap_ref[0:1, :]
        + raw * tap_ref[1:2, :]
        + pad_ref[9 : 9 + CTX, :] * tap_ref[2:3, :]
    ).astype(bf16)
    lane = lanes((CTX, 128))
    left = lane < HD
    step = softplus(jnp.where(left, raw[:, 80:81], raw[:, 81:82]))
    rate = jnp.where(left, rate_ref[0], rate_ref[1])
    decay = -(rate * step)
    high = rounded(decay)
    mid = rounded(decay - high)
    spot = lane % 4
    parts = jnp.where(
        spot == 0, high, jnp.where(spot == 1, mid, jnp.where(spot == 2, decay - high - mid, 0.0))
    ).astype(bf16)
    earlier = jnp.where(lanes((CTX, CTX)) < rows_of((CTX, CTX)), 1.0, 0.0).astype(bf16)
    sums = jnp.dot(earlier, parts, preferred_element_type=f32)
    before_f = sums[:, 0:1] + sums[:, 1:2] + sums[:, 2:3]
    before_b = sums[:, 64:65] + sums[:, 65:66] + sums[:, 66:67]
    upto_f = before_f + decay[:, 0:1]
    later_f = jnp.minimum(upto_f[CTX - 1 :] - upto_f, 0.0)
    act_wide = act.astype(f32)
    moved = rounded(jnp.where(left, act_wide, pltpu.roll(act_wide, HD, 1)) * step)
    moved = moved * jnp.exp(jnp.where(left, later_f, before_b))
    top = rounded(moved)
    dims = (((0,), (0,)), ((), ()))
    start = lax.dot_general(act, top.astype(bf16), dims, preferred_element_type=f32)
    start = start + lax.dot_general(
        act, (moved - top).astype(bf16), dims, preferred_element_type=f32
    )
    state = start[64:80]
    grow = jnp.exp(
        jnp.where(left, raw[:, 82:83] + raw[:, 83:84], raw[:, 84:85] + raw[:, 85:86])
    ).reshape(NSP, 8, 128)
    left8, left16 = lanes((8, 128)) < HD, lanes((16, 128)) < HD
    for k in range(NSP):
        m = NSP - 1 - k
        held_ref[k, :, 0:HD] = state[:, 0:HD]
        held_ref[m, :, HD:128] = state[:, HD:128]
        fresh = jnp.where(left16, recv_ref[k, 0:16, :].astype(f32), recv_ref[m, 0:16, :].astype(f32))
        growth = jnp.where(left8, grow[k], grow[m])
        state = state * jnp.concatenate([growth, growth], axis=0) + fresh
    out_ref[...] = held_ref[...].astype(bf16)


def output_kernel(
    place_ref, state_ref, gain_ref, c_ref, sr_ref, z_ref, y_hbm, own_hbm, other_hbm,
    out_ref, ny_ref, y_ref, own_ref, other_ref, sems,
):
    loads = [
        pltpu.make_async_copy(src, dst, sems.at[i])
        for i, (src, dst) in enumerate(
            ((y_hbm, y_ref), (own_hbm, own_ref), (other_hbm, other_ref))
        )
    ]
    for copy in loads:
        copy.start()
    core = place_ref[0]
    growth = jnp.exp(sr_ref[:, 128:256])
    c_in = c_ref[...]
    left = lanes((TOK, 128)) < HD
    squares = jnp.zeros((TOK, 128), f32)
    gated = []
    for q in range(4):
        cols = slice(q * 128, (q + 1) * 128)
        sums = []
        for head in (2 * q, 2 * q + 1):
            state = state_ref[head * 8 : head * 8 + 8].reshape(STATE, 128)
            both = jnp.dot(c_in, state, preferred_element_type=f32) * jnp.where(
                left, growth[:, head : head + 1], growth[:, HEADS + head : HEADS + head + 1]
            )
            sums.append(both + pltpu.roll(both, HD, 1))
        if q == 0:
            loads[0].wait()
        y = y_ref[:, cols] + jnp.where(left, sums[0], sums[1])
        g = y * silu(z_ref[:, cols].astype(f32))
        squares = squares + g * g
        gated.append(g)
    inv = lax.rsqrt(jnp.sum(squares, axis=1, keepdims=True) * (1.0 / INNER) + EPSILON)
    for q in range(4):
        cols = slice(q * 128, (q + 1) * 128)
        ny_ref[:, cols] = (gated[q] * inv * gain_ref[0:1, cols].astype(f32)).astype(bf16)
    half = INNER // 2
    mine = ny_ref[:, pl.ds(pl.multiple_of(core * half, half), half)]
    theirs = ny_ref[:, pl.ds(pl.multiple_of((1 - core) * half, half), half)]
    for copy in loads[1:]:
        copy.wait()
    for n in range(4):
        cols = slice(n * 512, (n + 1) * 512)
        out = jnp.dot(mine, own_ref[:, cols], preferred_element_type=f32)
        out = out + jnp.dot(theirs, other_ref[:, cols], preferred_element_type=f32)
        out_ref[:, cols] = out.astype(bf16)


def sum_kernel(tile_ref, gate_ref, out_hbm, out_ref, sem):
    total = tile_ref[0].astype(f32)
    for t in range(1, 4):
        total = total + tile_ref[t].astype(f32)
    out_ref[...] = (gate_ref[0:1, :] * total).astype(bf16)
    copy = pltpu.make_async_copy(out_ref, out_hbm, sem)
    copy.start()
    copy.wait()


def call(kernel, out_shape, n_args, smem, scratch=(), hbm=(), hbm_out=False, flops=10**8):
    space = {i: pltpu.SMEM for i in smem} | {i: pltpu.HBM for i in hbm}
    in_specs = [pl.BlockSpec(memory_space=space.get(i, pltpu.VMEM)) for i in range(n_args)]
    out = pl.BlockSpec(memory_space=pltpu.HBM if hbm_out else pltpu.VMEM)
    many = isinstance(out_shape, (list, tuple))
    return pl.pallas_call(
        kernel,
        out_shape=out_shape,
        in_specs=in_specs,
        out_specs=[out] * len(out_shape) if many else out,
        scratch_shapes=list(scratch),
        compiler_params=pltpu.CompilerParams(vmem_limit_bytes=30 * 2**20),
        cost_estimate=pl.CostEstimate(flops=flops, bytes_accessed=2**20, transcendentals=0),
        interpret=INTERPRET,
    )


def start_call(*args):
    return call(
        start_kernel,
        pltpu.HBM((8, 20, 128), f32),
        4,
        (0,),
        [pltpu.VMEM((8, 20, 128), f32), pltpu.SemaphoreType.DMA(())],
        hbm_out=True,
    )(*args)


def project_call(*args):
    outs = [
        ((NSP, 24, 128), bf16), ((ROWS, D), bf16), ((TOK, XB), bf16), ((TOK, 256), f32),
        ((8, D), f32),
    ]
    return call(
        project_kernel,
        [pltpu.HBM(*o) for o in outs],
        13,
        (0,),
        [
            *(pltpu.VMEM(*o) for o in outs),
            pltpu.VMEM((TOK + 16, INNER), f32),
            pltpu.VMEM((HALF, INNER), bf16),
            pltpu.SemaphoreType.DMA((6,)),
        ],
        hbm=(12,),
        hbm_out=True,
    )(*args[:12], pltpu.with_memory_space_constraint(args[12], pltpu.HBM))


def inside_call(*args):
    return call(
        inside_kernel,
        [
            jax.ShapeDtypeStruct((TOK, INNER), f32),
            jax.ShapeDtypeStruct((TOK, STATE), bf16),
            jax.ShapeDtypeStruct((TOK, INNER), bf16),
        ],
        9,
        (0,),
        [pltpu.VMEM((TOK + 16, STATE), f32)],
    )(*args)


def owner_call(*args):
    return call(
        owner_kernel,
        jax.ShapeDtypeStruct((NSP, 16, 128), bf16),
        3,
        (0,),
        [pltpu.VMEM((CTX + 16, 128), f32), pltpu.VMEM((NSP, 16, 128), f32)],
    )(*args)


def output_call(*args):
    return call(
        output_kernel,
        jax.ShapeDtypeStruct((TOK, D), bf16),
        9,
        (0,),
        [
            pltpu.VMEM((TOK, INNER), bf16),
            pltpu.VMEM((TOK, INNER), f32),
            pltpu.VMEM((INNER // 2, D), bf16),
            pltpu.VMEM((INNER // 2, D), bf16),
            pltpu.SemaphoreType.DMA((3,)),
        ],
        hbm=(6, 7, 8),
    )(*args[:6], *(pltpu.with_memory_space_constraint(a, pltpu.HBM) for a in args[6:]))


def sum_call(*args):
    return call(
        sum_kernel,
        pltpu.HBM((OWN, D), bf16),
        2,
        (),
        [pltpu.VMEM((OWN, D), bf16), pltpu.SemaphoreType.DMA(())],
        hbm_out=True,
    )(*args)


def swapped(x):
    return lax.ppermute(x, "dp", [(0, 1), (1, 0)])


def exchanged(x, axes):
    return lax.all_to_all(x, axes, 0, 0, tiled=True)


def sent_to_all(x, peers, axes):
    return exchanged(jnp.broadcast_to(x[None], (peers, *x.shape)), axes)


def small_weights(w_b, w_c, w_dt):
    steps = jnp.concatenate([w_dt[0], w_dt[1]], axis=1)
    steps = jnp.pad(steps, ((0, 0), (0, 128 - steps.shape[1])))
    return jnp.concatenate([w_b, w_c, steps], axis=1)


def packed_vectors(norm_gain, conv_x, conv_b, conv_c, decay_rate):
    def placed(v, row, col):
        v = v.astype(f32)
        return jnp.pad(v, ((row, 8 - row - v.shape[0]), (col, D - col - v.shape[1])))

    return (
        placed(norm_gain[None], 0, 0)
        + placed(conv_x, 1, 0)
        + placed(conv_b, 1, INNER)
        + placed(conv_c, 1, XB)
        + placed(decay_rate, 4, 0)
    )


def owner_taps(conv_x, conv_b, at):
    of_x = lax.dynamic_slice_in_dim(conv_x, at // 8 * HD, HD, 1)
    of_b = lax.dynamic_slice_in_dim(conv_b, at % 8 * 16, 16, 1)
    both = jnp.concatenate([of_x, of_b], axis=1).astype(f32)
    return jnp.pad(both, ((0, 0), (0, 128 - HD - 16)))


def shards(
    latent, condition, context, context_source, mod_weight, norm_gain,
    w_x, w_b, w_c, w_z, w_dt, conv_x, conv_b, conv_c, decay_rate, out_gain, w_out,
):
    at = lax.axis_index(SP)
    core = lax.axis_index("dp")
    tp = lax.axis_index("tp")
    place = jnp.stack([core, at, tp]).astype(jnp.int32)

    part = start_call(place, condition, context_source[None], mod_weight)
    part = exchanged(part, "sp_0")
    part = jnp.sum(part, axis=0)
    mods = sent_to_all(part, 32, ("sp_1", "tp"))

    rows = latent[0]
    blocks = [rows]
    for s in (1, 2, 3):
        blocks.append(lax.ppermute(rows, "tp", [(i, (i + s) % 4) for i in range(4)]))
    last, first = rows[OWN - 1 :], rows[:1]
    for s in (1, 2, 3):
        origin = (tp + 4 - s) % 4
        last = jnp.where(origin == 3, blocks[s][OWN - 1 :], last)
        first = jnp.where(origin == 0, blocks[s][:1], first)
    up = [(i, i + 1) for i in range(NSP - 1)]
    before = lax.ppermute(last, SP, up)
    after = lax.ppermute(first, SP, [(j, i) for i, j in up])
    edges = jnp.concatenate([before, after, jnp.zeros((6, D), bf16)], axis=0)

    small = small_weights(w_b, w_c, w_dt)
    other_x = swapped(w_x)
    other_small = swapped(small)
    other_z = swapped(w_z)
    other_out = swapped(w_out)

    misc = packed_vectors(norm_gain, conv_x, conv_b, conv_c, decay_rate)
    own_taps = owner_taps(conv_x, conv_b, at)
    own_rates = lax.dynamic_slice_in_dim(decay_rate, at // 8, 1, 1)[:, 0]

    send, h, xb, sr, gate = project_call(
        place, mods, *blocks, edges, context[0], misc, w_x, small, other_small, other_x
    )
    received = exchanged(send, SP)
    y_in, c_in, z_in = inside_call(
        place, h, w_z, other_z, small, other_small, xb, sr, misc
    )
    entering = owner_call(own_rates, received, own_taps)
    states = exchanged(entering, SP)
    partial = output_call(
        place, states, out_gain[None], c_in, sr, z_in, y_in, w_out, other_out
    )
    tiles = exchanged(partial.reshape(4, OWN, D), "tp")
    return sum_call(tiles, gate)[None]


def solution(mesh):
    torus = Mesh(
        mesh.devices.reshape(8, 8, mesh.shape["tp"], mesh.shape["dp"]), ("sp_0", "sp_1", "tp", "dp")
    )
    sp_tp = ("sp_0", "sp_1", "tp")
    placed = (
        P("dp", sp_tp, None),
        P("dp", None),
        P("dp", SP, None),
        P(),
        P(None, SP, "tp"),
        P(),
        P("dp", "tp"),
        P("dp", "tp"),
        P("dp", "tp"),
        P("dp", "tp"),
        P(None, "dp", "tp"),
        P(None, "tp"),
        P(None, "tp"),
        P(None, "tp"),
        P(None, "tp"),
        P("tp"),
        P(("tp", "dp"), None),
    )

    return jax.shard_map(
        shards, mesh=torus, in_specs=placed, out_specs=P("dp", sp_tp, None), check_vma=False
    )
```

```python
import jax
import jax.numpy as jnp
from jax import lax
from jax.experimental import pallas as pl
from jax.experimental.pallas import tpu as pltpu
from jax.sharding import Mesh
from jax.sharding import PartitionSpec as P


SP = ("sp_0", "sp_1")
ALL = ("sp_0", "sp_1", "tp")
EPSILON = 1e-06
INTERPRET = False

D = 2048
HALF = D // 2
TOK = 128
OWN = 32
INNER = 512
HEADS = 8
HD = 64
STATE = 128
NSP = 64
CTX_DEV = 8
CTX = NSP * CTX_DEV
XB = INNER + STATE
ROWS = TOK + 16

f32 = jnp.float32
bf16 = jnp.bfloat16
HIGHEST = lax.Precision.HIGHEST


def silu(v):
    return v / (1.0 + jnp.exp(-v))


def softplus(v):
    return jnp.maximum(v, 0.0) + jnp.log1p(jnp.exp(-jnp.abs(v)))


def rounded(v):
    return v.astype(bf16).astype(f32)


def lanes(shape):
    return lax.broadcasted_iota(jnp.int32, shape, 1)


def rows_of(shape):
    return lax.broadcasted_iota(jnp.int32, shape, 0)


def per_channel(table, first, chunk):
    left = table[:, first + 2 * chunk : first + 2 * chunk + 1]
    right = table[:, first + 2 * chunk + 1 : first + 2 * chunk + 2]
    shape = (table.shape[0], 128)
    return jnp.where(lanes(shape) < HD, left, right)


def softened(p, taps, first_col, conv_ref, before_ok, after_ok):
    width = p.shape[1]
    cols = slice(first_col, first_col + width)
    conv_ref[8 : 8 + TOK, :width] = p[:TOK]
    conv_ref[0:8, :width] = jnp.broadcast_to(p[TOK : TOK + 1] * before_ok, (8, width))
    conv_ref[8 + TOK : 16 + TOK, :width] = jnp.broadcast_to(
        p[TOK + 1 : TOK + 2] * after_ok, (8, width)
    )
    summed = (
        conv_ref[7 : 7 + TOK, :width] * taps[1:2, cols]
        + conv_ref[8 : 8 + TOK, :width] * taps[2:3, cols]
        + conv_ref[9 : 9 + TOK, :width] * taps[3:4, cols]
    )
    return silu(summed).astype(bf16)


def ends(at):
    return jnp.where(at > 0, 1.0, 0.0), jnp.where(at < NSP - 1, 1.0, 0.0)


def projected(h_ref, core, own_ref, other_ref, cols):
    mine = pl.multiple_of(core * HALF, HALF)
    theirs = pl.multiple_of((1 - core) * HALF, HALF)
    out = jnp.dot(h_ref[:, pl.ds(mine, HALF)], own_ref[:, cols], preferred_element_type=f32)
    return rounded(
        out
        + jnp.dot(h_ref[:, pl.ds(theirs, HALF)], other_ref[:, cols], preferred_element_type=f32)
    )


def pack_kernel(part_ref, rows_ref, halo_ref, out_ref):
    out_ref[0:OWN, :] = rows_ref[...]
    total = part_ref[0]
    for y in range(1, 8):
        total = total + part_ref[y]
    high = rounded(total)
    mid = rounded(total - high)
    parts = [high, mid, total - high - mid]
    zero = jnp.zeros((1, 128), f32)
    for m in range(16):
        cols = slice(m * 128, (m + 1) * 128)
        rows = [halo_ref[0:1, cols].astype(f32)]
        for r in range(7):
            k = r * 16 + m
            rows.append(parts[k // 20][k % 20 : k % 20 + 1] if k < 60 else zero)
        out_ref[OWN:, cols] = jnp.concatenate(rows, axis=0).astype(bf16)


def project_kernel(
    place_ref, blk0_ref, blk1_ref, blk2_ref, blk3_ref, ctx_ref, misc_ref,
    own_x, other_x, own_s, other_s,
    send_hbm, h_hbm, xb_hbm, sr_hbm, gate_hbm,
    send_ref, h_ref, xb_ref, sr_ref, gate_ref, conv_ref, mods_ref, edge_ref, sems,
):
    def store(i, src, dst):
        copy = pltpu.make_async_copy(src, dst, sems.at[i])
        copy.start()
        return copy

    core, at, tp = place_ref[0], place_ref[1], place_ref[2]
    blocks = (blk0_ref, blk1_ref, blk2_ref, blk3_ref)
    origin = [lax.rem(tp + 4 - s, 4) for s in range(4)]
    tails = [ref[OWN:, :].astype(f32) for ref in blocks]
    for s in range(4):

        def row(k, tail=tails[s]):
            return tail[1 + k // 16 : 2 + k // 16, (k % 16) * 128 : (k % 16 + 1) * 128]

        found = [row(i) + row(20 + i) + row(40 + i) for i in range(20)]
        found += [jnp.zeros((4, 128), f32)]
        mods_ref[pl.ds(pl.multiple_of(origin[s] * 24, 8), 24), :] = jnp.concatenate(found, axis=0)
    row8 = rows_of((8, D))
    before = sum(t * jnp.where(o == 0, 1.0, 0.0) for t, o in zip(tails, origin))
    after = sum(t * jnp.where(o == 3, 1.0, 0.0) for t, o in zip(tails, origin))
    edge_ref[...] = jnp.where(
        row8 == 0, before, jnp.where(row8 == 1, pltpu.roll(after, 1, 0), 0.0)
    )

    def inverse(ref, rows):
        squares = jnp.zeros((rows, 128), f32)
        for c in range(16):
            v = ref[:rows, c * 128 : (c + 1) * 128].astype(f32)
            squares = squares + v * v
        return lax.rsqrt(jnp.sum(squares, axis=1, keepdims=True) * (1.0 / D) + EPSILON)

    inv = [inverse(ref, OWN) for ref in blocks]
    inv_edge = inverse(edge_ref, 8)
    inv_ctx = inverse(ctx_ref, 8)
    for c in range(16):
        t, q = c // 4, c % 4
        cols = slice(c * 128, (c + 1) * 128)

        def mod(k, at=24 * t + q):
            return mods_ref[at + 4 * k : at + 4 * k + 1, :]

        gain = misc_ref[0:1, cols]
        shift, scale, cshift, cscale = mod(0), gain * (1.0 + mod(1)), mod(2), gain * (1.0 + mod(3))
        gate_ref[:, cols] = jnp.broadcast_to(mod(4), (8, 128))
        for s in range(4):
            h = blocks[s][:OWN, cols].astype(f32) * inv[s] * scale + shift
            h_ref[pl.ds(pl.multiple_of(origin[s] * OWN, OWN), OWN), cols] = h.astype(bf16)
        edge = edge_ref[:, cols] * inv_edge * scale + shift
        ctx = ctx_ref[:, cols].astype(f32) * inv_ctx * cscale + cshift
        h_ref[TOK:ROWS, cols] = jnp.concatenate([edge, ctx], axis=0).astype(bf16)
    stores = [store(0, h_ref, h_hbm), store(1, gate_ref, gate_hbm)]

    p = projected(h_ref, core, own_s, other_s, slice(2 * STATE, 2 * STATE + 128))
    step = softplus(p[:TOK])
    ctx_dt = p[TOK + 8 :]
    rate = misc_ref[4:5, 0:128] + pltpu.roll(misc_ref[4:8, 0:128], HEADS, 1)[1:2]
    log_decay = -(rate * step)
    ri, ci = rows_of((TOK, TOK)), lanes((TOK, TOK))
    lower = jnp.where(ri >= ci, 1.0, 0.0).astype(f32)
    upper = jnp.where(ri <= ci, 1.0, 0.0).astype(f32)
    ahead = jnp.dot(lower, log_decay, preferred_element_type=f32, precision=HIGHEST)
    behind = jnp.dot(upper, log_decay, preferred_element_type=f32, precision=HIGHEST)
    run = jnp.where(ci < HEADS, ahead, behind)
    sr_ref[:, 0:128] = step
    sr_ref[:, 128:256] = run
    stores.append(store(2, sr_ref, sr_hbm))
    total = jnp.where(lanes((1, 128)) < HEADS, run[TOK - 1 : TOK], run[0:1])
    to_end = jnp.exp(total - run)

    before_ok, after_ok = ends(at)
    p = projected(h_ref, core, own_s, other_s, slice(0, STATE))
    ctx_b = p[TOK + 8 :]
    b_in = softened(p, misc_ref, INNER, conv_ref, before_ok, after_ok)
    xb_ref[:, INNER:] = b_in
    p = projected(h_ref, core, own_x, other_x, slice(0, INNER))
    ctx_x = p[TOK + 8 :]
    x_in = softened(p, misc_ref, 0, conv_ref, before_ok, after_ok)
    xb_ref[:, :INNER] = x_in
    stores.append(store(3, xb_ref, xb_hbm))

    high = rounded(total)
    low = rounded(total - high)
    lane = lanes((8, 128))
    turned_b = [
        pltpu.roll(ctx_b, (64 - 16 * c) % 128, 1) if c != 4 else ctx_b for c in range(8)
    ]
    for head in range(HEADS):
        misc = jnp.zeros((8, 128), f32)
        for spot, table, col in (
            (80, ctx_dt, head), (81, ctx_dt, HEADS + head), (82, high, head), (83, low, head),
            (84, high, HEADS + head), (85, low, HEADS + head),
        ):
            misc = jnp.where(lane == spot, table[:, col : col + 1], misc)
        chunk = ctx_x[:, (head // 2) * 128 : (head // 2 + 1) * 128]
        if head % 2:
            chunk = pltpu.roll(chunk, HD, 1)
        misc = jnp.where(lane < HD, chunk, misc)
        for c in range(8):
            tile = jnp.where((lane >= 64) & (lane < 80), turned_b[c], misc)
            send_ref[head * 8 + c, 16:24, :] = tile.astype(bf16)

    left = ci < HD
    for q in range(4):
        sides = []
        for first in (0, HEADS):
            moved = rounded(x_in[:, q * 128 : (q + 1) * 128].astype(f32) * per_channel(step, first, q))
            ended = (moved * per_channel(to_end, first, q)).astype(bf16)
            sides.append(
                lax.dot_general(
                    b_in, ended, (((0,), (0,)), ((), ())), preferred_element_type=f32
                )
            )
        ahead, behind = sides
        for k, state in (
            (0, jnp.where(left, ahead, pltpu.roll(behind, HD, 1))),
            (1, jnp.where(left, pltpu.roll(ahead, HD, 1), behind)),
        ):
            head = 2 * q + k
            send_ref[head * 8 : head * 8 + 8, 0:16, :] = state.astype(bf16).reshape(8, 16, 128)
    stores.append(store(4, send_ref, send_hbm))
    for copy in stores:
        copy.wait()


def inside_kernel(
    place_ref, h_ref, own_z, other_z, own_s, other_s, xb_ref, sr_ref, misc_ref,
    y_ref, c_out_ref, z_ref, conv_ref,
):
    core, at = place_ref[0], place_ref[1]
    before_ok, after_ok = ends(at)
    p = projected(h_ref, core, own_s, other_s, slice(STATE, 2 * STATE))
    c_in = softened(p, misc_ref, INNER + STATE, conv_ref, before_ok, after_ok)
    c_out_ref[...] = c_in
    z_ref[...] = projected(h_ref, core, own_z, other_z, slice(0, INNER))[:TOK].astype(bf16)
    step, run = sr_ref[:, 0:128], sr_ref[:, 128:256]
    turned = run.T
    scores = lax.dot_general(
        c_in, xb_ref[:, INNER:], (((1,), (1,)), ((), ())), preferred_element_type=f32
    )
    ri, ci = rows_of((TOK, TOK)), lanes((TOK, TOK))
    for q in range(4):
        cols = slice(q * 128, (q + 1) * 128)
        x = xb_ref[:, cols].astype(f32)
        moved = jnp.concatenate(
            [(x * per_channel(step, first, q)).astype(bf16) for first in (0, HEADS)], axis=0
        )
        outs = []
        for head in (2 * q, 2 * q + 1):
            weights = []
            for first, kept in ((0, ri >= ci), (HEADS, ri <= ci)):
                k = first + head
                spread = run[:, k : k + 1] - turned[k : k + 1, :]
                decay = jnp.where(kept, jnp.exp(jnp.minimum(spread, 0.0)), 0.0)
                weights.append((scores * decay).astype(bf16))
            outs.append(
                jnp.dot(jnp.concatenate(weights, axis=1), moved, preferred_element_type=f32)
            )
        y_ref[:, cols] = jnp.where(ci < HD, outs[0], outs[1])


def owner_kernel(rate_ref, recv_ref, tap_ref, out_ref, pad_ref, held_ref):
    raw = recv_ref[:, 16:24, :].astype(f32).reshape(CTX, 128)
    pad_ref[0:8, :] = jnp.zeros((8, 128), f32)
    pad_ref[8 + CTX : 16 + CTX, :] = jnp.zeros((8, 128), f32)
    pad_ref[8 : 8 + CTX, :] = raw
    act = silu(
        pad_ref[7 : 7 + CTX, :] * tap_ref[0:1, :]
        + raw * tap_ref[1:2, :]
        + pad_ref[9 : 9 + CTX, :] * tap_ref[2:3, :]
    ).astype(bf16)
    lane = lanes((CTX, 128))
    left = lane < HD
    step = softplus(jnp.where(left, raw[:, 80:81], raw[:, 81:82]))
    rate = jnp.where(left, rate_ref[0], rate_ref[1])
    decay = -(rate * step)
    high = rounded(decay)
    mid = rounded(decay - high)
    spot = lane % 4
    parts = jnp.where(
        spot == 0, high, jnp.where(spot == 1, mid, jnp.where(spot == 2, decay - high - mid, 0.0))
    ).astype(bf16)
    earlier = jnp.where(lanes((CTX, CTX)) < rows_of((CTX, CTX)), 1.0, 0.0).astype(bf16)
    sums = jnp.dot(earlier, parts, preferred_element_type=f32)
    before_f = sums[:, 0:1] + sums[:, 1:2] + sums[:, 2:3]
    before_b = sums[:, 64:65] + sums[:, 65:66] + sums[:, 66:67]
    upto_f = before_f + decay[:, 0:1]
    later_f = jnp.minimum(upto_f[CTX - 1 :] - upto_f, 0.0)
    act_wide = act.astype(f32)
    moved = rounded(jnp.where(left, act_wide, pltpu.roll(act_wide, HD, 1)) * step)
    moved = moved * jnp.exp(jnp.where(left, later_f, before_b))
    top = rounded(moved)
    dims = (((0,), (0,)), ((), ()))
    start = lax.dot_general(act, top.astype(bf16), dims, preferred_element_type=f32)
    start = start + lax.dot_general(
        act, (moved - top).astype(bf16), dims, preferred_element_type=f32
    )
    state = start[64:80]
    grow = jnp.exp(
        jnp.where(left, raw[:, 82:83] + raw[:, 83:84], raw[:, 84:85] + raw[:, 85:86])
    ).reshape(NSP, 8, 128)
    left8, left16 = lanes((8, 128)) < HD, lanes((16, 128)) < HD
    for k in range(NSP):
        m = NSP - 1 - k
        held_ref[k, :, 0:HD] = state[:, 0:HD]
        held_ref[m, :, HD:128] = state[:, HD:128]
        fresh = jnp.where(left16, recv_ref[k, 0:16, :].astype(f32), recv_ref[m, 0:16, :].astype(f32))
        growth = jnp.where(left8, grow[k], grow[m])
        state = state * jnp.concatenate([growth, growth], axis=0) + fresh
    out_ref[...] = held_ref[...].astype(bf16)


def output_kernel(
    place_ref, state_ref, gain_ref, c_ref, sr_ref, z_ref, y_hbm, own_hbm, other_hbm,
    tile0_ref, tile1_ref, tile2_ref, tile3_ref, out_ref, ny_ref, y_ref, own_ref, other_ref, sems,
):
    loads = [
        pltpu.make_async_copy(src, dst, sems.at[i])
        for i, (src, dst) in enumerate(
            ((y_hbm, y_ref), (own_hbm, own_ref), (other_hbm, other_ref))
        )
    ]
    for copy in loads:
        copy.start()
    core = place_ref[0]
    growth = jnp.exp(sr_ref[:, 128:256])
    c_in = c_ref[...]
    left = lanes((TOK, 128)) < HD
    squares = jnp.zeros((TOK, 128), f32)
    gated = []
    for q in range(4):
        cols = slice(q * 128, (q + 1) * 128)
        sums = []
        for head in (2 * q, 2 * q + 1):
            state = state_ref[head * 8 : head * 8 + 8].reshape(STATE, 128)
            both = jnp.dot(c_in, state, preferred_element_type=f32) * jnp.where(
                left, growth[:, head : head + 1], growth[:, HEADS + head : HEADS + head + 1]
            )
            sums.append(both + pltpu.roll(both, HD, 1))
        if q == 0:
            loads[0].wait()
        y = y_ref[:, cols] + jnp.where(left, sums[0], sums[1])
        g = y * silu(z_ref[:, cols].astype(f32))
        squares = squares + g * g
        gated.append(g)
    inv = lax.rsqrt(jnp.sum(squares, axis=1, keepdims=True) * (1.0 / INNER) + EPSILON)
    for q in range(4):
        cols = slice(q * 128, (q + 1) * 128)
        ny_ref[:, cols] = (gated[q] * inv * gain_ref[0:1, cols].astype(f32)).astype(bf16)
    half = INNER // 2
    mine = ny_ref[:, pl.ds(pl.multiple_of(core * half, half), half)]
    theirs = ny_ref[:, pl.ds(pl.multiple_of((1 - core) * half, half), half)]
    for copy in loads[1:]:
        copy.wait()
    for n in range(4):
        cols = slice(n * 512, (n + 1) * 512)
        out = jnp.dot(mine, own_ref[:, cols], preferred_element_type=f32)
        out = out + jnp.dot(theirs, other_ref[:, cols], preferred_element_type=f32)
        out_ref[:, cols] = out.astype(bf16)
    tp = place_ref[2]
    for s, tile in enumerate((tile0_ref, tile1_ref, tile2_ref, tile3_ref)):
        tile[...] = out_ref[pl.ds(pl.multiple_of(lax.rem(tp + s, 4) * OWN, OWN), OWN), :]


def sum_kernel(tile0_ref, tile1_ref, tile2_ref, tile3_ref, gate_ref, out_hbm, out_ref, sem):
    total = tile0_ref[...].astype(f32)
    for tile in (tile1_ref, tile2_ref, tile3_ref):
        total = total + tile[...].astype(f32)
    out_ref[...] = (gate_ref[0:1, :] * total).astype(bf16)
    copy = pltpu.make_async_copy(out_ref, out_hbm, sem)
    copy.start()
    copy.wait()


def call(kernel, out_shape, n_args, smem, scratch=(), hbm=(), hbm_out=False, flops=10**8):
    space = {i: pltpu.SMEM for i in smem} | {i: pltpu.HBM for i in hbm}
    in_specs = [pl.BlockSpec(memory_space=space.get(i, pltpu.VMEM)) for i in range(n_args)]
    out = pl.BlockSpec(memory_space=pltpu.HBM if hbm_out else pltpu.VMEM)
    many = isinstance(out_shape, (list, tuple))
    return pl.pallas_call(
        kernel,
        out_shape=out_shape,
        in_specs=in_specs,
        out_specs=[out] * len(out_shape) if many else out,
        scratch_shapes=list(scratch),
        compiler_params=pltpu.CompilerParams(vmem_limit_bytes=30 * 2**20),
        cost_estimate=pl.CostEstimate(flops=flops, bytes_accessed=2**20, transcendentals=0),
        interpret=INTERPRET,
    )


def pack_call(*args):
    return call(pack_kernel, jax.ShapeDtypeStruct((OWN + 8, D), bf16), 3, ())(*args)


def project_call(*args):
    outs = [
        ((NSP, 24, 128), bf16), ((ROWS, D), bf16), ((TOK, XB), bf16), ((TOK, 256), f32),
        ((8, D), f32),
    ]
    return call(
        project_kernel,
        [pltpu.HBM(*o) for o in outs],
        11,
        (0,),
        [
            *(pltpu.VMEM(*o) for o in outs),
            pltpu.VMEM((TOK + 16, INNER), f32),
            pltpu.VMEM((96, 128), f32),
            pltpu.VMEM((8, D), f32),
            pltpu.SemaphoreType.DMA((5,)),
        ],
        hbm_out=True,
    )(*args)


def inside_call(*args):
    return call(
        inside_kernel,
        [
            jax.ShapeDtypeStruct((TOK, INNER), f32),
            jax.ShapeDtypeStruct((TOK, STATE), bf16),
            jax.ShapeDtypeStruct((TOK, INNER), bf16),
        ],
        9,
        (0,),
        [pltpu.VMEM((TOK + 16, STATE), f32)],
    )(*args)


def owner_call(*args):
    return call(
        owner_kernel,
        jax.ShapeDtypeStruct((NSP, 16, 128), bf16),
        3,
        (0,),
        [pltpu.VMEM((CTX + 16, 128), f32), pltpu.VMEM((NSP, 16, 128), f32)],
    )(*args)


def output_call(*args):
    return call(
        output_kernel,
        [jax.ShapeDtypeStruct((OWN, D), bf16)] * 4,
        9,
        (0,),
        [
            pltpu.VMEM((TOK, D), bf16),
            pltpu.VMEM((TOK, INNER), bf16),
            pltpu.VMEM((TOK, INNER), f32),
            pltpu.VMEM((INNER // 2, D), bf16),
            pltpu.VMEM((INNER // 2, D), bf16),
            pltpu.SemaphoreType.DMA((3,)),
        ],
        hbm=(6, 7, 8),
    )(*args[:6], *(pltpu.with_memory_space_constraint(a, pltpu.HBM) for a in args[6:]))


def sum_call(*args):
    return call(
        sum_kernel,
        pltpu.HBM((OWN, D), bf16),
        5,
        (),
        [pltpu.VMEM((OWN, D), bf16), pltpu.SemaphoreType.DMA(())],
        hbm_out=True,
    )(*args)


def swapped(x):
    return lax.ppermute(x, "dp", [(0, 1), (1, 0)])


def exchanged(x, axes):
    return lax.all_to_all(x, axes, 0, 0, tiled=True)


def turned(by):
    return [(i, (i + by) % 4) for i in range(4)]


def sent_to_all(x, peers, axes):
    return exchanged(jnp.broadcast_to(x[None], (peers, *x.shape)), axes)


def small_weights(w_b, w_c, w_dt):
    steps = jnp.concatenate([w_dt[0], w_dt[1]], axis=1)
    steps = jnp.pad(steps, ((0, 0), (0, 128 - steps.shape[1])))
    return jnp.concatenate([w_b, w_c, steps], axis=1)


def packed_vectors(norm_gain, conv_x, conv_b, conv_c, decay_rate):
    def placed(v, row, col):
        v = v.astype(f32)
        return jnp.pad(v, ((row, 8 - row - v.shape[0]), (col, D - col - v.shape[1])))

    return (
        placed(norm_gain[None], 0, 0)
        + placed(conv_x, 1, 0)
        + placed(conv_b, 1, INNER)
        + placed(conv_c, 1, XB)
        + placed(decay_rate, 4, 0)
    )


def owner_taps(conv_x, conv_b, at):
    of_x = lax.dynamic_slice_in_dim(conv_x, at // 8 * HD, HD, 1)
    of_b = lax.dynamic_slice_in_dim(conv_b, at % 8 * 16, 16, 1)
    both = jnp.concatenate([of_x, of_b], axis=1).astype(f32)
    return jnp.pad(both, ((0, 0), (0, 128 - HD - 16)))


def shards(
    latent, condition, context, context_source, mod_weight, norm_gain,
    w_x, w_b, w_c, w_z, w_dt, conv_x, conv_b, conv_c, decay_rate, out_gain, w_out,
):
    at = lax.axis_index(SP)
    core = lax.axis_index("dp")
    tp = lax.axis_index("tp")
    place = jnp.stack([core, at, tp]).astype(jnp.int32)
    row_count = mod_weight.shape[1]

    rows = latent[0]
    edge = jnp.where(tp == 3, rows[OWN - 1 :], rows[:1])
    pairs = [(4 * i + 3, 4 * i + 4) for i in range(NSP - 1)]
    pairs += [(j, i) for i, j in pairs]
    halo = lax.ppermute(edge, ALL, pairs)

    act = jnp.stack(
        [silu(condition[0].astype(f32)), silu(context_source.astype(f32))]
    ).astype(bf16)
    act = lax.dynamic_slice_in_dim(act, at * row_count, row_count, 1)
    part = jnp.einsum("ar,krc->akc", act, mod_weight, preferred_element_type=f32)
    part = jnp.stack([part[0, 0], part[0, 1], part[1, 0], part[1, 1], part[0, 2]])
    part = part.reshape(20, 128)
    part = sent_to_all(part, 8, "sp_0")
    part = jnp.sum(part, axis=0)
    part = sent_to_all(part, 8, "sp_1")
    blocks = [pack_call(part, rows, halo)]
    for s in (1, 2, 3):
        blocks.append(lax.ppermute(blocks[0], "tp", turned(s)))

    small = small_weights(w_b, w_c, w_dt)
    other_x = swapped(w_x)
    other_small = swapped(small)
    other_z = swapped(w_z)
    other_out = swapped(w_out)

    misc = packed_vectors(norm_gain, conv_x, conv_b, conv_c, decay_rate)
    own_taps = owner_taps(conv_x, conv_b, at)
    own_rates = lax.dynamic_slice_in_dim(decay_rate, at // 8, 1, 1)[:, 0]

    send, h, xb, sr, gate = project_call(
        place, *blocks, context[0], misc, w_x, other_x, small, other_small
    )
    received = exchanged(send, SP)
    y_in, c_in, z_in = inside_call(
        place, h, w_z, other_z, small, other_small, xb, sr, misc
    )
    entering = owner_call(own_rates, received, own_taps)
    states = exchanged(entering, SP)
    tiles = output_call(
        place, states, out_gain[None], c_in, sr, z_in, y_in, w_out, other_out
    )
    received = [tiles[0]]
    for s in (1, 2, 3):
        received.append(lax.ppermute(tiles[s], "tp", turned(s)))
    return sum_call(*received, gate)[None]


def solution(mesh):
    torus = Mesh(
        mesh.devices.reshape(8, 8, mesh.shape["tp"], mesh.shape["dp"]), ("sp_0", "sp_1", "tp", "dp")
    )
    sp_tp = ("sp_0", "sp_1", "tp")
    placed = (
        P("dp", sp_tp, None),
        P("dp", None),
        P("dp", SP, None),
        P(),
        P(None, SP, "tp"),
        P(),
        P("dp", "tp"),
        P("dp", "tp"),
        P("dp", "tp"),
        P("dp", "tp"),
        P(None, "dp", "tp"),
        P(None, "tp"),
        P(None, "tp"),
        P(None, "tp"),
        P(None, "tp"),
        P("tp"),
        P(("tp", "dp"), None),
    )

    return jax.shard_map(
        shards, mesh=torus, in_specs=placed, out_specs=P("dp", sp_tp, None), check_vma=False
    )
```

```python
import jax
import jax.numpy as jnp
from jax import lax
from jax.experimental import pallas as pl
from jax.experimental.pallas import tpu as pltpu
from jax.sharding import Mesh
from jax.sharding import PartitionSpec as P


SP = ("sp_0", "sp_1")
ALL = ("sp_0", "sp_1", "tp")
EPSILON = 1e-06
INTERPRET = False

D = 2048
HALF = D // 2
TOK = 128
OWN = 32
INNER = 512
HEADS = 8
HD = 64
STATE = 128
NSP = 64
CTX_DEV = 8
CTX = NSP * CTX_DEV
XB = INNER + STATE
ROWS = TOK + 16

f32 = jnp.float32
bf16 = jnp.bfloat16
HIGHEST = lax.Precision.HIGHEST


def silu(v):
    return v / (1.0 + jnp.exp(-v))


def softplus(v):
    return jnp.maximum(v, 0.0) + jnp.log1p(jnp.exp(-jnp.abs(v)))


def rounded(v):
    return v.astype(bf16).astype(f32)


def lanes(shape):
    return lax.broadcasted_iota(jnp.int32, shape, 1)


def rows_of(shape):
    return lax.broadcasted_iota(jnp.int32, shape, 0)


def per_channel(table, first, chunk):
    left = table[:, first + 2 * chunk : first + 2 * chunk + 1]
    right = table[:, first + 2 * chunk + 1 : first + 2 * chunk + 2]
    shape = (table.shape[0], 128)
    return jnp.where(lanes(shape) < HD, left, right)


def softened(p, taps, first_col, conv_ref, before_ok, after_ok):
    width = p.shape[1]
    cols = slice(first_col, first_col + width)
    conv_ref[8 : 8 + TOK, :width] = p[:TOK]
    conv_ref[0:8, :width] = jnp.broadcast_to(p[TOK : TOK + 1] * before_ok, (8, width))
    conv_ref[8 + TOK : 16 + TOK, :width] = jnp.broadcast_to(
        p[TOK + 1 : TOK + 2] * after_ok, (8, width)
    )
    summed = (
        conv_ref[7 : 7 + TOK, :width] * taps[1:2, cols]
        + conv_ref[8 : 8 + TOK, :width] * taps[2:3, cols]
        + conv_ref[9 : 9 + TOK, :width] * taps[3:4, cols]
    )
    return silu(summed).astype(bf16)


def ends(at):
    return jnp.where(at > 0, 1.0, 0.0), jnp.where(at < NSP - 1, 1.0, 0.0)


def projected(h_ref, core, own_ref, other_ref, cols):
    mine = pl.multiple_of(core * HALF, HALF)
    theirs = pl.multiple_of((1 - core) * HALF, HALF)
    out = jnp.dot(h_ref[:, pl.ds(mine, HALF)], own_ref[:, cols], preferred_element_type=f32)
    return rounded(
        out
        + jnp.dot(h_ref[:, pl.ds(theirs, HALF)], other_ref[:, cols], preferred_element_type=f32)
    )


def pack_kernel(part_ref, rows_ref, halo_ref, out_ref):
    out_ref[0:OWN, :] = rows_ref[...]
    total = part_ref[0]
    for y in range(1, 8):
        total = total + part_ref[y]
    high = rounded(total)
    mid = rounded(total - high)
    parts = [high, mid, total - high - mid]
    zero = jnp.zeros((1, 128), f32)
    for m in range(16):
        cols = slice(m * 128, (m + 1) * 128)
        rows = [halo_ref[0:1, cols].astype(f32)]
        for r in range(7):
            k = r * 16 + m
            rows.append(parts[k // 20][k % 20 : k % 20 + 1] if k < 60 else zero)
        out_ref[OWN:, cols] = jnp.concatenate(rows, axis=0).astype(bf16)


def project_kernel(
    place_ref, blk0_ref, blk1_ref, blk2_ref, blk3_ref, ctx_ref, misc_ref,
    own_x, other_x, own_s, other_s,
    send_hbm, h_hbm, xb_hbm, sr_hbm, gate_hbm,
    send_ref, h_ref, xb_ref, sr_ref, gate_ref, conv_ref, mods_ref, edge_ref, sems,
):
    def store(i, src, dst):
        copy = pltpu.make_async_copy(src, dst, sems.at[i])
        copy.start()
        return copy

    core, at, tp = place_ref[0], place_ref[1], place_ref[2]
    blocks = (blk0_ref, blk1_ref, blk2_ref, blk3_ref)
    origin = [lax.rem(tp + 4 - s, 4) for s in range(4)]
    tails = [ref[OWN:, :].astype(f32) for ref in blocks]
    for s in range(4):

        def row(k, tail=tails[s]):
            return tail[1 + k // 16 : 2 + k // 16, (k % 16) * 128 : (k % 16 + 1) * 128]

        found = [row(i) + row(20 + i) + row(40 + i) for i in range(20)]
        found += [jnp.zeros((4, 128), f32)]
        mods_ref[pl.ds(pl.multiple_of(origin[s] * 24, 8), 24), :] = jnp.concatenate(found, axis=0)
    row8 = rows_of((8, D))
    before = sum(t * jnp.where(o == 0, 1.0, 0.0) for t, o in zip(tails, origin))
    after = sum(t * jnp.where(o == 3, 1.0, 0.0) for t, o in zip(tails, origin))
    edge_ref[...] = jnp.where(
        row8 == 0, before, jnp.where(row8 == 1, pltpu.roll(after, 1, 0), 0.0)
    )

    def inverse(ref, rows):
        squares = jnp.zeros((rows, 128), f32)
        for c in range(16):
            v = ref[:rows, c * 128 : (c + 1) * 128].astype(f32)
            squares = squares + v * v
        return lax.rsqrt(jnp.sum(squares, axis=1, keepdims=True) * (1.0 / D) + EPSILON)

    inv = [inverse(ref, OWN) for ref in blocks]
    inv_edge = inverse(edge_ref, 8)
    inv_ctx = inverse(ctx_ref, 8)
    for c in range(16):
        t, q = c // 4, c % 4
        cols = slice(c * 128, (c + 1) * 128)

        def mod(k, at=24 * t + q):
            return mods_ref[at + 4 * k : at + 4 * k + 1, :]

        gain = misc_ref[0:1, cols]
        shift, scale, cshift, cscale = mod(0), gain * (1.0 + mod(1)), mod(2), gain * (1.0 + mod(3))
        gate_ref[:, cols] = jnp.broadcast_to(mod(4), (8, 128))
        for s in range(4):
            h = blocks[s][:OWN, cols].astype(f32) * inv[s] * scale + shift
            h_ref[pl.ds(pl.multiple_of(origin[s] * OWN, OWN), OWN), cols] = h.astype(bf16)
        edge = edge_ref[:, cols] * inv_edge * scale + shift
        ctx = ctx_ref[:, cols].astype(f32) * inv_ctx * cscale + cshift
        h_ref[TOK:ROWS, cols] = jnp.concatenate([edge, ctx], axis=0).astype(bf16)
    stores = [store(0, h_ref, h_hbm), store(1, gate_ref, gate_hbm)]

    both = projected(h_ref, core, own_s, other_s, slice(0, STATE + 128))
    step = softplus(both[:TOK, STATE:])
    ctx_dt = both[TOK + 8 :, STATE:]
    rate = misc_ref[4:5, 0:128] + pltpu.roll(misc_ref[4:8, 0:128], HEADS, 1)[1:2]
    log_decay = -(rate * step)
    ri, ci = rows_of((TOK, TOK)), lanes((TOK, TOK))
    lower = jnp.where(ri >= ci, 1.0, 0.0).astype(f32)
    upper = jnp.where(ri <= ci, 1.0, 0.0).astype(f32)
    ahead = jnp.dot(lower, log_decay, preferred_element_type=f32, precision=HIGHEST)
    behind = jnp.dot(upper, log_decay, preferred_element_type=f32, precision=HIGHEST)
    run = jnp.where(ci < HEADS, ahead, behind)
    sr_ref[:, 0:128] = step
    sr_ref[:, 128:256] = run
    stores.append(store(2, sr_ref, sr_hbm))
    total = jnp.where(lanes((1, 128)) < HEADS, run[TOK - 1 : TOK], run[0:1])
    to_end = jnp.exp(total - run)

    before_ok, after_ok = ends(at)
    ctx_b = both[TOK + 8 :, :STATE]
    b_in = softened(both[:, :STATE], misc_ref, INNER, conv_ref, before_ok, after_ok)
    xb_ref[:, INNER:] = b_in
    p = projected(h_ref, core, own_x, other_x, slice(0, INNER))
    ctx_x = p[TOK + 8 :]
    x_in = softened(p, misc_ref, 0, conv_ref, before_ok, after_ok)
    xb_ref[:, :INNER] = x_in
    stores.append(store(3, xb_ref, xb_hbm))

    high = rounded(total)
    low = rounded(total - high)
    lane = lanes((8, 128))
    turned_b = [
        pltpu.roll(ctx_b, (64 - 16 * c) % 128, 1) if c != 4 else ctx_b for c in range(8)
    ]
    for head in range(HEADS):
        misc = jnp.zeros((8, 128), f32)
        for spot, table, col in (
            (80, ctx_dt, head), (81, ctx_dt, HEADS + head), (82, high, head), (83, low, head),
            (84, high, HEADS + head), (85, low, HEADS + head),
        ):
            misc = jnp.where(lane == spot, table[:, col : col + 1], misc)
        chunk = ctx_x[:, (head // 2) * 128 : (head // 2 + 1) * 128]
        if head % 2:
            chunk = pltpu.roll(chunk, HD, 1)
        misc = jnp.where(lane < HD, chunk, misc)
        for c in range(8):
            tile = jnp.where((lane >= 64) & (lane < 80), turned_b[c], misc)
            send_ref[head * 8 + c, 16:24, :] = tile.astype(bf16)

    left = ci < HD
    for q in range(4):
        sides = []
        for first in (0, HEADS):
            moved = rounded(x_in[:, q * 128 : (q + 1) * 128].astype(f32) * per_channel(step, first, q))
            ended = (moved * per_channel(to_end, first, q)).astype(bf16)
            sides.append(
                lax.dot_general(
                    b_in, ended, (((0,), (0,)), ((), ())), preferred_element_type=f32
                )
            )
        ahead, behind = sides
        for k, state in (
            (0, jnp.where(left, ahead, pltpu.roll(behind, HD, 1))),
            (1, jnp.where(left, pltpu.roll(ahead, HD, 1), behind)),
        ):
            head = 2 * q + k
            send_ref[head * 8 : head * 8 + 8, 0:16, :] = state.astype(bf16).reshape(8, 16, 128)
        part = pl.ds(16 * q, 16)
        stores.append(store(4 + q, send_ref.at[part], send_hbm.at[part]))
    for copy in stores:
        copy.wait()


def inside_kernel(
    place_ref, h_ref, own_z, other_z, own_s, other_s, xb_ref, sr_ref, misc_ref,
    y_ref, c_out_ref, z_ref, conv_ref,
):
    core, at = place_ref[0], place_ref[1]
    before_ok, after_ok = ends(at)
    p = projected(h_ref, core, own_s, other_s, slice(STATE + 128, 2 * STATE + 128))
    c_in = softened(p, misc_ref, INNER + STATE, conv_ref, before_ok, after_ok)
    c_out_ref[...] = c_in
    z_ref[...] = projected(h_ref, core, own_z, other_z, slice(0, INNER))[:TOK].astype(bf16)
    step, run = sr_ref[:, 0:128], sr_ref[:, 128:256]
    turned = run.T
    scores = lax.dot_general(
        c_in, xb_ref[:, INNER:], (((1,), (1,)), ((), ())), preferred_element_type=f32
    )
    ri, ci = rows_of((TOK, TOK)), lanes((TOK, TOK))
    for q in range(4):
        cols = slice(q * 128, (q + 1) * 128)
        x = xb_ref[:, cols].astype(f32)
        moved = jnp.concatenate(
            [(x * per_channel(step, first, q)).astype(bf16) for first in (0, HEADS)], axis=0
        )
        outs = []
        for head in (2 * q, 2 * q + 1):
            weights = []
            for first, kept in ((0, ri >= ci), (HEADS, ri <= ci)):
                k = first + head
                spread = run[:, k : k + 1] - turned[k : k + 1, :]
                decay = jnp.where(kept, jnp.exp(jnp.minimum(spread, 0.0)), 0.0)
                weights.append((scores * decay).astype(bf16))
            outs.append(
                jnp.dot(jnp.concatenate(weights, axis=1), moved, preferred_element_type=f32)
            )
        y_ref[:, cols] = jnp.where(ci < HD, outs[0], outs[1])


def owner_kernel(rate_ref, recv_ref, tap_ref, out_ref, pad_ref, held_ref):
    raw = recv_ref[:, 16:24, :].astype(f32).reshape(CTX, 128)
    pad_ref[0:8, :] = jnp.zeros((8, 128), f32)
    pad_ref[8 + CTX : 16 + CTX, :] = jnp.zeros((8, 128), f32)
    pad_ref[8 : 8 + CTX, :] = raw
    act = silu(
        pad_ref[7 : 7 + CTX, :] * tap_ref[0:1, :]
        + raw * tap_ref[1:2, :]
        + pad_ref[9 : 9 + CTX, :] * tap_ref[2:3, :]
    ).astype(bf16)
    lane = lanes((CTX, 128))
    left = lane < HD
    step = softplus(jnp.where(left, raw[:, 80:81], raw[:, 81:82]))
    rate = jnp.where(left, rate_ref[0], rate_ref[1])
    decay = -(rate * step)
    high = rounded(decay)
    mid = rounded(decay - high)
    spot = lane % 4
    parts = jnp.where(
        spot == 0, high, jnp.where(spot == 1, mid, jnp.where(spot == 2, decay - high - mid, 0.0))
    ).astype(bf16)
    earlier = jnp.where(lanes((CTX, CTX)) < rows_of((CTX, CTX)), 1.0, 0.0).astype(bf16)
    sums = jnp.dot(earlier, parts, preferred_element_type=f32)
    before_f = sums[:, 0:1] + sums[:, 1:2] + sums[:, 2:3]
    before_b = sums[:, 64:65] + sums[:, 65:66] + sums[:, 66:67]
    upto_f = before_f + decay[:, 0:1]
    later_f = jnp.minimum(upto_f[CTX - 1 :] - upto_f, 0.0)
    act_wide = act.astype(f32)
    moved = rounded(jnp.where(left, act_wide, pltpu.roll(act_wide, HD, 1)) * step)
    moved = moved * jnp.exp(jnp.where(left, later_f, before_b))
    top = rounded(moved)
    dims = (((0,), (0,)), ((), ()))
    start = lax.dot_general(act, top.astype(bf16), dims, preferred_element_type=f32)
    start = start + lax.dot_general(
        act, (moved - top).astype(bf16), dims, preferred_element_type=f32
    )
    state = start[64:80]
    grow = jnp.exp(
        jnp.where(left, raw[:, 82:83] + raw[:, 83:84], raw[:, 84:85] + raw[:, 85:86])
    ).reshape(NSP, 8, 128)
    left8, left16 = lanes((8, 128)) < HD, lanes((16, 128)) < HD
    for k in range(NSP):
        m = NSP - 1 - k
        held_ref[k, :, 0:HD] = state[:, 0:HD]
        held_ref[m, :, HD:128] = state[:, HD:128]
        fresh = jnp.where(left16, recv_ref[k, 0:16, :].astype(f32), recv_ref[m, 0:16, :].astype(f32))
        growth = jnp.where(left8, grow[k], grow[m])
        state = state * jnp.concatenate([growth, growth], axis=0) + fresh
    out_ref[...] = held_ref[...].astype(bf16)


def output_kernel(
    place_ref, state_ref, gain_ref, c_ref, sr_ref, z_ref, y_hbm, own_hbm, other_hbm,
    out_ref, ny_ref, y_ref, own_ref, other_ref, sems,
):
    loads = [
        pltpu.make_async_copy(src, dst, sems.at[i])
        for i, (src, dst) in enumerate(
            ((y_hbm, y_ref), (own_hbm, own_ref), (other_hbm, other_ref))
        )
    ]
    for copy in loads:
        copy.start()
    core = place_ref[0]
    growth = jnp.exp(sr_ref[:, 128:256])
    c_in = c_ref[...]
    left = lanes((TOK, 128)) < HD
    squares = jnp.zeros((TOK, 128), f32)
    gated = []
    for q in range(4):
        cols = slice(q * 128, (q + 1) * 128)
        sums = []
        for head in (2 * q, 2 * q + 1):
            state = state_ref[head * 8 : head * 8 + 8].reshape(STATE, 128)
            both = jnp.dot(c_in, state, preferred_element_type=f32) * jnp.where(
                left, growth[:, head : head + 1], growth[:, HEADS + head : HEADS + head + 1]
            )
            sums.append(both + pltpu.roll(both, HD, 1))
        if q == 0:
            loads[0].wait()
        y = y_ref[:, cols] + jnp.where(left, sums[0], sums[1])
        g = y * silu(z_ref[:, cols].astype(f32))
        squares = squares + g * g
        gated.append(g)
    inv = lax.rsqrt(jnp.sum(squares, axis=1, keepdims=True) * (1.0 / INNER) + EPSILON)
    for q in range(4):
        cols = slice(q * 128, (q + 1) * 128)
        ny_ref[:, cols] = (gated[q] * inv * gain_ref[0:1, cols].astype(f32)).astype(bf16)
    half = INNER // 2
    mine = ny_ref[:, pl.ds(pl.multiple_of(core * half, half), half)]
    theirs = ny_ref[:, pl.ds(pl.multiple_of((1 - core) * half, half), half)]
    for copy in loads[1:]:
        copy.wait()
    for n in range(4):
        cols = slice(n * 512, (n + 1) * 512)
        out = jnp.dot(mine, own_ref[:, cols], preferred_element_type=f32)
        out = out + jnp.dot(theirs, other_ref[:, cols], preferred_element_type=f32)
        out_ref[:, cols] = out.astype(bf16)


def sum_kernel(tile_ref, gate_ref, out_hbm, out_ref, sem):
    total = tile_ref[0].astype(f32)
    for t in range(1, 4):
        total = total + tile_ref[t].astype(f32)
    out_ref[...] = (gate_ref[0:1, :] * total).astype(bf16)
    copy = pltpu.make_async_copy(out_ref, out_hbm, sem)
    copy.start()
    copy.wait()


def call(kernel, out_shape, n_args, smem, scratch=(), hbm=(), hbm_out=False, flops=10**8):
    space = {i: pltpu.SMEM for i in smem} | {i: pltpu.HBM for i in hbm}
    in_specs = [pl.BlockSpec(memory_space=space.get(i, pltpu.VMEM)) for i in range(n_args)]
    out = pl.BlockSpec(memory_space=pltpu.HBM if hbm_out else pltpu.VMEM)
    many = isinstance(out_shape, (list, tuple))
    return pl.pallas_call(
        kernel,
        out_shape=out_shape,
        in_specs=in_specs,
        out_specs=[out] * len(out_shape) if many else out,
        scratch_shapes=list(scratch),
        compiler_params=pltpu.CompilerParams(vmem_limit_bytes=30 * 2**20),
        cost_estimate=pl.CostEstimate(flops=flops, bytes_accessed=2**20, transcendentals=0),
        interpret=INTERPRET,
    )


def pack_call(*args):
    return call(pack_kernel, jax.ShapeDtypeStruct((OWN + 8, D), bf16), 3, ())(*args)


def project_call(*args):
    outs = [
        ((NSP, 24, 128), bf16), ((ROWS, D), bf16), ((TOK, XB), bf16), ((TOK, 256), f32),
        ((8, D), f32),
    ]
    return call(
        project_kernel,
        [pltpu.HBM(*o) for o in outs],
        11,
        (0,),
        [
            *(pltpu.VMEM(*o) for o in outs),
            pltpu.VMEM((TOK + 16, INNER), f32),
            pltpu.VMEM((96, 128), f32),
            pltpu.VMEM((8, D), f32),
            pltpu.SemaphoreType.DMA((8,)),
        ],
        hbm_out=True,
    )(*args)


def inside_call(*args):
    return call(
        inside_kernel,
        [
            jax.ShapeDtypeStruct((TOK, INNER), f32),
            jax.ShapeDtypeStruct((TOK, STATE), bf16),
            jax.ShapeDtypeStruct((TOK, INNER), bf16),
        ],
        9,
        (0,),
        [pltpu.VMEM((TOK + 16, STATE), f32)],
    )(*args)


def owner_call(*args):
    return call(
        owner_kernel,
        jax.ShapeDtypeStruct((NSP, 16, 128), bf16),
        3,
        (0,),
        [pltpu.VMEM((CTX + 16, 128), f32), pltpu.VMEM((NSP, 16, 128), f32)],
    )(*args)


def output_call(*args):
    return call(
        output_kernel,
        jax.ShapeDtypeStruct((TOK, D), bf16),
        9,
        (0,),
        [
            pltpu.VMEM((TOK, INNER), bf16),
            pltpu.VMEM((TOK, INNER), f32),
            pltpu.VMEM((INNER // 2, D), bf16),
            pltpu.VMEM((INNER // 2, D), bf16),
            pltpu.SemaphoreType.DMA((3,)),
        ],
        hbm=(6, 7, 8),
    )(*args[:6], *(pltpu.with_memory_space_constraint(a, pltpu.HBM) for a in args[6:]))


def sum_call(*args):
    return call(
        sum_kernel,
        pltpu.HBM((OWN, D), bf16),
        2,
        (),
        [pltpu.VMEM((OWN, D), bf16), pltpu.SemaphoreType.DMA(())],
        hbm_out=True,
    )(*args)


def swapped(x):
    return lax.ppermute(x, "dp", [(0, 1), (1, 0)])


def exchanged(x, axes):
    return lax.all_to_all(x, axes, 0, 0, tiled=True)


def turned(by):
    return [(i, (i + by) % 4) for i in range(4)]


def sent_to_all(x, peers, axes):
    return exchanged(jnp.broadcast_to(x[None], (peers, *x.shape)), axes)


def small_weights(w_b, w_c, w_dt):
    steps = jnp.concatenate([w_dt[0], w_dt[1]], axis=1)
    steps = jnp.pad(steps, ((0, 0), (0, 128 - steps.shape[1])))
    return jnp.concatenate([w_b, steps, w_c], axis=1)


def packed_vectors(norm_gain, conv_x, conv_b, conv_c, decay_rate):
    def placed(v, row, col):
        v = v.astype(f32)
        return jnp.pad(v, ((row, 8 - row - v.shape[0]), (col, D - col - v.shape[1])))

    return (
        placed(norm_gain[None], 0, 0)
        + placed(conv_x, 1, 0)
        + placed(conv_b, 1, INNER)
        + placed(conv_c, 1, XB)
        + placed(decay_rate, 4, 0)
    )


def owner_taps(conv_x, conv_b, at):
    of_x = lax.dynamic_slice_in_dim(conv_x, at // 8 * HD, HD, 1)
    of_b = lax.dynamic_slice_in_dim(conv_b, at % 8 * 16, 16, 1)
    both = jnp.concatenate([of_x, of_b], axis=1).astype(f32)
    return jnp.pad(both, ((0, 0), (0, 128 - HD - 16)))


def shards(
    latent, condition, context, context_source, mod_weight, norm_gain,
    w_x, w_b, w_c, w_z, w_dt, conv_x, conv_b, conv_c, decay_rate, out_gain, w_out,
):
    at = lax.axis_index(SP)
    core = lax.axis_index("dp")
    tp = lax.axis_index("tp")
    place = jnp.stack([core, at, tp]).astype(jnp.int32)
    row_count = mod_weight.shape[1]

    rows = latent[0]
    edge = jnp.where(tp == 3, rows[OWN - 1 :], rows[:1])
    pairs = [(4 * i + 3, 4 * i + 4) for i in range(NSP - 1)]
    pairs += [(j, i) for i, j in pairs]
    halo = lax.ppermute(edge, ALL, pairs)

    act = jnp.stack(
        [silu(condition[0].astype(f32)), silu(context_source.astype(f32))]
    ).astype(bf16)
    act = lax.dynamic_slice_in_dim(act, at * row_count, row_count, 1)
    part = jnp.einsum("ar,krc->akc", act, mod_weight, preferred_element_type=f32)
    part = jnp.stack([part[0, 0], part[0, 1], part[1, 0], part[1, 1], part[0, 2]])
    part = part.reshape(20, 128)
    part = sent_to_all(part, 8, "sp_0")
    part = jnp.sum(part, axis=0)
    part = sent_to_all(part, 8, "sp_1")
    blocks = [pack_call(part, rows, halo)]
    for s in (1, 2, 3):
        blocks.append(lax.ppermute(blocks[0], "tp", turned(s)))

    small = small_weights(w_b, w_c, w_dt)
    other_x = swapped(w_x)
    other_small = swapped(small)
    other_z = swapped(w_z)
    other_out = swapped(w_out)

    misc = packed_vectors(norm_gain, conv_x, conv_b, conv_c, decay_rate)
    own_taps = owner_taps(conv_x, conv_b, at)
    own_rates = lax.dynamic_slice_in_dim(decay_rate, at // 8, 1, 1)[:, 0]

    send, h, xb, sr, gate = project_call(
        place, *blocks, context[0], misc, w_x, other_x, small, other_small
    )
    received = exchanged(send, SP)
    y_in, c_in, z_in = inside_call(
        place, h, w_z, other_z, small, other_small, xb, sr, misc
    )
    entering = owner_call(own_rates, received, own_taps)
    states = exchanged(entering, SP)
    partial = output_call(
        place, states, out_gain[None], c_in, sr, z_in, y_in, w_out, other_out
    )
    tiles = exchanged(partial.reshape(4, OWN, D), "tp")
    return sum_call(tiles, gate)[None]


def solution(mesh):
    torus = Mesh(
        mesh.devices.reshape(8, 8, mesh.shape["tp"], mesh.shape["dp"]), ("sp_0", "sp_1", "tp", "dp")
    )
    sp_tp = ("sp_0", "sp_1", "tp")
    placed = (
        P("dp", sp_tp, None),
        P("dp", None),
        P("dp", SP, None),
        P(),
        P(None, SP, "tp"),
        P(),
        P("dp", "tp"),
        P("dp", "tp"),
        P("dp", "tp"),
        P("dp", "tp"),
        P(None, "dp", "tp"),
        P(None, "tp"),
        P(None, "tp"),
        P(None, "tp"),
        P(None, "tp"),
        P("tp"),
        P(("tp", "dp"), None),
    )

    return jax.shard_map(
        shards, mesh=torus, in_specs=placed, out_specs=P("dp", sp_tp, None), check_vma=False
    )
```

```python
import jax
import jax.numpy as jnp
from jax import lax
from jax.experimental import pallas as pl
from jax.experimental.pallas import tpu as pltpu
from jax.sharding import Mesh
from jax.sharding import PartitionSpec as P


SP = ("sp_0", "sp_1")
ALL = ("sp_0", "sp_1", "tp")
EPSILON = 1e-06
INTERPRET = False

D = 2048
HALF = D // 2
TOK = 128
OWN = 32
INNER = 512
HEADS = 8
HD = 64
STATE = 128
NSP = 64
CTX_DEV = 8
CTX = NSP * CTX_DEV
XB = INNER + STATE
ROWS = TOK + 16

f32 = jnp.float32
bf16 = jnp.bfloat16
HIGHEST = lax.Precision.HIGHEST


def silu(v):
    return v / (1.0 + jnp.exp(-v))


def softplus(v):
    return jnp.maximum(v, 0.0) + jnp.log1p(jnp.exp(-jnp.abs(v)))


def rounded(v):
    return v.astype(bf16).astype(f32)


def lanes(shape):
    return lax.broadcasted_iota(jnp.int32, shape, 1)


def rows_of(shape):
    return lax.broadcasted_iota(jnp.int32, shape, 0)


def per_channel(table, first, chunk):
    left = table[:, first + 2 * chunk : first + 2 * chunk + 1]
    right = table[:, first + 2 * chunk + 1 : first + 2 * chunk + 2]
    shape = (table.shape[0], 128)
    return jnp.where(lanes(shape) < HD, left, right)


def softened(p, taps, first_col, conv_ref, before_ok, after_ok):
    width = p.shape[1]
    cols = slice(first_col, first_col + width)
    conv_ref[8 : 8 + TOK, :width] = p[:TOK]
    conv_ref[0:8, :width] = jnp.broadcast_to(p[TOK : TOK + 1] * before_ok, (8, width))
    conv_ref[8 + TOK : 16 + TOK, :width] = jnp.broadcast_to(
        p[TOK + 1 : TOK + 2] * after_ok, (8, width)
    )
    summed = (
        conv_ref[7 : 7 + TOK, :width] * taps[1:2, cols]
        + conv_ref[8 : 8 + TOK, :width] * taps[2:3, cols]
        + conv_ref[9 : 9 + TOK, :width] * taps[3:4, cols]
    )
    return silu(summed).astype(bf16)


def ends(at):
    return jnp.where(at > 0, 1.0, 0.0), jnp.where(at < NSP - 1, 1.0, 0.0)


def projected(h_ref, core, own_ref, other_ref, cols):
    mine = pl.multiple_of(core * HALF, HALF)
    theirs = pl.multiple_of((1 - core) * HALF, HALF)
    out = jnp.dot(h_ref[:, pl.ds(mine, HALF)], own_ref[:, cols], preferred_element_type=f32)
    return rounded(
        out
        + jnp.dot(h_ref[:, pl.ds(theirs, HALF)], other_ref[:, cols], preferred_element_type=f32)
    )


def pack_kernel(part_ref, rows_ref, halo_ref, out_ref):
    out_ref[0:OWN, :] = rows_ref[...]
    total = part_ref[0]
    for y in range(1, 8):
        total = total + part_ref[y]
    high = rounded(total)
    mid = rounded(total - high)
    parts = [high, mid, total - high - mid]
    zero = jnp.zeros((1, 128), f32)
    for m in range(16):
        cols = slice(m * 128, (m + 1) * 128)
        rows = [halo_ref[0:1, cols].astype(f32)]
        for r in range(7):
            k = r * 16 + m
            rows.append(parts[k // 20][k % 20 : k % 20 + 1] if k < 60 else zero)
        out_ref[OWN:, cols] = jnp.concatenate(rows, axis=0).astype(bf16)


def project_kernel(
    place_ref, blk0_ref, blk1_ref, blk2_ref, blk3_ref, ctx_ref, misc_ref,
    own_x, other_x, own_s, other_s,
    send_hbm, h_hbm, xb_hbm, sr_hbm, gate_hbm,
    send_ref, h_ref, xb_ref, sr_ref, gate_ref, conv_ref, mods_ref, edge_ref, sems,
):
    def store(i, src, dst):
        copy = pltpu.make_async_copy(src, dst, sems.at[i])
        copy.start()
        return copy

    core, at, tp = place_ref[0], place_ref[1], place_ref[2]
    blocks = (blk0_ref, blk1_ref, blk2_ref, blk3_ref)
    origin = [lax.rem(tp + 4 - s, 4) for s in range(4)]
    tails = [ref[OWN:, :].astype(f32) for ref in blocks]
    for s in range(4):

        def row(k, tail=tails[s]):
            return tail[1 + k // 16 : 2 + k // 16, (k % 16) * 128 : (k % 16 + 1) * 128]

        found = [row(i) + row(20 + i) + row(40 + i) for i in range(20)]
        found += [jnp.zeros((4, 128), f32)]
        mods_ref[pl.ds(pl.multiple_of(origin[s] * 24, 8), 24), :] = jnp.concatenate(found, axis=0)
    row8 = rows_of((8, D))
    before = sum(t * jnp.where(o == 0, 1.0, 0.0) for t, o in zip(tails, origin))
    after = sum(t * jnp.where(o == 3, 1.0, 0.0) for t, o in zip(tails, origin))
    edge_ref[...] = jnp.where(
        row8 == 0, before, jnp.where(row8 == 1, pltpu.roll(after, 1, 0), 0.0)
    )

    def inverse(ref, rows):
        squares = jnp.zeros((rows, 128), f32)
        for c in range(16):
            v = ref[:rows, c * 128 : (c + 1) * 128].astype(f32)
            squares = squares + v * v
        return lax.rsqrt(jnp.sum(squares, axis=1, keepdims=True) * (1.0 / D) + EPSILON)

    inv = [inverse(ref, OWN) for ref in blocks]
    inv_edge = inverse(edge_ref, 8)
    inv_ctx = inverse(ctx_ref, 8)
    for c in range(16):
        t, q = c // 4, c % 4
        cols = slice(c * 128, (c + 1) * 128)

        def mod(k, at=24 * t + q):
            return mods_ref[at + 4 * k : at + 4 * k + 1, :]

        gain = misc_ref[0:1, cols]
        shift, scale, cshift, cscale = mod(0), gain * (1.0 + mod(1)), mod(2), gain * (1.0 + mod(3))
        gate_ref[:, cols] = jnp.broadcast_to(mod(4), (8, 128))
        for s in range(4):
            h = blocks[s][:OWN, cols].astype(f32) * inv[s] * scale + shift
            h_ref[pl.ds(pl.multiple_of(origin[s] * OWN, OWN), OWN), cols] = h.astype(bf16)
        edge = edge_ref[:, cols] * inv_edge * scale + shift
        ctx = ctx_ref[:, cols].astype(f32) * inv_ctx * cscale + cshift
        h_ref[TOK:ROWS, cols] = jnp.concatenate([edge, ctx], axis=0).astype(bf16)
    stores = [store(0, h_ref, h_hbm), store(1, gate_ref, gate_hbm)]

    both = projected(h_ref, core, own_s, other_s, slice(0, STATE + 128))
    step = softplus(both[:TOK, STATE:])
    ctx_dt = both[TOK + 8 :, STATE:]
    rate = misc_ref[4:5, 0:128] + pltpu.roll(misc_ref[4:8, 0:128], HEADS, 1)[1:2]
    log_decay = -(rate * step)
    ri, ci = rows_of((TOK, TOK)), lanes((TOK, TOK))
    lower = jnp.where(ri >= ci, 1.0, 0.0).astype(f32)
    upper = jnp.where(ri <= ci, 1.0, 0.0).astype(f32)
    ahead = jnp.dot(lower, log_decay, preferred_element_type=f32, precision=HIGHEST)
    behind = jnp.dot(upper, log_decay, preferred_element_type=f32, precision=HIGHEST)
    run = jnp.where(ci < HEADS, ahead, behind)
    sr_ref[:, 0:128] = step
    sr_ref[:, 128:256] = run
    stores.append(store(2, sr_ref, sr_hbm))
    total = jnp.where(lanes((1, 128)) < HEADS, run[TOK - 1 : TOK], run[0:1])
    to_end = jnp.exp(total - run)

    before_ok, after_ok = ends(at)
    ctx_b = both[TOK + 8 :, :STATE]
    b_in = softened(both[:, :STATE], misc_ref, INNER, conv_ref, before_ok, after_ok)
    xb_ref[:, INNER:] = b_in
    p = projected(h_ref, core, own_x, other_x, slice(0, INNER))
    ctx_x = p[TOK + 8 :]
    x_in = softened(p, misc_ref, 0, conv_ref, before_ok, after_ok)
    xb_ref[:, :INNER] = x_in
    stores.append(store(3, xb_ref, xb_hbm))

    high = rounded(total)
    low = rounded(total - high)
    lane = lanes((8, 128))
    turned_b = [
        pltpu.roll(ctx_b, (64 - 16 * c) % 128, 1) if c != 4 else ctx_b for c in range(8)
    ]
    for head in range(HEADS):
        misc = jnp.zeros((8, 128), f32)
        for spot, table, col in (
            (80, ctx_dt, head), (81, ctx_dt, HEADS + head), (82, high, head), (83, low, head),
            (84, high, HEADS + head), (85, low, HEADS + head),
        ):
            misc = jnp.where(lane == spot, table[:, col : col + 1], misc)
        chunk = ctx_x[:, (head // 2) * 128 : (head // 2 + 1) * 128]
        if head % 2:
            chunk = pltpu.roll(chunk, HD, 1)
        misc = jnp.where(lane < HD, chunk, misc)
        for c in range(8):
            tile = jnp.where((lane >= 64) & (lane < 80), turned_b[c], misc)
            send_ref[head * 8 + c, 16:24, :] = tile.astype(bf16)

    left = ci < HD
    for q in range(4):
        sides = []
        for first in (0, HEADS):
            moved = rounded(x_in[:, q * 128 : (q + 1) * 128].astype(f32) * per_channel(step, first, q))
            ended = (moved * per_channel(to_end, first, q)).astype(bf16)
            sides.append(
                lax.dot_general(
                    b_in, ended, (((0,), (0,)), ((), ())), preferred_element_type=f32
                )
            )
        ahead, behind = sides
        for k, state in (
            (0, jnp.where(left, ahead, pltpu.roll(behind, HD, 1))),
            (1, jnp.where(left, pltpu.roll(ahead, HD, 1), behind)),
        ):
            head = 2 * q + k
            send_ref[head * 8 : head * 8 + 8, 0:16, :] = state.astype(bf16).reshape(8, 16, 128)
        part = pl.ds(16 * q, 16)
        stores.append(store(4 + q, send_ref.at[part], send_hbm.at[part]))
    for copy in stores:
        copy.wait()


def inside_kernel(
    place_ref, h_ref, own_z, other_z, own_s, other_s, xb_ref, sr_ref, misc_ref,
    y_ref, c_out_ref, z_ref, conv_ref,
):
    core, at = place_ref[0], place_ref[1]
    before_ok, after_ok = ends(at)
    p = projected(h_ref, core, own_s, other_s, slice(STATE + 128, 2 * STATE + 128))
    c_in = softened(p, misc_ref, INNER + STATE, conv_ref, before_ok, after_ok)
    c_out_ref[...] = c_in
    z_ref[...] = projected(h_ref, core, own_z, other_z, slice(0, INNER))[:TOK].astype(bf16)
    step, run = sr_ref[:, 0:128], sr_ref[:, 128:256]
    turned = run.T
    scores = lax.dot_general(
        c_in, xb_ref[:, INNER:], (((1,), (1,)), ((), ())), preferred_element_type=f32
    )
    ri, ci = rows_of((TOK, TOK)), lanes((TOK, TOK))
    for q in range(4):
        cols = slice(q * 128, (q + 1) * 128)
        x = xb_ref[:, cols].astype(f32)
        moved = jnp.concatenate(
            [(x * per_channel(step, first, q)).astype(bf16) for first in (0, HEADS)], axis=0
        )
        outs = []
        for head in (2 * q, 2 * q + 1):
            weights = []
            for first, kept in ((0, ri >= ci), (HEADS, ri <= ci)):
                k = first + head
                spread = run[:, k : k + 1] - turned[k : k + 1, :]
                decay = jnp.where(kept, jnp.exp(jnp.minimum(spread, 0.0)), 0.0)
                weights.append((scores * decay).astype(bf16))
            outs.append(
                jnp.dot(jnp.concatenate(weights, axis=1), moved, preferred_element_type=f32)
            )
        y_ref[:, cols] = jnp.where(ci < HD, outs[0], outs[1])


def owner_kernel(rate_ref, recv_ref, tap_ref, out_ref, pad_ref, held_ref):
    raw = recv_ref[:, 16:24, :].astype(f32).reshape(CTX, 128)
    pad_ref[0:8, :] = jnp.zeros((8, 128), f32)
    pad_ref[8 + CTX : 16 + CTX, :] = jnp.zeros((8, 128), f32)
    pad_ref[8 : 8 + CTX, :] = raw
    act = silu(
        pad_ref[7 : 7 + CTX, :] * tap_ref[0:1, :]
        + raw * tap_ref[1:2, :]
        + pad_ref[9 : 9 + CTX, :] * tap_ref[2:3, :]
    ).astype(bf16)
    lane = lanes((CTX, 128))
    left = lane < HD
    step = softplus(jnp.where(left, raw[:, 80:81], raw[:, 81:82]))
    rate = jnp.where(left, rate_ref[0], rate_ref[1])
    decay = -(rate * step)
    high = rounded(decay)
    parts = jnp.concatenate([high.astype(bf16), (decay - high).astype(bf16)], axis=1)
    earlier = jnp.where(lanes((CTX, CTX)) < rows_of((CTX, CTX)), 1.0, 0.0).astype(bf16)
    sums = jnp.dot(earlier, parts, preferred_element_type=f32)
    before = sums[:, :128] + sums[:, 128:]
    upto = before + decay
    later = jnp.minimum(upto[CTX - 1 :] - upto, 0.0)
    act_wide = act.astype(f32)
    moved = rounded(jnp.where(left, act_wide, pltpu.roll(act_wide, HD, 1)) * step)
    moved = moved * jnp.exp(jnp.where(left, later, before))
    top = rounded(moved)
    dims = (((0,), (0,)), ((), ()))
    start = lax.dot_general(act, top.astype(bf16), dims, preferred_element_type=f32)
    start = start + lax.dot_general(
        act, (moved - top).astype(bf16), dims, preferred_element_type=f32
    )
    state = start[64:80]
    grow = jnp.exp(
        jnp.where(left, raw[:, 82:83] + raw[:, 83:84], raw[:, 84:85] + raw[:, 85:86])
    ).reshape(NSP, 8, 128)
    left8, left16 = lanes((8, 128)) < HD, lanes((16, 128)) < HD
    for k in range(NSP):
        m = NSP - 1 - k
        held_ref[k, :, 0:HD] = state[:, 0:HD]
        held_ref[m, :, HD:128] = state[:, HD:128]
        fresh = jnp.where(left16, recv_ref[k, 0:16, :].astype(f32), recv_ref[m, 0:16, :].astype(f32))
        growth = jnp.where(left8, grow[k], grow[m])
        state = state * jnp.concatenate([growth, growth], axis=0) + fresh
    out_ref[...] = held_ref[...].astype(bf16)


def output_kernel(
    place_ref, state_ref, gain_ref, c_ref, sr_ref, z_ref, y_hbm, own_hbm, other_hbm,
    out_ref, ny_ref, y_ref, own_ref, other_ref, sems,
):
    loads = [
        pltpu.make_async_copy(src, dst, sems.at[i])
        for i, (src, dst) in enumerate(
            ((y_hbm, y_ref), (own_hbm, own_ref), (other_hbm, other_ref))
        )
    ]
    for copy in loads:
        copy.start()
    core = place_ref[0]
    growth = jnp.exp(sr_ref[:, 128:256])
    c_in = c_ref[...]
    left = lanes((TOK, 128)) < HD
    squares = jnp.zeros((TOK, 128), f32)
    gated = []
    for q in range(4):
        cols = slice(q * 128, (q + 1) * 128)
        sums = []
        for head in (2 * q, 2 * q + 1):
            state = state_ref[head * 8 : head * 8 + 8].reshape(STATE, 128)
            both = jnp.dot(c_in, state, preferred_element_type=f32) * jnp.where(
                left, growth[:, head : head + 1], growth[:, HEADS + head : HEADS + head + 1]
            )
            sums.append(both + pltpu.roll(both, HD, 1))
        if q == 0:
            loads[0].wait()
        y = y_ref[:, cols] + jnp.where(left, sums[0], sums[1])
        g = y * silu(z_ref[:, cols].astype(f32))
        squares = squares + g * g
        gated.append(g)
    inv = lax.rsqrt(jnp.sum(squares, axis=1, keepdims=True) * (1.0 / INNER) + EPSILON)
    for q in range(4):
        cols = slice(q * 128, (q + 1) * 128)
        ny_ref[:, cols] = (gated[q] * inv * gain_ref[0:1, cols].astype(f32)).astype(bf16)
    half = INNER // 2
    mine = ny_ref[:, pl.ds(pl.multiple_of(core * half, half), half)]
    theirs = ny_ref[:, pl.ds(pl.multiple_of((1 - core) * half, half), half)]
    for copy in loads[1:]:
        copy.wait()
    for n in range(4):
        cols = slice(n * 512, (n + 1) * 512)
        out = jnp.dot(mine, own_ref[:, cols], preferred_element_type=f32)
        out = out + jnp.dot(theirs, other_ref[:, cols], preferred_element_type=f32)
        out_ref[:, cols] = out.astype(bf16)


def sum_kernel(tile_ref, gate_ref, out_hbm, out_ref, sem):
    total = tile_ref[0].astype(f32)
    for t in range(1, 4):
        total = total + tile_ref[t].astype(f32)
    out_ref[...] = (gate_ref[0:1, :] * total).astype(bf16)
    copy = pltpu.make_async_copy(out_ref, out_hbm, sem)
    copy.start()
    copy.wait()


def call(kernel, out_shape, n_args, smem, scratch=(), hbm=(), hbm_out=False, flops=10**8):
    space = {i: pltpu.SMEM for i in smem} | {i: pltpu.HBM for i in hbm}
    in_specs = [pl.BlockSpec(memory_space=space.get(i, pltpu.VMEM)) for i in range(n_args)]
    out = pl.BlockSpec(memory_space=pltpu.HBM if hbm_out else pltpu.VMEM)
    many = isinstance(out_shape, (list, tuple))
    return pl.pallas_call(
        kernel,
        out_shape=out_shape,
        in_specs=in_specs,
        out_specs=[out] * len(out_shape) if many else out,
        scratch_shapes=list(scratch),
        compiler_params=pltpu.CompilerParams(vmem_limit_bytes=30 * 2**20),
        cost_estimate=pl.CostEstimate(flops=flops, bytes_accessed=2**20, transcendentals=0),
        interpret=INTERPRET,
    )


def pack_call(*args):
    return call(pack_kernel, jax.ShapeDtypeStruct((OWN + 8, D), bf16), 3, ())(*args)


def project_call(*args):
    outs = [
        ((NSP, 24, 128), bf16), ((ROWS, D), bf16), ((TOK, XB), bf16), ((TOK, 256), f32),
        ((8, D), f32),
    ]
    return call(
        project_kernel,
        [pltpu.HBM(*o) for o in outs],
        11,
        (0,),
        [
            *(pltpu.VMEM(*o) for o in outs),
            pltpu.VMEM((TOK + 16, INNER), f32),
            pltpu.VMEM((96, 128), f32),
            pltpu.VMEM((8, D), f32),
            pltpu.SemaphoreType.DMA((8,)),
        ],
        hbm_out=True,
    )(*args)


def inside_call(*args):
    return call(
        inside_kernel,
        [
            jax.ShapeDtypeStruct((TOK, INNER), f32),
            jax.ShapeDtypeStruct((TOK, STATE), bf16),
            jax.ShapeDtypeStruct((TOK, INNER), bf16),
        ],
        9,
        (0,),
        [pltpu.VMEM((TOK + 16, STATE), f32)],
    )(*args)


def owner_call(*args):
    return call(
        owner_kernel,
        jax.ShapeDtypeStruct((NSP, 16, 128), bf16),
        3,
        (0,),
        [pltpu.VMEM((CTX + 16, 128), f32), pltpu.VMEM((NSP, 16, 128), f32)],
    )(*args)


def output_call(*args):
    return call(
        output_kernel,
        jax.ShapeDtypeStruct((TOK, D), bf16),
        9,
        (0,),
        [
            pltpu.VMEM((TOK, INNER), bf16),
            pltpu.VMEM((TOK, INNER), f32),
            pltpu.VMEM((INNER // 2, D), bf16),
            pltpu.VMEM((INNER // 2, D), bf16),
            pltpu.SemaphoreType.DMA((3,)),
        ],
        hbm=(6, 7, 8),
    )(*args[:6], *(pltpu.with_memory_space_constraint(a, pltpu.HBM) for a in args[6:]))


def sum_call(*args):
    return call(
        sum_kernel,
        pltpu.HBM((OWN, D), bf16),
        2,
        (),
        [pltpu.VMEM((OWN, D), bf16), pltpu.SemaphoreType.DMA(())],
        hbm_out=True,
    )(*args)


def swapped(x):
    return lax.ppermute(x, "dp", [(0, 1), (1, 0)])


def exchanged(x, axes):
    return lax.all_to_all(x, axes, 0, 0, tiled=True)


def turned(by):
    return [(i, (i + by) % 4) for i in range(4)]


def sent_to_all(x, peers, axes):
    return exchanged(jnp.broadcast_to(x[None], (peers, *x.shape)), axes)


def small_weights(w_b, w_c, w_dt):
    steps = jnp.concatenate([w_dt[0], w_dt[1]], axis=1)
    steps = jnp.pad(steps, ((0, 0), (0, 128 - steps.shape[1])))
    return jnp.concatenate([w_b, steps, w_c], axis=1)


def packed_vectors(norm_gain, conv_x, conv_b, conv_c, decay_rate):
    def placed(v, row, col):
        v = v.astype(f32)
        return jnp.pad(v, ((row, 8 - row - v.shape[0]), (col, D - col - v.shape[1])))

    return (
        placed(norm_gain[None], 0, 0)
        + placed(conv_x, 1, 0)
        + placed(conv_b, 1, INNER)
        + placed(conv_c, 1, XB)
        + placed(decay_rate, 4, 0)
    )


def owner_taps(conv_x, conv_b, at):
    of_x = lax.dynamic_slice_in_dim(conv_x, at // 8 * HD, HD, 1)
    of_b = lax.dynamic_slice_in_dim(conv_b, at % 8 * 16, 16, 1)
    both = jnp.concatenate([of_x, of_b], axis=1).astype(f32)
    return jnp.pad(both, ((0, 0), (0, 128 - HD - 16)))


def shards(
    latent, condition, context, context_source, mod_weight, norm_gain,
    w_x, w_b, w_c, w_z, w_dt, conv_x, conv_b, conv_c, decay_rate, out_gain, w_out,
):
    at = lax.axis_index(SP)
    core = lax.axis_index("dp")
    tp = lax.axis_index("tp")
    place = jnp.stack([core, at, tp]).astype(jnp.int32)
    row_count = mod_weight.shape[1]

    rows = latent[0]
    edge = jnp.where(tp == 3, rows[OWN - 1 :], rows[:1])
    pairs = [(4 * i + 3, 4 * i + 4) for i in range(NSP - 1)]
    pairs += [(j, i) for i, j in pairs]
    halo = lax.ppermute(edge, ALL, pairs)

    act = jnp.stack(
        [silu(condition[0].astype(f32)), silu(context_source.astype(f32))]
    ).astype(bf16)
    act = lax.dynamic_slice_in_dim(act, at * row_count, row_count, 1)
    part = jnp.einsum("ar,krc->akc", act, mod_weight, preferred_element_type=f32)
    part = jnp.stack([part[0, 0], part[0, 1], part[1, 0], part[1, 1], part[0, 2]])
    part = part.reshape(20, 128)
    part = sent_to_all(part, 8, "sp_0")
    part = jnp.sum(part, axis=0)
    part = sent_to_all(part, 8, "sp_1")
    blocks = [pack_call(part, rows, halo)]
    for s in (1, 2, 3):
        blocks.append(lax.ppermute(blocks[0], "tp", turned(s)))

    small = small_weights(w_b, w_c, w_dt)
    other_x = swapped(w_x)
    other_small = swapped(small)
    other_z = swapped(w_z)
    other_out = swapped(w_out)

    misc = packed_vectors(norm_gain, conv_x, conv_b, conv_c, decay_rate)
    own_taps = owner_taps(conv_x, conv_b, at)
    own_rates = lax.dynamic_slice_in_dim(decay_rate, at // 8, 1, 1)[:, 0]

    send, h, xb, sr, gate = project_call(
        place, *blocks, context[0], misc, w_x, other_x, small, other_small
    )
    received = exchanged(send, SP)
    y_in, c_in, z_in = inside_call(
        place, h, w_z, other_z, small, other_small, xb, sr, misc
    )
    entering = owner_call(own_rates, received, own_taps)
    states = exchanged(entering, SP)
    partial = output_call(
        place, states, out_gain[None], c_in, sr, z_in, y_in, w_out, other_out
    )
    tiles = exchanged(partial.reshape(4, OWN, D), "tp")
    return sum_call(tiles, gate)[None]


def solution(mesh):
    torus = Mesh(
        mesh.devices.reshape(8, 8, mesh.shape["tp"], mesh.shape["dp"]), ("sp_0", "sp_1", "tp", "dp")
    )
    sp_tp = ("sp_0", "sp_1", "tp")
    placed = (
        P("dp", sp_tp, None),
        P("dp", None),
        P("dp", SP, None),
        P(),
        P(None, SP, "tp"),
        P(),
        P("dp", "tp"),
        P("dp", "tp"),
        P("dp", "tp"),
        P("dp", "tp"),
        P(None, "dp", "tp"),
        P(None, "tp"),
        P(None, "tp"),
        P(None, "tp"),
        P(None, "tp"),
        P("tp"),
        P(("tp", "dp"), None),
    )

    return jax.shard_map(
        shards, mesh=torus, in_specs=placed, out_specs=P("dp", sp_tp, None), check_vma=False
    )
```
